32 devices in a mesh: rep: 2 (over x), fs: 8 (over z, y), tp: 2 (over core).
Axes of the slice: x: 2, y: 2, z: 4, core: 2. Of those that a mesh axis runs over, the one named last changes fastest.
Arguments:
- states: bfloat16 [6144, 2048], P(('rep', 'fs'), 'tp'), may hold values from -6 to 6
- mix_gain: float32 [2048], replicated, may hold values from 0.1 to 1.9
- w_value: bfloat16 [2048, 2048], P('fs', 'tp'), may hold values from -1 to 1
- w_gate: bfloat16 [2048, 2048], P('fs', 'tp'), may hold values from -0.125 to 0.125
- conv_kernel: float32 [31, 2048], replicated, may hold values from -1 to 1
- chan_gain: float32 [2048], replicated, may hold values from 0.1 to 1.9
- w_mix_out: bfloat16 [2048, 2048], P('fs', 'tp'), may hold values from -0.125 to 0.125
- mlp_gain: float32 [2048], replicated, may hold values from 0.1 to 1.9
- w_up: bfloat16 [2048, 6144], P('fs', 'tp'), may hold values from -0.125 to 0.125
- w_down_t: bfloat16 [2048, 6144], P('fs', 'tp'), may hold values from -0.078125 to 0.078125
Outputs:
- layer_out: bfloat16 [6144, 2048], P(('rep', 'fs'), 'tp')
The draws below stay inside these ranges and needn't reach their ends.
All inputs are finite; a program needn't handle non-finite values.
Results may differ from the reference program's by a relative error of at most 0.017.
Values may be sent and summed in bfloat16 or wider, within the bound.
A program may use at most 64 MiB of HBM per device.

```python
import jax
import jax.numpy as jnp
from jax import lax

D = 2048
FF = 6144
KWIDTH = 31
LENGTH = 128
SEQS = 3
ROWS = 384
TOKENS = 6144
N_TP = 2


def draw_w_value(key, part):
    first_key, second_key = jax.random.split(jax.random.fold_in(key, 17))
    column = jnp.arange(D, dtype=jnp.float32)
    ramp = 10.0 ** (column / D)
    base = jnp.clip(jax.random.normal(first_key, (D, D), jnp.float32), -6.0, 6.0)
    jitter = jax.random.uniform(second_key, (D,), jnp.float32, 0.7, 1.3)
    scale = ramp * jitter / (3.0 * jnp.sqrt(jnp.float32(D)))
    return jnp.clip(base * scale[None, :], -1.0, 1.0).astype(jnp.bfloat16)


def shard_levels(own_key, shape, cuts, low, high):
    loudness, own = 1.0, jax.random.fold_in(own_key, 6)
    for position, blocks in cuts:
        heights = jnp.exp(jax.random.uniform(jax.random.fold_in(own, position), (blocks,), jnp.float32, low / len(cuts), high / len(cuts)))
        loudness = loudness * jnp.repeat(heights, shape[position] // blocks).reshape([-1 if axis == position else 1 for axis in range(len(shape))])
    return loudness


def normal_values(key, shape, deviation, most, cuts=(), kind=jnp.bfloat16):
    values = deviation * jax.random.normal(key, shape, jnp.float32)
    if cuts:
        values = values * shard_levels(key, shape, cuts, -0.22, 0.18)
    return jnp.clip(values, -most, most).astype(kind)


def setup_inputs(seed: int = 0) -> dict:
    arg_keys = jax.random.split(jax.random.key(seed), 11)
    return {
        "states": normal_values(arg_keys[0], (TOKENS, D), 1.0, 6.0, ((0, 16), (1, 2))),
        "mix_gain": jnp.clip(1.0 + 0.18 * jax.random.normal(arg_keys[1], (D,), jnp.float32), 0.1, 1.9),
        "w_value": draw_w_value(jax.random.fold_in(arg_keys[10], 71), 0),
        "w_gate": normal_values(arg_keys[3], (D, D), D ** -0.5, 0.125, ((0, 8), (1, 2))),
        "conv_kernel": normal_values(arg_keys[4], (KWIDTH, D), KWIDTH ** -0.5, 1.0, (), jnp.float32),
        "chan_gain": jnp.clip(1.0 + 0.18 * jax.random.normal(arg_keys[5], (D,), jnp.float32), 0.1, 1.9),
        "w_mix_out": normal_values(arg_keys[6], (D, D), D ** -0.5, 0.125, ((0, 8), (1, 2))),
        "mlp_gain": jnp.clip(1.0 + 0.18 * jax.random.normal(arg_keys[7], (D,), jnp.float32), 0.1, 1.9),
        "w_up": normal_values(arg_keys[8], (D, FF), D ** -0.5, 0.125, ((0, 8), (1, 2))),
        "w_down_t": normal_values(arg_keys[9], (D, FF), FF ** -0.5, 0.078125, ((0, 8), (1, 2))),
    }


EPS = 1e-06

def rms_norm(rows, gain):
    values = rows.astype(jnp.float32)
    scaled = values * lax.rsqrt(lax.optimization_barrier(jnp.mean(values * values, axis=-1, keepdims=True)) + EPS)
    return (scaled * gain).astype(jnp.bfloat16)

def causal_filter(gated, conv_kernel):
    width = gated.shape[1]
    blocks = gated.reshape(SEQS, LENGTH, width)
    padded = jnp.pad(blocks, ((0, 0), (KWIDTH - 1, 0), (0, 0)))
    total = jnp.zeros_like(blocks)
    for tap in range(KWIDTH):
        total = total + conv_kernel[tap][None, None, :] * padded[:, tap:tap + LENGTH, :]
    return total.reshape(SEQS * LENGTH, width)

def project_out(activated, weight_t):
    block = activated.shape[1] // N_TP
    total = jnp.zeros((activated.shape[0], weight_t.shape[0]), jnp.float32)
    for index in range(N_TP):
        piece = lax.dot_general(activated[:, index * block:(index + 1) * block], weight_t[:, index * block:(index + 1) * block], (((1,), (1,)), ((), ())), preferred_element_type=jnp.float32)
        total = total + piece.astype(jnp.bfloat16).astype(jnp.float32)
    return total

def one_group(rows, mix_gain, w_value, w_gate, conv_kernel, chan_gain, w_mix_out, mlp_gain, w_up, w_down_t):
    normed = rms_norm(rows, mix_gain)
    value = jnp.dot(normed, w_value, preferred_element_type=jnp.float32)
    gate = jnp.dot(normed, w_gate, preferred_element_type=jnp.float32)
    gated = value * jax.nn.sigmoid(gate)
    filtered = causal_filter(gated, conv_kernel)
    mean_rows = lax.optimization_barrier(jnp.mean(filtered, axis=-1, keepdims=True))
    variance = lax.optimization_barrier(jnp.mean(filtered * filtered, axis=-1, keepdims=True)) - mean_rows * mean_rows
    activated = jax.nn.silu((filtered - mean_rows) * lax.rsqrt(variance + EPS) * chan_gain).astype(jnp.bfloat16)
    middle = (rows.astype(jnp.float32) + project_out(activated, w_mix_out)).astype(jnp.bfloat16)
    normed_mid = rms_norm(middle, mlp_gain)
    upward = jnp.dot(normed_mid, w_up, preferred_element_type=jnp.float32)
    hidden = jnp.square(jnp.maximum(upward, 0.0)).astype(jnp.bfloat16)
    return (middle.astype(jnp.float32) + project_out(hidden, w_down_t)).astype(jnp.bfloat16)

def reference(states, mix_gain, w_value, w_gate, conv_kernel, chan_gain, w_mix_out, mlp_gain, w_up, w_down_t):
    groups = states.reshape(states.shape[0] // ROWS, ROWS, states.shape[1])

    def apply(rows):
        return one_group(rows, mix_gain, w_value, w_gate, conv_kernel, chan_gain, w_mix_out, mlp_gain, w_up, w_down_t)
    return lax.map(apply, groups).reshape(states.shape)
```

```python
import functools

import jax
import jax.numpy as jnp
from jax import lax
from jax.experimental import pallas as pl
from jax.experimental.pallas import tpu as pltpu
from jax.sharding import PartitionSpec as P

LENGTH = 128
LANES = 128
LEAD = 32
EPS = 1e-06
MESH = pl.DeviceIdType.MESH


def times_transposed(left, right):
    return lax.dot_general(
        left, right, (((1,), (1,)), ((), ())), preferred_element_type=jnp.float32
    )


def ring_kernel(
    sizes,
    states, mix_gain, w_value, w_gate, conv_kernel, chan_gain, w_mix, mlp_gain, w_up, w_down,
    out,
    weights, rows_in, rows_mid, normed, padded, filtered, activated, hidden,
    own_stats, peer_stats, mix_parts, mix_peers, fed_parts, fed_peers,
    load_sems, ring_send, ring_recv, in_send, in_recv, mid_send, mid_recv,
    stat_send, stat_recv, mix_send, mix_recv, fed_send, fed_recv,
):
    reps, n, tps, rows, channels, width, ups = sizes
    own_width = width * reps
    half_way = n // 2
    shard = channels // n
    tokens = reps * rows
    pieces = tokens // LENGTH
    chunks = 3 + 2 * ups
    rep, fs, tp = lax.axis_index("rep"), lax.axis_index("fs"), lax.axis_index("tp")
    taps = conv_kernel.shape[0]
    blocks, _, block = mix_parts.shape
    per_tp = own_width // block

    def ring_index(place):
        place = lax.rem(place + n, n)
        return jnp.where(place < half_way, 2 * place, 2 * (n - 1 - place) + 1)

    place = jnp.where(lax.rem(fs, 2) == 0, fs // 2, n - 1 - fs // 2)
    neighbours = (ring_index(place + 1), ring_index(place - 1))

    barrier = pltpu.get_barrier_semaphore()
    for other in neighbours:
        pl.semaphore_signal(barrier, inc=1, device_id={"fs": other}, device_id_type=MESH)
    for dr in range(reps):
        for dt in range(tps):
            if dr or dt:
                pl.semaphore_signal(
                    barrier, inc=1,
                    device_id={"rep": lax.rem(rep + dr, reps), "tp": lax.rem(tp + dt, tps)},
                    device_id_type=MESH,
                )

    own_rows = pl.ds(pl.multiple_of(rep * rows, rows), rows)
    own_cols = pl.ds(pl.multiple_of(tp * own_width, own_width), own_width)

    def shard_at(owner, start=0, size=None):
        size = shard if size is None else size
        return pl.ds(pl.multiple_of(owner * shard + start, size), size)

    def hop(c, s, way):
        sign = 1 if way == 0 else -1
        owner = ring_index(place - sign * (s - 1))
        span = shard_at(owner)
        if s == half_way:
            span = shard_at(owner, way * (shard // 2), shard // 2)
        return pltpu.make_async_remote_copy(
            src_ref=weights.at[c, span, :],
            dst_ref=weights.at[c, span, :],
            send_sem=ring_send.at[way, c],
            recv_sem=ring_recv.at[way, c, s - 1],
            device_id={"fs": neighbours[way]},
            device_id_type=MESH,
        )

    loads = []
    for c in range(chunks):
        if c < 3:
            source, column = (w_value, w_gate, w_mix)[c], rep * width
        elif c < 3 + ups:
            source, column = w_up, (rep * ups + c - 3) * width
        else:
            source, column = w_down, (rep * ups + c - 3 - ups) * width
        loads.append(
            pltpu.make_async_copy(
                source.at[:, pl.ds(pl.multiple_of(column, width), width)],
                weights.at[c, shard_at(fs), :],
                load_sems.at[c],
            )
        )
        loads[-1].start()
    own_load = pltpu.make_async_copy(states, rows_in.at[own_rows, own_cols], load_sems.at[chunks])
    own_load.start()
    pl.semaphore_wait(barrier, 1 + reps * tps)

    def pump(c, s):
        for way in range(2):
            if s == 1:
                if way == 0:
                    loads[c].wait()
            else:
                before = hop(c, s - 1, way)
                before.wait_recv()
                before.wait_send()
            hop(c, s, way).start()

    def arrived(c):
        for way in range(2):
            last = hop(c, half_way, way)
            last.wait_recv()
            last.wait_send()

    def spread(source, target, send, recv):
        def copy(dr, dt, ahead):
            if ahead:
                span = pl.ds(pl.multiple_of(lax.rem(rep + reps - dr, reps) * rows, rows), rows)
                src = target.at[span, own_cols]
            else:
                span, src = own_rows, source
            step_r = 0 if ahead else dr
            return pltpu.make_async_remote_copy(
                src_ref=src,
                dst_ref=target.at[span, own_cols],
                send_sem=send.at[dr, dt],
                recv_sem=recv.at[dr, dt],
                device_id={"rep": lax.rem(rep + step_r, reps), "tp": lax.rem(tp + dt, tps)},
                device_id_type=MESH,
            )

        first = [copy(dr, 0, False) for dr in range(1, reps)]
        near = [copy(0, dt, False) for dt in range(1, tps)]
        for one in first + near:
            one.start()

        def forward():
            later = []
            for dr in range(1, reps):
                first[dr - 1].wait_recv()
                for dt in range(1, tps):
                    one = copy(dr, dt, True)
                    one.start()
                    later.append(one)
            return later

        def finish(later):
            for one in near + later:
                one.wait_recv()
            for one in first + near + later:
                one.wait_send()

        return forward, finish

    def norm_all(source, gain):
        def one(i, carry):
            span = pl.ds(pl.multiple_of(i * 64, 64), 64)
            x = source[span, :].astype(jnp.float32)
            scale = lax.rsqrt(jnp.mean(x * x, axis=-1, keepdims=True) + EPS)
            normed[span, :] = (x * scale * gain[...]).astype(jnp.bfloat16)
            return carry

        lax.fori_loop(0, tokens // 64, one, 0)

    def seq_rows(i):
        return pl.ds(pl.multiple_of(i * LENGTH, LENGTH), LENGTH)

    def mixer_rows(i):
        x = normed[seq_rows(i), :]
        value = jnp.dot(x, weights[0], preferred_element_type=jnp.float32)
        gate = jnp.dot(x, weights[1], preferred_element_type=jnp.float32)
        padded[LEAD : LEAD + LENGTH, :] = value * jax.nn.sigmoid(gate)

        def column(j, sums):
            cols = pl.ds(pl.multiple_of(j * LANES, LANES), LANES)
            from_all = pl.multiple_of(tp * own_width + rep * width + j * LANES, LANES)
            kern = conv_kernel[:, pl.ds(from_all, LANES)]
            total = jnp.zeros((LENGTH, LANES), jnp.float32)
            for tap in range(taps):
                begin = LEAD - (taps - 1) + tap
                total = total + kern[tap : tap + 1, :] * padded[begin : begin + LENGTH, cols]
            filtered[seq_rows(i), cols] = total
            return sums[0] + total, sums[1] + total * total

        zero = jnp.zeros((LENGTH, LANES), jnp.float32)
        one, two = lax.fori_loop(0, width // LANES, column, (zero, zero))
        lane = lax.broadcasted_iota(jnp.int32, (LENGTH, LANES), 1)
        both = jnp.where(
            lane == 0,
            jnp.sum(one, axis=-1, keepdims=True),
            jnp.where(lane == 1, jnp.sum(two, axis=-1, keepdims=True), 0.0),
        )
        own_stats[:, seq_rows(i)] = both.T[0:8, :]

    def stat_copies():
        copies = []
        for dr in range(reps):
            for dt in range(tps):
                if dr or dt:
                    copies.append(
                        pltpu.make_async_remote_copy(
                            src_ref=own_stats,
                            dst_ref=peer_stats.at[dr * tps + dt],
                            send_sem=stat_send.at[dr, dt],
                            recv_sem=stat_recv.at[dr, dt],
                            device_id={
                                "rep": lax.rem(rep + dr, reps),
                                "tp": lax.rem(tp + dt, tps),
                            },
                            device_id_type=MESH,
                        )
                    )
        return copies

    def activate_rows(i, carry):
        total = own_stats[:, seq_rows(i)]
        for k in range(1, reps * tps):
            total = total + peer_stats[k, :, seq_rows(i)]
        turned = jnp.concatenate([total] * (LANES // 8), axis=0).T
        mean = turned[:, 0:1] / channels
        variance = turned[:, 1:2] / channels - mean * mean
        gain_at = pl.multiple_of(tp * own_width + rep * width, LANES)
        gain = chan_gain[:, pl.ds(gain_at, width)]
        x = (filtered[seq_rows(i), :] - mean) * lax.rsqrt(variance + EPS) * gain
        activated[seq_rows(i), :] = (x / (1.0 + jnp.exp(-x))).astype(jnp.bfloat16)
        return carry

    def share(order, o, left, pieces_of, parts, peers, send, recv):
        span = pl.ds(pl.multiple_of(o * block, block), block)

        def one(i):
            at = pl.ds(pl.multiple_of(i * rows, rows), rows)
            total = None
            for k, c in enumerate(pieces_of):
                term = times_transposed(
                    left[at, k * width : (k + 1) * width], weights[c, span, :]
                )
                total = term if total is None else total + term
            parts[o, at, :] = total.astype(jnp.bfloat16)

        keeper = o // per_tp
        dt = lax.rem(keeper + tps - tp, tps)
        waits = []
        for dr in [*range(1, reps), 0]:
            to = lax.rem(rep + dr, reps)
            one(to)
            copy = pltpu.make_async_remote_copy(
                src_ref=parts.at[o, pl.ds(pl.multiple_of(to * rows, rows), rows), :],
                dst_ref=peers.at[dr * tps + dt, lax.rem(o, per_tp)],
                send_sem=send.at[order, dr],
                recv_sem=recv.at[dr * tps + dt, lax.rem(o, per_tp)],
                device_id={"rep": to, "tp": keeper},
                device_id_type=MESH,
            )
            if dr:
                copy.start()
                waits.append(copy.wait_send)
            else:
                pl.when(keeper != tp)(copy.start)
                waits.append(lambda k=keeper, c=copy: pl.when(k != tp)(c.wait_send))
        return waits

    def wait_peers(j, parts, peers, send, recv):
        for k in range(1, reps * tps):
            dr, dt = k // tps, k % tps
            pltpu.make_async_remote_copy(
                src_ref=parts.at[0, own_rows, :],
                dst_ref=peers.at[k, j],
                send_sem=send.at[0, 0],
                recv_sem=recv.at[k, j],
                device_id={"rep": lax.rem(rep + dr, reps), "tp": lax.rem(tp + dt, tps)},
                device_id_type=MESH,
            ).wait_recv()

    def total_of(j, parts, peers):
        total = parts[tp * per_tp + j, own_rows, :].astype(jnp.float32)
        for k in range(1, reps * tps):
            total = total + peers[k, j].astype(jnp.float32)
        return total

    stepwise = blocks == n

    def owners(s):
        if s in (0, half_way):
            return [ring_index(place + s)]
        return [ring_index(place - s), ring_index(place + s)]

    def steps_of(c):
        return range(1, half_way + 1)

    first, second = (0, 1), (2, 3)
    third = tuple(range(4, 3 + ups))
    fourth = tuple(range(3 + ups, chunks))

    pump(0, 1)
    pump(1, 1)
    forward, finish = spread(states, rows_in, in_send, in_recv)
    padded[0:LEAD, :] = jnp.zeros((LEAD, width), jnp.float32)
    pump(0, 2)
    pump(1, 2)
    later = forward()
    for s in range(3, half_way + 1):
        pump(0, s)
        if s == 3:
            own_load.wait()
            finish(later)
        pump(1, s)
        if s == 3:
            norm_all(rows_in, mix_gain)
    pump(2, 1)
    pump(3, 1)
    arrived(0)
    arrived(1)

    todo = [(c, s) for s in range(2, half_way + 1) for c in second]

    def next_hop():
        if todo:
            pump(*todo.pop(0))

    for i in range(0, pieces, 2):
        lax.fori_loop(
            i, min(i + 2, pieces), lambda k, carry: (mixer_rows(k), carry)[1], 0
        )
        next_hop()
    stats = stat_copies()
    for one in stats:
        one.start()
    for one in stats:
        one.wait_recv()
    lax.fori_loop(0, pieces, activate_rows, 0)
    waits = []
    mix = (activated, (2,), mix_parts, mix_peers, mix_send, mix_recv)
    if stepwise:
        for s in range(half_way - 1):
            for o in owners(s):
                waits += share(len(waits) // reps, o, *mix)
    while todo:
        next_hop()
    if stepwise:
        for o in owners(half_way - 1):
            waits += share(len(waits) // reps, o, *mix)
    for c in third:
        pump(c, 1)
    arrived(2)
    if stepwise:
        waits += share(len(waits) // reps, owners(half_way)[0], *mix)
    else:
        for o in range(blocks):
            waits += share(o, o, *mix)

    todo = [(c, s) for s in range(2, half_way + 1) for c in third]
    for _ in range(len(todo) // 2):
        next_hop()
    for j in range(per_tp):
        wait_peers(j, mix_parts, mix_peers, mix_send, mix_recv)
        at = pl.ds(pl.multiple_of(tp * own_width + j * block, block), block)
        rows_mid[own_rows, at] = (
            rows_in[own_rows, at].astype(jnp.float32) + total_of(j, mix_parts, mix_peers)
        ).astype(jnp.bfloat16)
    forward, finish = spread(rows_mid.at[own_rows, own_cols], rows_mid, mid_send, mid_recv)
    while todo:
        next_hop()
    for c in fourth:
        pump(c, 1)
    arrived(3)
    for c in third:
        arrived(c)
    later = forward()
    finish(later)
    norm_all(rows_mid, mlp_gain)
    todo = [(c, s) for s in range(2, half_way + 1) for c in fourth]
    next_hop()
    for k in range(ups):

        def up_rows(i, carry):
            at = pl.ds(pl.multiple_of(i * rows, rows), rows)
            x = jnp.dot(normed[at, :], weights[3 + k], preferred_element_type=jnp.float32)
            x = jnp.maximum(x, 0.0)
            hidden[at, k * width : (k + 1) * width] = (x * x).astype(jnp.bfloat16)
            return carry

        lax.fori_loop(0, reps, up_rows, 0)
        next_hop()
    done = []
    fed = (hidden, fourth, fed_parts, fed_peers, fed_send, fed_recv)
    if stepwise:
        for o in owners(0):
            done += share(len(done) // reps, o, *fed)
    for s in range(2, half_way + 1):
        while todo and todo[0][1] <= s:
            next_hop()
        if stepwise:
            for o in owners(s - 1):
                done += share(len(done) // reps, o, *fed)
    for c in fourth:
        arrived(c)
    if stepwise:
        done += share(len(done) // reps, owners(half_way)[0], *fed)
    else:
        for o in range(blocks):
            done += share(o, o, *fed)
    for j in range(per_tp):
        wait_peers(j, fed_parts, fed_peers, fed_send, fed_recv)
        at = pl.ds(pl.multiple_of(tp * own_width + j * block, block), block)
        out[:, j * block : (j + 1) * block] = (
            rows_mid[own_rows, at].astype(jnp.float32) + total_of(j, fed_parts, fed_peers)
        ).astype(jnp.bfloat16)
    for one in stats:
        one.wait_send()
    for wait in waits + done:
        wait()


def ring_body(mesh, states, mix_gain, w_value, w_gate, conv_kernel, chan_gain, w_mix, mlp_gain, w_up, w_down):
    reps, n, tps = mesh.shape["rep"], mesh.shape["fs"], mesh.shape["tp"]
    rows, own_width = states.shape
    width = own_width // reps
    channels = own_width * tps
    ups = w_up.shape[1] // own_width
    tokens = rows * reps
    group = reps * tps
    block = channels // n if channels // n >= LANES else own_width
    blocks, per_tp = channels // block, own_width // block
    chunks = 3 + 2 * ups
    bf16, f32 = jnp.bfloat16, jnp.float32
    vmem, hbm = pl.BlockSpec(memory_space=pltpu.VMEM), pl.BlockSpec(memory_space=pl.ANY)
    dma = pltpu.SemaphoreType.DMA
    return pl.pallas_call(
        functools.partial(ring_kernel, (reps, n, tps, rows, channels, width, ups)),
        out_shape=jax.ShapeDtypeStruct((rows, own_width), bf16),
        in_specs=[hbm, vmem, hbm, hbm, vmem, vmem, hbm, vmem, hbm, hbm],
        out_specs=vmem,
        scratch_shapes=[
            pltpu.VMEM((chunks, channels, width), bf16),
            pltpu.VMEM((tokens, channels), bf16),
            pltpu.VMEM((tokens, channels), bf16),
            pltpu.VMEM((tokens, channels), bf16),
            pltpu.VMEM((LEAD + LENGTH, width), f32),
            pltpu.VMEM((tokens, width), f32),
            pltpu.VMEM((tokens, width), bf16),
            pltpu.VMEM((tokens, ups * width), bf16),
            pltpu.VMEM((8, tokens), f32),
            pltpu.VMEM((group, 8, tokens), f32),
            pltpu.VMEM((blocks, tokens, block), bf16),
            pltpu.VMEM((group, per_tp, rows, block), bf16),
            pltpu.VMEM((blocks, tokens, block), bf16),
            pltpu.VMEM((group, per_tp, rows, block), bf16),
            dma((chunks + 1,)),
            dma((2, chunks)),
            dma((2, chunks, n // 2)),
            dma((reps, tps)),
            dma((reps, tps)),
            dma((reps, tps)),
            dma((reps, tps)),
            dma((reps, tps)),
            dma((reps, tps)),
            dma((blocks, reps)),
            dma((group, per_tp)),
            dma((blocks, reps)),
            dma((group, per_tp)),
        ],
        compiler_params=pltpu.CompilerParams(
            collective_id=0, has_side_effects=True, vmem_limit_bytes=62 * 1024 * 1024
        ),
    )(
        states, mix_gain[None, :], w_value, w_gate, conv_kernel, chan_gain[None, :], w_mix,
        mlp_gain[None, :], w_up, w_down,
    )


def plane_kernel(
    sizes,
    states, mix_gain, w_value, w_gate, conv_kernel, chan_gain, w_mix, mlp_gain, w_up, w_down,
    out,
    weights, rows_in, rows_mid, normed, padded, filtered, activated, hidden, own_in, own_mid,
    own_stats, peer_stats, mix_parts, mix_peers, fed_parts, fed_peers,
    load_sems, y_send, y_recv, near_send, far_send, line_recv, twin_send, twin_recv,
    in_send, in_recv, mid_send, mid_recv,
    stat_send, stat_recv, mix_send, mix_recv, fed_send, fed_recv,
):
    reps, n, tps, rows, channels, sub, ups = sizes
    ys = tps
    zs = n // ys
    members = reps * ys
    width = sub * tps
    own_width = sub * members
    shard = channels // n
    plane_shard = shard * ys
    tokens = reps * rows
    pieces = tokens // LENGTH
    chunks = 3 + 2 * ups
    rep, fs, tp = lax.axis_index("rep"), lax.axis_index("fs"), lax.axis_index("tp")
    z, y = fs // ys, lax.rem(fs, ys)
    other_rep, other_y, other_tp = reps - 1 - rep, ys - 1 - y, tps - 1 - tp
    other_fs = z * ys + other_y
    own_group = rep * ys + y
    taps = conv_kernel.shape[0]
    blocks, _, block = mix_parts.shape
    per_tp = own_width // block

    has_next = (z < zs - 1, z > 0)
    next_fs = (fs + ys, fs - ys)
    is_home = tp == y

    barrier = pltpu.get_barrier_semaphore()
    for dr in range(reps):
        for dy in range(ys):
            for dt in range(tps):
                if dr or dy or dt:
                    pl.semaphore_signal(
                        barrier, inc=1,
                        device_id={
                            "rep": lax.rem(rep + dr, reps),
                            "fs": z * ys + lax.rem(y + dy, ys),
                            "tp": lax.rem(tp + dt, tps),
                        },
                        device_id_type=MESH,
                    )
    for way in range(2):
        @pl.when(has_next[way])
        def _():
            pl.semaphore_signal(
                barrier, inc=1, device_id={"fs": next_fs[way]}, device_id_type=MESH
            )

    def remote(src, dst, send, recv, **where):
        return pltpu.make_async_remote_copy(
            src_ref=src, dst_ref=dst, send_sem=send, recv_sem=recv,
            device_id=where, device_id_type=MESH,
        )

    def rows_of(index, size=shard):
        return pl.ds(pl.multiple_of(index * size, size), size)

    def rep_rows(r):
        return pl.ds(pl.multiple_of(r * rows, rows), rows)

    half = pl.ds(pl.multiple_of(tp * sub, sub), sub)

    def columns_of(c, group):
        if c < 3:
            source, at = (w_value, w_gate, w_mix)[c], group
        elif c < 3 + ups:
            source, at = w_up, group * ups + c - 3
        else:
            source, at = w_down, group * ups + c - 3 - ups
        return source.at[:, pl.ds(pl.multiple_of(at * sub, sub), sub)]

    loads = [
        pltpu.make_async_copy(
            columns_of(c, own_group), weights.at[c, rows_of(fs), half], load_sems.at[c]
        )
        for c in range(chunks)
    ]
    home_cols = pl.ds(pl.multiple_of(tp * own_width, own_width), own_width)
    own_load = pltpu.make_async_copy(states, own_in, load_sems.at[chunks])
    home_load = pltpu.make_async_copy(
        states, rows_in.at[rep_rows(rep), home_cols], load_sems.at[chunks + 1]
    )
    for c in range(chunks):
        loads[c].start()
    pl.when(is_home)(home_load.start)
    own_load.start()
    along_line = sum(jnp.where(has, 1, 0) for has in has_next)
    pl.semaphore_wait(barrier, reps * ys * tps - 1 + along_line)

    def across(c):
        return remote(
            columns_of(c, rep * ys + other_y), weights.at[c, rows_of(fs), half],
            y_send.at[c], y_recv.at[c], fs=other_fs,
        )

    middle = jnp.minimum(z, zs - 1 - z)

    def offset_at(i):
        near = (i + 1) // 2 if i % 2 else -(i // 2)
        far = jnp.where(2 * z < zs - 1, i - middle, middle - i)
        return jnp.where(i <= 2 * middle, near, far)

    offsets = [offset_at(i) for i in range(zs)]
    planes = [z + off for off in offsets]

    def twin(c, i):
        span = rows_of(planes[i], plane_shard)
        return remote(
            weights.at[c, span, half], weights.at[c, span, half],
            twin_send.at[c, i], twin_recv.at[c, i], tp=other_tp,
        )

    def near(c, way, index):
        span = rows_of(index)
        return remote(
            weights.at[c, span, half], weights.at[c, span, half],
            near_send.at[c, way], line_recv.at[way, c, 0], fs=next_fs[way],
        )

    def near_all(c, way):
        span = rows_of(z, plane_shard)
        return remote(
            weights.at[c, span, half], weights.at[c, span, half],
            near_send.at[c, way], line_recv.at[way, c, 0], fs=next_fs[way],
        )

    def own(c):
        loads[c].wait()
        for way in range(2):
            pl.when(has_next[way])(near(c, way, fs).start)
        across(c).wait_recv()
        for way in range(2):
            pl.when(has_next[way])(near(c, way, other_fs).start)
        twin(c, 0).start()

    def far(c, i):
        off, plane = offsets[i], planes[i]
        upward = off < 0
        way = jnp.where(upward, 0, 1)
        step = jnp.abs(off)
        span = rows_of(plane, plane_shard)
        arrival = remote(
            weights.at[c, span, half], weights.at[c, span, half],
            far_send.at[c, i - 1], line_recv.at[way, c, step - 1], fs=other_fs,
        )
        goes = jnp.where(upward, z < zs - 1, z > 0)
        onward = remote(
            weights.at[c, span, half], weights.at[c, span, half],
            far_send.at[c, i - 1], line_recv.at[way, c, jnp.minimum(step, zs - 2)],
            fs=jnp.where(upward, fs + ys, fs - ys),
        )
        return arrival, goes, onward

    def arrive(c, i):
        arrival, goes, onward = far(c, i)
        arrival.wait_recv()
        pl.when(goes)(onward.start)
        twin(c, i).start()

    def ready(c, i):
        twin(c, i).wait_recv()

    def drain(c):
        across(c).wait_send()
        for way in range(2):
            pl.when(has_next[way])(near_all(c, way).wait_send)
        for i in range(zs):
            twin(c, i).wait_send()
            if i:
                _, goes, onward = far(c, i)
                pl.when(goes)(onward.wait_send)

    def spread(source, target, send, recv):
        def at(r, h, j):
            start = pl.multiple_of(h * own_width + j * block, block)
            return target.at[rep_rows(r), pl.ds(start, block)]

        def copies(j):
            src = source.at[:, j * block : (j + 1) * block]
            dst = at(rep, tp, j)
            along = remote(src, dst, send.at[0, j], recv.at[1, tp, j], rep=other_rep, tp=y)
            over = remote(src, dst, send.at[1, j], recv.at[0, tp, j], fs=other_fs, tp=y)
            inside = remote(src, dst, send.at[2, j], recv.at[0, tp, j], tp=y)
            return along, over, inside

        def passing(j):
            one, two = at(other_rep, 0, j), at(rep, 1, j)
            over = remote(one, one, send.at[3, j], recv.at[1, 0, j], fs=other_fs)
            along = remote(two, two, send.at[3, j], recv.at[1, 1, j], rep=other_rep)
            return over, along

        def arrival(dr, h, j):
            dst = at(rep if dr == 0 else other_rep, h, j)
            return remote(dst, dst, send.at[0, j], recv.at[dr, h, j], rep=other_rep)

        def start(j):
            along, over, inside = copies(j)
            along.start()
            over.start()
            pl.when(jnp.logical_not(is_home))(inside.start)

        def forward(j):
            over, along = passing(j)

            @pl.when(is_home)
            def _():
                arrival(1, 0, j).wait_recv()
                over.start()

            @pl.when(jnp.logical_not(is_home))
            def _():
                arrival(0, 1, j).wait_recv()
                along.start()

        def finish(j):
            arrival(1, 1, j).wait_recv()

            @pl.when(is_home)
            def _():
                arrival(0, other_tp, j).wait_recv()

            @pl.when(jnp.logical_not(is_home))
            def _():
                arrival(0, 0, j).wait_recv()
                arrival(1, 0, j).wait_recv()

        def settle(j):
            along, over, inside = copies(j)
            along.wait_send()
            over.wait_send()
            pl.when(jnp.logical_not(is_home))(inside.wait_send)
            passing(j)[0].wait_send()

        return start, forward, finish, settle

    def norm_all(source, gain):
        def one(i, carry):
            span = pl.ds(pl.multiple_of(i * 64, 64), 64)
            x = source[span, :].astype(jnp.float32)
            scale = lax.rsqrt(jnp.mean(x * x, axis=-1, keepdims=True) + EPS)
            normed[span, :] = (x * scale * gain[...]).astype(jnp.bfloat16)
            return carry

        lax.fori_loop(0, tokens // 64, one, 0)

    def seq_rows(i):
        return pl.ds(pl.multiple_of(i * LENGTH, LENGTH), LENGTH)

    def mixer_rows(i):
        x = normed[seq_rows(i), :]
        value = jnp.dot(x, weights[0], preferred_element_type=jnp.float32)
        gate = jnp.dot(x, weights[1], preferred_element_type=jnp.float32)
        padded[LEAD : LEAD + LENGTH, :] = value * jax.nn.sigmoid(gate)
        per_sub = sub // LANES

        def column(j, sums):
            cols = pl.ds(pl.multiple_of(j * LANES, LANES), LANES)
            from_all = pl.multiple_of(
                (j // per_sub) * own_width + own_group * sub + lax.rem(j, per_sub) * LANES, LANES
            )
            kern = conv_kernel[:, pl.ds(from_all, LANES)]
            total = jnp.zeros((LENGTH, LANES), jnp.float32)
            for tap in range(taps):
                begin = LEAD - (taps - 1) + tap
                total = total + kern[tap : tap + 1, :] * padded[begin : begin + LENGTH, cols]
            filtered[seq_rows(i), cols] = total
            return sums[0] + total, sums[1] + total * total

        zero = jnp.zeros((LENGTH, LANES), jnp.float32)
        one, two = lax.fori_loop(0, width // LANES, column, (zero, zero))
        lane = lax.broadcasted_iota(jnp.int32, (LENGTH, LANES), 1)
        both = jnp.where(
            lane == 0,
            jnp.sum(one, axis=-1, keepdims=True),
            jnp.where(lane == 1, jnp.sum(two, axis=-1, keepdims=True), 0.0),
        )
        own_stats[:, seq_rows(i)] = both.T[0:8, :]

    def stat_copies():
        return [
            remote(
                own_stats, peer_stats.at[dr * ys + dy], stat_send.at[dr, dy],
                stat_recv.at[dr, dy],
                rep=lax.rem(rep + dr, reps), fs=z * ys + lax.rem(y + dy, ys),
            )
            for dr in range(reps) for dy in range(ys) if dr or dy
        ]

    def activate_rows(i, carry):
        total = own_stats[:, seq_rows(i)]
        for k in range(1, members):
            total = total + peer_stats[k, :, seq_rows(i)]
        turned = jnp.concatenate([total] * (LANES // 8), axis=0).T
        mean = turned[:, 0:1] / channels
        variance = turned[:, 1:2] / channels - mean * mean
        gain = jnp.concatenate(
            [
                chan_gain[:, pl.ds(pl.multiple_of(t * own_width + own_group * sub, sub), sub)]
                for t in range(tps)
            ],
            axis=1,
        )
        x = (filtered[seq_rows(i), :] - mean) * lax.rsqrt(variance + EPS) * gain
        activated[seq_rows(i), :] = (x / (1.0 + jnp.exp(-x))).astype(jnp.bfloat16)
        return carry

    def share(order, o, left, pieces_of, parts, peers, send, recv):
        span = rows_of(o, block)
        keeper, kept = o // per_tp, lax.rem(o, per_tp)
        waits = []
        for dr in [*range(1, reps), 0]:
            to = lax.rem(rep + dr, reps)
            at = rep_rows(to)
            total = None
            for k, c in enumerate(pieces_of):
                term = times_transposed(
                    left[at, k * width : (k + 1) * width], weights[c, span, :]
                )
                total = term if total is None else total + term
            parts[o, at, :] = total.astype(jnp.bfloat16)
            slot = (reps - dr) % reps * ys + lax.rem(y + ys - tp, ys)
            copy = remote(
                parts.at[o, at, :], peers.at[slot, kept], send.at[order, dr],
                recv.at[slot, kept], rep=to, fs=z * ys + tp, tp=keeper,
            )
            if dr:
                copy.start()
                waits.append(copy.wait_send)
            else:
                away = jnp.logical_not(jnp.logical_and(is_home, keeper == tp))
                pl.when(away)(copy.start)
                waits.append(lambda w=away, c=copy: pl.when(w)(c.wait_send))
        return waits

    def wait_peers(j, parts, peers, send, recv):
        def one(k):
            return remote(
                parts.at[0, rep_rows(rep), :], peers.at[k, j], send.at[0, 0], recv.at[k, j],
                rep=other_rep,
            )

        for k in range(1, members):
            one(k).wait_recv()

        @pl.when(is_home)
        def _():
            peers[0, j] = parts[tp * per_tp + j, rep_rows(rep), :]

        pl.when(jnp.logical_not(is_home))(one(0).wait_recv)

    def total_of(j, peers):
        total = peers[0, j].astype(jnp.float32)
        for k in range(1, members):
            total = total + peers[k, j].astype(jnp.float32)
        return total

    third = tuple(range(3, 3 + ups))
    fourth = tuple(range(3 + ups, chunks))
    per_plane = plane_shard // block

    start_in, forward_in, finish_in, settle_in = spread(states, rows_in, in_send, in_recv)
    start_mid, forward_mid, finish_mid, settle_mid = spread(own_mid, rows_mid, mid_send, mid_recv)

    across(0).start()
    across(1).start()
    own(0)
    for j in range(per_tp):
        start_in(j)
    own(1)
    for c in range(2, chunks):
        across(c).start()
    padded[0:LEAD, :] = jnp.zeros((LEAD, width), jnp.float32)
    arrive(0, 1)
    for j in range(per_tp // 2):
        forward_in(j)
    arrive(0, 2)
    for j in range(per_tp // 2, per_tp):
        forward_in(j)
    arrive(0, 3)
    own(2)
    pl.when(is_home)(home_load.wait)
    arrive(1, 1)
    for j in range(per_tp):
        finish_in(j)
    norm_all(rows_in, mix_gain)
    arrive(1, 2)
    own(3)
    arrive(1, 3)
    for c in (0, 1):
        for i in range(zs):
            ready(c, i)

    todo = [functools.partial(arrive, 2, i) for i in range(1, zs)]
    todo.append(functools.partial(own, 4))
    for i in range(0, pieces, 2):
        lax.fori_loop(
            i, min(i + 2, pieces), lambda k, carry: (mixer_rows(k), carry)[1], 0
        )
        if todo:
            todo.pop(0)()
    stats = stat_copies()
    for one in stats:
        one.start()
    while todo:
        todo.pop(0)()
    for one in stats:
        one.wait_recv()
    lax.fori_loop(0, pieces, activate_rows, 0)
    waits = []
    mix = (activated, (2,), mix_parts, mix_peers, mix_send, mix_recv)
    for i in range(zs):
        ready(2, i)
        for b in range(per_plane):
            waits += share(len(waits) // reps, planes[i] * per_plane + b, *mix)

    todo = [functools.partial(arrive, 3, i) for i in range(1, zs)]
    for c in range(4, 3 + ups):
        todo.append(functools.partial(own, c + 1))
        todo += [functools.partial(arrive, c, i) for i in range(1, zs)]
    todo += [functools.partial(own, c) for c in range(4 + ups, chunks)]
    steps = 2 * per_tp + 1
    cuts = [len(todo) * k // steps for k in range(steps + 1)]

    def do_some(k):
        for one in todo[cuts[k] : cuts[k + 1]]:
            one()

    own_load.wait()
    do_some(0)
    for j in range(per_tp):
        wait_peers(j, mix_parts, mix_peers, mix_send, mix_recv)
        cols = slice(j * block, (j + 1) * block)
        own_mid[:, cols] = (
            own_in[:, cols].astype(jnp.float32) + total_of(j, mix_peers)
        ).astype(jnp.bfloat16)
        start_mid(j)

        @pl.when(is_home)
        def _():
            start = pl.multiple_of(tp * own_width + j * block, block)
            rows_mid[rep_rows(rep), pl.ds(start, block)] = own_mid[:, cols]

        do_some(1 + j)
        if j:
            forward_mid(j - 1)
    forward_mid(per_tp - 1)
    for j in range(per_tp):
        do_some(1 + per_tp + j)
        finish_mid(j)
    norm_all(rows_mid, mlp_gain)
    for c in third:
        for i in range(zs):
            ready(c, i)

    def up_some(k):
        def up_rows(i, carry):
            at = rep_rows(i)
            x = jnp.dot(normed[at, :], weights[3 + k], preferred_element_type=jnp.float32)
            x = jnp.maximum(x, 0.0)
            hidden[at, k * width : (k + 1) * width] = (x * x).astype(jnp.bfloat16)
            return carry

        lax.fori_loop(0, reps, up_rows, 0)

    for k in range(ups):
        up_some(k)
        arrive(fourth[k], 1)
    done = []
    fed = (hidden, fourth, fed_parts, fed_peers, fed_send, fed_recv)
    for i in range(zs):
        if i > 1:
            for c in fourth:
                arrive(c, i)
        for c in fourth:
            ready(c, i)
        for b in range(per_plane):
            done += share(len(done) // reps, planes[i] * per_plane + b, *fed)
    for j in range(per_tp):
        wait_peers(j, fed_parts, fed_peers, fed_send, fed_recv)
        cols = slice(j * block, (j + 1) * block)
        out[:, cols] = (
            own_mid[:, cols].astype(jnp.float32) + total_of(j, fed_peers)
        ).astype(jnp.bfloat16)
    for one in stats:
        one.wait_send()
    for j in range(per_tp):
        settle_in(j)
        settle_mid(j)
    for c in range(chunks):
        drain(c)
    for wait in waits + done:
        wait()


def plane_body(mesh, states, mix_gain, w_value, w_gate, conv_kernel, chan_gain, w_mix, mlp_gain, w_up, w_down):
    reps, n, tps = mesh.shape["rep"], mesh.shape["fs"], mesh.shape["tp"]
    rows, own_width = states.shape
    ys = tps
    zs, members = n // ys, reps * ys
    sub = own_width // members
    width = sub * tps
    channels = own_width * tps
    ups = w_up.shape[1] // own_width
    tokens = rows * reps
    block = channels // n
    blocks, per_tp = channels // block, own_width // block
    chunks = 3 + 2 * ups
    bf16, f32 = jnp.bfloat16, jnp.float32
    vmem, hbm = pl.BlockSpec(memory_space=pltpu.VMEM), pl.BlockSpec(memory_space=pl.ANY)
    dma = pltpu.SemaphoreType.DMA
    return pl.pallas_call(
        functools.partial(plane_kernel, (reps, n, tps, rows, channels, sub, ups)),
        out_shape=jax.ShapeDtypeStruct((rows, own_width), bf16),
        in_specs=[hbm, vmem, hbm, hbm, vmem, vmem, hbm, vmem, hbm, hbm],
        out_specs=vmem,
        scratch_shapes=[
            pltpu.VMEM((chunks, channels, width), bf16),
            pltpu.VMEM((tokens, channels), bf16),
            pltpu.VMEM((tokens, channels), bf16),
            pltpu.VMEM((tokens, channels), bf16),
            pltpu.VMEM((LEAD + LENGTH, width), f32),
            pltpu.VMEM((tokens, width), f32),
            pltpu.VMEM((tokens, width), bf16),
            pltpu.VMEM((tokens, ups * width), bf16),
            pltpu.VMEM((rows, own_width), bf16),
            pltpu.VMEM((rows, own_width), bf16),
            pltpu.VMEM((8, tokens), f32),
            pltpu.VMEM((members, 8, tokens), f32),
            pltpu.VMEM((blocks, tokens, block), bf16),
            pltpu.VMEM((members, per_tp, rows, block), bf16),
            pltpu.VMEM((blocks, tokens, block), bf16),
            pltpu.VMEM((members, per_tp, rows, block), bf16),
            dma((chunks + 2,)),
            dma((chunks,)),
            dma((chunks,)),
            dma((chunks, 2)),
            dma((chunks, zs - 1)),
            dma((2, chunks, zs - 1)),
            dma((chunks, zs)),
            dma((chunks, zs)),
            dma((4, per_tp)),
            dma((reps, tps, per_tp)),
            dma((4, per_tp)),
            dma((reps, tps, per_tp)),
            dma((reps, ys)),
            dma((reps, ys)),
            dma((blocks, reps)),
            dma((members, per_tp)),
            dma((blocks, reps)),
            dma((members, per_tp)),
        ],
        compiler_params=pltpu.CompilerParams(
            collective_id=0, has_side_effects=True, vmem_limit_bytes=62 * 1024 * 1024
        ),
    )(
        states, mix_gain[None, :], w_value, w_gate, conv_kernel, chan_gain[None, :], w_mix,
        mlp_gain[None, :], w_up, w_down,
    )


def body(mesh, states, *weights):
    reps, n, tps = mesh.shape["rep"], mesh.shape["fs"], mesh.shape["tp"]
    own_width = states.shape[1]
    channels = own_width * tps
    planar = (
        reps == tps == 2
        and n % tps == 0
        and n // tps > 2
        and own_width % (reps * tps * LANES) == 0
        and channels % (n * LANES) == 0
        and own_width % (channels // n) == 0
    )
    return (plane_body if planar else ring_body)(mesh, states, *weights)


def solution(mesh):
    in_specs = (
        P(("rep", "fs"), "tp"),
        P(),
        P("fs", "tp"),
        P("fs", "tp"),
        P(),
        P(),
        P("fs", "tp"),
        P(),
        P("fs", "tp"),
        P("fs", "tp"),
    )
    out_specs = P(("rep", "fs"), "tp")
    return jax.shard_map(
        functools.partial(body, mesh),
        mesh=mesh, in_specs=in_specs, out_specs=out_specs, check_vma=False,
    )
```

```python
import functools

import jax
import jax.numpy as jnp
from jax import lax
from jax.experimental import pallas as pl
from jax.experimental.pallas import tpu as pltpu
from jax.sharding import PartitionSpec as P

LENGTH = 128
LANES = 128
LEAD = 32
EPS = 1e-06
MESH = pl.DeviceIdType.MESH


def times_transposed(left, right):
    return lax.dot_general(
        left, right, (((1,), (1,)), ((), ())), preferred_element_type=jnp.float32
    )


def ring_kernel(
    sizes,
    states, mix_gain, w_value, w_gate, conv_kernel, chan_gain, w_mix, mlp_gain, w_up, w_down,
    out,
    weights, rows_in, rows_mid, normed, padded, filtered, activated, hidden,
    own_stats, peer_stats, mix_parts, mix_peers, fed_parts, fed_peers,
    load_sems, ring_send, ring_recv, in_send, in_recv, mid_send, mid_recv,
    stat_send, stat_recv, mix_send, mix_recv, fed_send, fed_recv,
):
    reps, n, tps, rows, channels, width, ups = sizes
    own_width = width * reps
    half_way = n // 2
    shard = channels // n
    tokens = reps * rows
    pieces = tokens // LENGTH
    chunks = 3 + 2 * ups
    rep, fs, tp = lax.axis_index("rep"), lax.axis_index("fs"), lax.axis_index("tp")
    taps = conv_kernel.shape[0]
    blocks, _, block = mix_parts.shape
    per_tp = own_width // block

    def ring_index(place):
        place = lax.rem(place + n, n)
        return jnp.where(place < half_way, 2 * place, 2 * (n - 1 - place) + 1)

    place = jnp.where(lax.rem(fs, 2) == 0, fs // 2, n - 1 - fs // 2)
    neighbours = (ring_index(place + 1), ring_index(place - 1))

    barrier = pltpu.get_barrier_semaphore()
    for other in neighbours:
        pl.semaphore_signal(barrier, inc=1, device_id={"fs": other}, device_id_type=MESH)
    for dr in range(reps):
        for dt in range(tps):
            if dr or dt:
                pl.semaphore_signal(
                    barrier, inc=1,
                    device_id={"rep": lax.rem(rep + dr, reps), "tp": lax.rem(tp + dt, tps)},
                    device_id_type=MESH,
                )

    own_rows = pl.ds(pl.multiple_of(rep * rows, rows), rows)
    own_cols = pl.ds(pl.multiple_of(tp * own_width, own_width), own_width)

    def shard_at(owner, start=0, size=None):
        size = shard if size is None else size
        return pl.ds(pl.multiple_of(owner * shard + start, size), size)

    def hop(c, s, way):
        sign = 1 if way == 0 else -1
        owner = ring_index(place - sign * (s - 1))
        span = shard_at(owner)
        if s == half_way:
            span = shard_at(owner, way * (shard // 2), shard // 2)
        return pltpu.make_async_remote_copy(
            src_ref=weights.at[c, span, :],
            dst_ref=weights.at[c, span, :],
            send_sem=ring_send.at[way, c],
            recv_sem=ring_recv.at[way, c, s - 1],
            device_id={"fs": neighbours[way]},
            device_id_type=MESH,
        )

    loads = []
    for c in range(chunks):
        if c < 3:
            source, column = (w_value, w_gate, w_mix)[c], rep * width
        elif c < 3 + ups:
            source, column = w_up, (rep * ups + c - 3) * width
        else:
            source, column = w_down, (rep * ups + c - 3 - ups) * width
        loads.append(
            pltpu.make_async_copy(
                source.at[:, pl.ds(pl.multiple_of(column, width), width)],
                weights.at[c, shard_at(fs), :],
                load_sems.at[c],
            )
        )
        loads[-1].start()
    own_load = pltpu.make_async_copy(states, rows_in.at[own_rows, own_cols], load_sems.at[chunks])
    own_load.start()
    pl.semaphore_wait(barrier, 1 + reps * tps)

    def pump(c, s):
        for way in range(2):
            if s == 1:
                if way == 0:
                    loads[c].wait()
            else:
                before = hop(c, s - 1, way)
                before.wait_recv()
                before.wait_send()
            hop(c, s, way).start()

    def arrived(c):
        for way in range(2):
            last = hop(c, half_way, way)
            last.wait_recv()
            last.wait_send()

    def spread(source, target, send, recv):
        def copy(dr, dt, ahead):
            if ahead:
                span = pl.ds(pl.multiple_of(lax.rem(rep + reps - dr, reps) * rows, rows), rows)
                src = target.at[span, own_cols]
            else:
                span, src = own_rows, source
            step_r = 0 if ahead else dr
            return pltpu.make_async_remote_copy(
                src_ref=src,
                dst_ref=target.at[span, own_cols],
                send_sem=send.at[dr, dt],
                recv_sem=recv.at[dr, dt],
                device_id={"rep": lax.rem(rep + step_r, reps), "tp": lax.rem(tp + dt, tps)},
                device_id_type=MESH,
            )

        first = [copy(dr, 0, False) for dr in range(1, reps)]
        near = [copy(0, dt, False) for dt in range(1, tps)]
        for one in first + near:
            one.start()

        def forward():
            later = []
            for dr in range(1, reps):
                first[dr - 1].wait_recv()
                for dt in range(1, tps):
                    one = copy(dr, dt, True)
                    one.start()
                    later.append(one)
            return later

        def finish(later):
            for one in near + later:
                one.wait_recv()
            for one in first + near + later:
                one.wait_send()

        return forward, finish

    def norm_all(source, gain):
        def one(i, carry):
            span = pl.ds(pl.multiple_of(i * 64, 64), 64)
            x = source[span, :].astype(jnp.float32)
            scale = lax.rsqrt(jnp.mean(x * x, axis=-1, keepdims=True) + EPS)
            normed[span, :] = (x * scale * gain[...]).astype(jnp.bfloat16)
            return carry

        lax.fori_loop(0, tokens // 64, one, 0)

    def seq_rows(i):
        return pl.ds(pl.multiple_of(i * LENGTH, LENGTH), LENGTH)

    def mixer_rows(i):
        x = normed[seq_rows(i), :]
        value = jnp.dot(x, weights[0], preferred_element_type=jnp.float32)
        gate = jnp.dot(x, weights[1], preferred_element_type=jnp.float32)
        padded[LEAD : LEAD + LENGTH, :] = value * jax.nn.sigmoid(gate)

        def column(j, sums):
            cols = pl.ds(pl.multiple_of(j * LANES, LANES), LANES)
            from_all = pl.multiple_of(tp * own_width + rep * width + j * LANES, LANES)
            kern = conv_kernel[:, pl.ds(from_all, LANES)]
            total = jnp.zeros((LENGTH, LANES), jnp.float32)
            for tap in range(taps):
                begin = LEAD - (taps - 1) + tap
                total = total + kern[tap : tap + 1, :] * padded[begin : begin + LENGTH, cols]
            filtered[seq_rows(i), cols] = total
            return sums[0] + total, sums[1] + total * total

        zero = jnp.zeros((LENGTH, LANES), jnp.float32)
        one, two = lax.fori_loop(0, width // LANES, column, (zero, zero))
        lane = lax.broadcasted_iota(jnp.int32, (LENGTH, LANES), 1)
        both = jnp.where(
            lane == 0,
            jnp.sum(one, axis=-1, keepdims=True),
            jnp.where(lane == 1, jnp.sum(two, axis=-1, keepdims=True), 0.0),
        )
        own_stats[:, seq_rows(i)] = both.T[0:8, :]

    def stat_copies():
        copies = []
        for dr in range(reps):
            for dt in range(tps):
                if dr or dt:
                    copies.append(
                        pltpu.make_async_remote_copy(
                            src_ref=own_stats,
                            dst_ref=peer_stats.at[dr * tps + dt],
                            send_sem=stat_send.at[dr, dt],
                            recv_sem=stat_recv.at[dr, dt],
                            device_id={
                                "rep": lax.rem(rep + dr, reps),
                                "tp": lax.rem(tp + dt, tps),
                            },
                            device_id_type=MESH,
                        )
                    )
        return copies

    def activate_rows(i, carry):
        total = own_stats[:, seq_rows(i)]
        for k in range(1, reps * tps):
            total = total + peer_stats[k, :, seq_rows(i)]
        turned = jnp.concatenate([total] * (LANES // 8), axis=0).T
        mean = turned[:, 0:1] / channels
        variance = turned[:, 1:2] / channels - mean * mean
        gain_at = pl.multiple_of(tp * own_width + rep * width, LANES)
        gain = chan_gain[:, pl.ds(gain_at, width)]
        x = (filtered[seq_rows(i), :] - mean) * lax.rsqrt(variance + EPS) * gain
        activated[seq_rows(i), :] = (x / (1.0 + jnp.exp(-x))).astype(jnp.bfloat16)
        return carry

    def share(order, o, left, pieces_of, parts, peers, send, recv):
        span = pl.ds(pl.multiple_of(o * block, block), block)

        def one(i):
            at = pl.ds(pl.multiple_of(i * rows, rows), rows)
            total = None
            for k, c in enumerate(pieces_of):
                term = times_transposed(
                    left[at, k * width : (k + 1) * width], weights[c, span, :]
                )
                total = term if total is None else total + term
            parts[o, at, :] = total.astype(jnp.bfloat16)

        keeper = o // per_tp
        dt = lax.rem(keeper + tps - tp, tps)
        waits = []
        for dr in [*range(1, reps), 0]:
            to = lax.rem(rep + dr, reps)
            one(to)
            copy = pltpu.make_async_remote_copy(
                src_ref=parts.at[o, pl.ds(pl.multiple_of(to * rows, rows), rows), :],
                dst_ref=peers.at[dr * tps + dt, lax.rem(o, per_tp)],
                send_sem=send.at[order, dr],
                recv_sem=recv.at[dr * tps + dt, lax.rem(o, per_tp)],
                device_id={"rep": to, "tp": keeper},
                device_id_type=MESH,
            )
            if dr:
                copy.start()
                waits.append(copy.wait_send)
            else:
                pl.when(keeper != tp)(copy.start)
                waits.append(lambda k=keeper, c=copy: pl.when(k != tp)(c.wait_send))
        return waits

    def wait_peers(j, parts, peers, send, recv):
        for k in range(1, reps * tps):
            dr, dt = k // tps, k % tps
            pltpu.make_async_remote_copy(
                src_ref=parts.at[0, own_rows, :],
                dst_ref=peers.at[k, j],
                send_sem=send.at[0, 0],
                recv_sem=recv.at[k, j],
                device_id={"rep": lax.rem(rep + dr, reps), "tp": lax.rem(tp + dt, tps)},
                device_id_type=MESH,
            ).wait_recv()

    def total_of(j, parts, peers):
        total = parts[tp * per_tp + j, own_rows, :].astype(jnp.float32)
        for k in range(1, reps * tps):
            total = total + peers[k, j].astype(jnp.float32)
        return total

    stepwise = blocks == n

    def owners(s):
        if s in (0, half_way):
            return [ring_index(place + s)]
        return [ring_index(place - s), ring_index(place + s)]

    def steps_of(c):
        return range(1, half_way + 1)

    first, second = (0, 1), (2, 3)
    third = tuple(range(4, 3 + ups))
    fourth = tuple(range(3 + ups, chunks))

    pump(0, 1)
    pump(1, 1)
    forward, finish = spread(states, rows_in, in_send, in_recv)
    padded[0:LEAD, :] = jnp.zeros((LEAD, width), jnp.float32)
    pump(0, 2)
    pump(1, 2)
    later = forward()
    for s in range(3, half_way + 1):
        pump(0, s)
        if s == 3:
            own_load.wait()
            finish(later)
        pump(1, s)
        if s == 3:
            norm_all(rows_in, mix_gain)
    pump(2, 1)
    pump(3, 1)
    arrived(0)
    arrived(1)

    todo = [(c, s) for s in range(2, half_way + 1) for c in second]

    def next_hop():
        if todo:
            pump(*todo.pop(0))

    for i in range(0, pieces, 2):
        lax.fori_loop(
            i, min(i + 2, pieces), lambda k, carry: (mixer_rows(k), carry)[1], 0
        )
        next_hop()
    stats = stat_copies()
    for one in stats:
        one.start()
    for one in stats:
        one.wait_recv()
    lax.fori_loop(0, pieces, activate_rows, 0)
    waits = []
    mix = (activated, (2,), mix_parts, mix_peers, mix_send, mix_recv)
    if stepwise:
        for s in range(half_way - 1):
            for o in owners(s):
                waits += share(len(waits) // reps, o, *mix)
    while todo:
        next_hop()
    if stepwise:
        for o in owners(half_way - 1):
            waits += share(len(waits) // reps, o, *mix)
    for c in third:
        pump(c, 1)
    arrived(2)
    if stepwise:
        waits += share(len(waits) // reps, owners(half_way)[0], *mix)
    else:
        for o in range(blocks):
            waits += share(o, o, *mix)

    todo = [(c, s) for s in range(2, half_way + 1) for c in third]
    for _ in range(len(todo) // 2):
        next_hop()
    for j in range(per_tp):
        wait_peers(j, mix_parts, mix_peers, mix_send, mix_recv)
        at = pl.ds(pl.multiple_of(tp * own_width + j * block, block), block)
        rows_mid[own_rows, at] = (
            rows_in[own_rows, at].astype(jnp.float32) + total_of(j, mix_parts, mix_peers)
        ).astype(jnp.bfloat16)
    forward, finish = spread(rows_mid.at[own_rows, own_cols], rows_mid, mid_send, mid_recv)
    while todo:
        next_hop()
    for c in fourth:
        pump(c, 1)
    arrived(3)
    for c in third:
        arrived(c)
    later = forward()
    finish(later)
    norm_all(rows_mid, mlp_gain)
    todo = [(c, s) for s in range(2, half_way + 1) for c in fourth]
    next_hop()
    for k in range(ups):

        def up_rows(i, carry):
            at = pl.ds(pl.multiple_of(i * rows, rows), rows)
            x = jnp.dot(normed[at, :], weights[3 + k], preferred_element_type=jnp.float32)
            x = jnp.maximum(x, 0.0)
            hidden[at, k * width : (k + 1) * width] = (x * x).astype(jnp.bfloat16)
            return carry

        lax.fori_loop(0, reps, up_rows, 0)
        next_hop()
    done = []
    fed = (hidden, fourth, fed_parts, fed_peers, fed_send, fed_recv)
    if stepwise:
        for o in owners(0):
            done += share(len(done) // reps, o, *fed)
    for s in range(2, half_way + 1):
        while todo and todo[0][1] <= s:
            next_hop()
        if stepwise:
            for o in owners(s - 1):
                done += share(len(done) // reps, o, *fed)
    for c in fourth:
        arrived(c)
    if stepwise:
        done += share(len(done) // reps, owners(half_way)[0], *fed)
    else:
        for o in range(blocks):
            done += share(o, o, *fed)
    for j in range(per_tp):
        wait_peers(j, fed_parts, fed_peers, fed_send, fed_recv)
        at = pl.ds(pl.multiple_of(tp * own_width + j * block, block), block)
        out[:, j * block : (j + 1) * block] = (
            rows_mid[own_rows, at].astype(jnp.float32) + total_of(j, fed_parts, fed_peers)
        ).astype(jnp.bfloat16)
    for one in stats:
        one.wait_send()
    for wait in waits + done:
        wait()


def ring_body(mesh, states, mix_gain, w_value, w_gate, conv_kernel, chan_gain, w_mix, mlp_gain, w_up, w_down):
    reps, n, tps = mesh.shape["rep"], mesh.shape["fs"], mesh.shape["tp"]
    rows, own_width = states.shape
    width = own_width // reps
    channels = own_width * tps
    ups = w_up.shape[1] // own_width
    tokens = rows * reps
    group = reps * tps
    block = channels // n if channels // n >= LANES else own_width
    blocks, per_tp = channels // block, own_width // block
    chunks = 3 + 2 * ups
    bf16, f32 = jnp.bfloat16, jnp.float32
    vmem, hbm = pl.BlockSpec(memory_space=pltpu.VMEM), pl.BlockSpec(memory_space=pl.ANY)
    dma = pltpu.SemaphoreType.DMA
    return pl.pallas_call(
        functools.partial(ring_kernel, (reps, n, tps, rows, channels, width, ups)),
        out_shape=jax.ShapeDtypeStruct((rows, own_width), bf16),
        in_specs=[hbm, vmem, hbm, hbm, vmem, vmem, hbm, vmem, hbm, hbm],
        out_specs=vmem,
        scratch_shapes=[
            pltpu.VMEM((chunks, channels, width), bf16),
            pltpu.VMEM((tokens, channels), bf16),
            pltpu.VMEM((tokens, channels), bf16),
            pltpu.VMEM((tokens, channels), bf16),
            pltpu.VMEM((LEAD + LENGTH, width), f32),
            pltpu.VMEM((tokens, width), f32),
            pltpu.VMEM((tokens, width), bf16),
            pltpu.VMEM((tokens, ups * width), bf16),
            pltpu.VMEM((8, tokens), f32),
            pltpu.VMEM((group, 8, tokens), f32),
            pltpu.VMEM((blocks, tokens, block), bf16),
            pltpu.VMEM((group, per_tp, rows, block), bf16),
            pltpu.VMEM((blocks, tokens, block), bf16),
            pltpu.VMEM((group, per_tp, rows, block), bf16),
            dma((chunks + 1,)),
            dma((2, chunks)),
            dma((2, chunks, n // 2)),
            dma((reps, tps)),
            dma((reps, tps)),
            dma((reps, tps)),
            dma((reps, tps)),
            dma((reps, tps)),
            dma((reps, tps)),
            dma((blocks, reps)),
            dma((group, per_tp)),
            dma((blocks, reps)),
            dma((group, per_tp)),
        ],
        compiler_params=pltpu.CompilerParams(
            collective_id=0, has_side_effects=True, vmem_limit_bytes=62 * 1024 * 1024
        ),
    )(
        states, mix_gain[None, :], w_value, w_gate, conv_kernel, chan_gain[None, :], w_mix,
        mlp_gain[None, :], w_up, w_down,
    )


def plane_kernel(
    sizes,
    states, mix_gain, w_value, w_gate, conv_kernel, chan_gain, w_mix, mlp_gain, w_up, w_down,
    out,
    weights, rows_in, rows_mid, normed, padded, filtered, activated, hidden, own_in, own_mid,
    own_stats, peer_stats, mix_parts, stage, mix_peers, fed_parts, fed_peers,
    load_sems, y_send, y_recv, near_send, far_send, line_recv, last_recv,
    twin_send, twin_recv, last_twin,
    in_send, in_recv, mid_send, mid_recv,
    stat_send, stat_recv, stage_send, stage_recv, mix_send, mix_recv, fed_send, fed_recv,
):
    reps, n, tps, rows, channels, sub, ups = sizes
    ys = tps
    zs = n // ys
    members = reps * ys
    width = sub * tps
    own_width = sub * members
    shard = channels // n
    plane_shard = shard * ys
    tokens = reps * rows
    seqs = rows // LENGTH
    chunks = 3 + 2 * ups
    rep, fs, tp = lax.axis_index("rep"), lax.axis_index("fs"), lax.axis_index("tp")
    z, y = fs // ys, lax.rem(fs, ys)
    other_rep, other_y, other_tp = reps - 1 - rep, ys - 1 - y, tps - 1 - tp
    other_fs = z * ys + other_y
    own_group = rep * ys + y
    taps = conv_kernel.shape[0]
    blocks, _, block = mix_parts.shape
    per_tp = own_width // block

    third = tuple(range(3, 3 + ups))
    is_home = tp == y
    not_home = jnp.logical_not(is_home)
    fourth = tuple(range(3 + ups, chunks))
    per_plane = plane_shard // block
    has_next = (z < zs - 1, z > 0)
    next_fs = (fs + ys, fs - ys)
    def scoped(name):
        def wrap(f):
            def run(*args):
                with jax.named_scope("_".join([name, *(str(a) for a in args[:2] if isinstance(a, int))])):
                    return f(*args)
            return run
        return wrap

    barrier = pltpu.get_barrier_semaphore()
    for dr in range(reps):
        for dy in range(ys):
            for dt in range(tps):
                if dr or dy or dt:
                    pl.semaphore_signal(
                        barrier, inc=1,
                        device_id={
                            "rep": lax.rem(rep + dr, reps),
                            "fs": z * ys + lax.rem(y + dy, ys),
                            "tp": lax.rem(tp + dt, tps),
                        },
                        device_id_type=MESH,
                    )
    for way in range(2):
        @pl.when(has_next[way])
        def _():
            pl.semaphore_signal(
                barrier, inc=1, device_id={"fs": next_fs[way]}, device_id_type=MESH
            )

    def remote(src, dst, send, recv, **where):
        return pltpu.make_async_remote_copy(
            src_ref=src, dst_ref=dst, send_sem=send, recv_sem=recv,
            device_id=where, device_id_type=MESH,
        )

    def rows_of(index, size=shard):
        return pl.ds(pl.multiple_of(index * size, size), size)

    def rep_rows(r):
        return pl.ds(pl.multiple_of(r * rows, rows), rows)

    half = pl.ds(pl.multiple_of(tp * sub, sub), sub)

    def columns_of(c, group):
        if c < 3:
            source, at = (w_value, w_gate, w_mix)[c], group
        elif c < 3 + ups:
            source, at = w_up, group * ups + c - 3
        else:
            source, at = w_down, group * ups + c - 3 - ups
        return source.at[:, pl.ds(pl.multiple_of(at * sub, sub), sub)]

    loads = [
        pltpu.make_async_copy(
            columns_of(c, own_group), weights.at[c, rows_of(fs), half], load_sems.at[min(c, 3)]
        )
        for c in range(chunks)
    ]
    home_cols = pl.ds(pl.multiple_of(tp * own_width, own_width), own_width)
    own_load = pltpu.make_async_copy(states, own_in, load_sems.at[4])
    home_load = pltpu.make_async_copy(
        states, rows_in.at[rep_rows(rep), home_cols], load_sems.at[5]
    )
    for c in range(chunks):
        loads[c].start()
    pl.when(is_home)(home_load.start)
    own_load.start()
    along_line = sum(jnp.where(has, 1, 0) for has in has_next)
    pl.semaphore_wait(barrier, reps * ys * tps - 1 + along_line)

    def across(c):
        return remote(
            columns_of(c, rep * ys + other_y), weights.at[c, rows_of(fs), half],
            y_send.at[0], y_recv.at[c], fs=other_fs,
        )

    middle = jnp.minimum(z, zs - 1 - z)

    def offset_at(i):
        low = 2 * z < zs - 1
        near = -(i + 1) // 2 if i % 2 else i // 2
        near = jnp.where(low, near, -near)
        far = jnp.where(low, i - middle, middle - i)
        return jnp.where(i <= 2 * middle, near, far)

    offsets = [offset_at(i) for i in range(zs)]
    planes = [z + off for off in offsets]

    def moved(chunk, span, send, recv, **where):
        at = weights.at[chunk, span, half]
        return remote(at, at, send, recv, **where)

    def group_of(c):
        return slice(0, 2) if c < 2 else c if c == 2 else slice(3, 3 + ups)

    def twin(c, i):
        return moved(
            c, rows_of(planes[i], plane_shard), twin_send.at[c], twin_recv.at[0 if c < 2 else min(c - 1, 2)],
            tp=other_tp,
        )

    def twin_last(c, i, b):
        return moved(
            c, rows_of(planes[i] * ys + b), twin_send.at[c], last_twin.at[i, b], tp=other_tp
        )

    def ready(c):
        group = group_of(c)
        whole_half = weights.at[group, :, half]
        remote(
            whole_half, whole_half, twin_send.at[c], twin_recv.at[0 if c < 2 else min(c - 1, 2)], tp=other_tp
        ).wait_recv()

    def ready_last(i, b):
        moved(
            slice(3 + ups, chunks), rows_of(planes[i] * ys + b), twin_send.at[0],
            last_twin.at[i, b], tp=other_tp,
        ).wait_recv()

    def near(c, way, part):
        recv = last_recv.at[z, part] if c in fourth else line_recv.at[c, z]
        return moved(c, rows_of(z * ys + part), near_send.at[way], recv, fs=next_fs[way])

    @scoped("begin")
    def begin(c):
        if c < 3:
            loads[c].wait()
        elif c == 3:
            at = weights.at[3:, rows_of(fs), half]
            pltpu.make_async_copy(at, at, load_sems.at[3]).wait()
        for way in range(2):
            pl.when(has_next[way])(near(c, way, y).start)

    @scoped("own")
    def own(c):
        across(c).wait_recv()
        for way in range(2):
            pl.when(has_next[way])(near(c, way, other_y).start)
        if c in fourth:
            for b in range(ys):
                twin_last(c, 0, b).start()
        else:
            twin(c, 0).start()

    goes = [jnp.where(off < 0, z < zs - 1, z > 0) for off in offsets]

    def onward(chunk, i, span, recv):
        to = jnp.where(offsets[i] < 0, fs + ys, fs - ys)
        return moved(chunk, span, far_send.at[i - 1], recv, fs=to)

    @scoped("arrive")
    def arrive(c, i):
        copy = onward(c, i, rows_of(planes[i], plane_shard), line_recv.at[c, planes[i]])
        copy.wait_recv()
        pl.when(goes[i])(copy.start)
        twin(c, i).start()

    @scoped("arrive_last")
    def arrive_last(i, b):
        span, recv = rows_of(planes[i] * ys + b), last_recv.at[planes[i], b]
        copy = onward(slice(3 + ups, chunks), i, span, recv)
        copy.wait_recv()
        for c in fourth:
            pl.when(goes[i])(onward(c, i, span, recv).start)
        for c in fourth:
            twin_last(c, i, b).start()

    @scoped("drain")
    def drain(chunk):
        moved(chunk, slice(None), twin_send.at[chunk], twin_recv.at[0], tp=other_tp).wait_send()

    @scoped("drain_all")
    def drain_all():
        every = slice(None)
        moved(every, rows_of(fs), y_send.at[0], y_recv.at[0], fs=other_fs).wait_send()
        for way in range(2):
            copy = moved(
                every, rows_of(z, plane_shard), near_send.at[way], y_recv.at[0], fs=next_fs[way]
            )
            pl.when(has_next[way])(copy.wait_send)
        for i in range(1, zs):
            copy = onward(every, i, rows_of(planes[i], plane_shard), y_recv.at[0])
            pl.when(goes[i])(copy.wait_send)

    def spread(source, target, send, recv, over_from):
        def at(r, h, j):
            start = pl.multiple_of(h * own_width + j * block, block)
            return target.at[rep_rows(r), pl.ds(start, block)]

        def copies(j):
            if isinstance(j, slice):
                src, dst, j = source, target.at[rep_rows(rep), home_cols], 0
            else:
                src, dst = source.at[:, j * block : (j + 1) * block], at(rep, tp, j)
            along = remote(src, dst, send.at[0], recv.at[1, tp, j], rep=other_rep, tp=y)
            over = remote(src, dst, send.at[1], recv.at[0, tp, j], fs=other_fs, tp=y)
            inside = remote(src, dst, send.at[2], recv.at[0, tp, j], tp=y)
            return along, over, inside

        def passing(h, j):
            if h == 0 and j >= over_from:
                one = at(other_rep, 0, j)
                return remote(one, one, send.at[3], recv.at[1, 0, j], fs=other_fs)
            two = at(rep, h, j)
            return remote(two, two, send.at[3 + h], recv.at[1, h, j], rep=other_rep)

        def arrival(dr, h, j):
            dst = at(rep if dr == 0 else other_rep, h, j)
            return remote(dst, dst, send.at[0], recv.at[dr, h, j], rep=other_rep)

        def start(j):
            along, over, inside = copies(j)
            along.start()
            over.start()
            pl.when(jnp.logical_not(is_home))(inside.start)

        @scoped("forward")
        def forward(j):
            if j >= over_from:
                @pl.when(is_home)
                def _():
                    arrival(1, 0, j).wait_recv()
                    passing(0, j).start()

            @pl.when(jnp.logical_not(is_home))
            def _():
                for h in range(tps):
                    if h or j < over_from:
                        arrival(0, h, j).wait_recv()
                        passing(h, j).start()

        @scoped("finish")
        def finish(j):
            arrival(1, 1, j).wait_recv()

            @pl.when(is_home)
            def _():
                arrival(0, other_tp, j).wait_recv()
                if j < over_from:
                    arrival(1, 0, j).wait_recv()

            @pl.when(jnp.logical_not(is_home))
            def _():
                arrival(1, 0, j).wait_recv()
                if j >= over_from:
                    arrival(0, 0, j).wait_recv()

        def settle():
            along, over, inside = copies(slice(None))
            along.wait_send()
            over.wait_send()
            pl.when(not_home)(inside.wait_send)

            def part(k, blocks_sent):
                if blocks_sent:
                    sent = target.at[rep_rows(rep), : blocks_sent * block]
                    remote(sent, sent, send.at[k], recv.at[0, 0, 0], fs=other_fs).wait_send()

            pl.when(is_home)(functools.partial(part, 3, per_tp - over_from))

            @pl.when(not_home)
            def _():
                part(3, over_from)
                part(4, per_tp)

        return start, forward, finish, settle

    @scoped("norm")
    def norm_all(source, gain):
        def one(i, carry):
            span = pl.ds(pl.multiple_of(i * 64, 64), 64)
            x = source[span, :].astype(jnp.float32)
            scale = lax.rsqrt(jnp.mean(x * x, axis=-1, keepdims=True) + EPS)
            normed[span, :] = (x * scale * gain[...]).astype(jnp.bfloat16)
            return carry

        lax.fori_loop(0, tokens // 64, one, 0)

    def seq_rows(i):
        return pl.ds(pl.multiple_of(i * LENGTH, LENGTH), LENGTH)

    def mixer_rows(i):
        x = normed[seq_rows(i), :]
        value = jnp.dot(x, weights[0], preferred_element_type=jnp.float32)
        gate = jnp.dot(x, weights[1], preferred_element_type=jnp.float32)
        padded[LEAD : LEAD + LENGTH, :] = value * jax.nn.sigmoid(gate)
        per_sub = sub // LANES

        def column(j, sums):
            cols = pl.ds(pl.multiple_of(j * LANES, LANES), LANES)
            from_all = pl.multiple_of(
                (j // per_sub) * own_width + own_group * sub + lax.rem(j, per_sub) * LANES, LANES
            )
            kern = conv_kernel[:, pl.ds(from_all, LANES)]
            total = jnp.zeros((LENGTH, LANES), jnp.float32)
            for tap in range(taps):
                begin = LEAD - (taps - 1) + tap
                total = total + kern[tap : tap + 1, :] * padded[begin : begin + LENGTH, cols]
            filtered[seq_rows(i), cols] = total
            return sums[0] + total, sums[1] + total * total

        zero = jnp.zeros((LENGTH, LANES), jnp.float32)
        one, two = lax.fori_loop(0, width // LANES, column, (zero, zero))
        lane = lax.broadcasted_iota(jnp.int32, (LENGTH, LANES), 1)
        both = jnp.where(
            lane == 0,
            jnp.sum(one, axis=-1, keepdims=True),
            jnp.where(lane == 1, jnp.sum(two, axis=-1, keepdims=True), 0.0),
        )
        own_stats[i // seqs, :, seq_rows(lax.rem(i, seqs))] = both.T[0:8, :]

    def stat_copies(r):
        return [
            remote(
                own_stats.at[r], peer_stats.at[dr * ys + dy, r], stat_send.at[r],
                stat_recv.at[r],
                rep=lax.rem(rep + dr, reps), fs=z * ys + lax.rem(y + dy, ys),
            )
            for dr in range(reps) for dy in range(ys) if dr or dy
        ]

    def stat_waits(r):
        at = peer_stats.at[1:, r]
        return remote(at, at, stat_send.at[r], stat_recv.at[r], rep=other_rep)

    def activate_rows(i, carry):
        within = seq_rows(lax.rem(i, seqs))
        total = own_stats[i // seqs, :, within]
        for k in range(1, members):
            total = total + peer_stats[k, i // seqs, :, within]
        turned = jnp.concatenate([total] * (LANES // 8), axis=0).T
        mean = turned[:, 0:1] / channels
        variance = turned[:, 1:2] / channels - mean * mean
        gain = jnp.concatenate(
            [
                chan_gain[:, pl.ds(pl.multiple_of(t * own_width + own_group * sub, sub), sub)]
                for t in range(tps)
            ],
            axis=1,
        )
        x = (filtered[seq_rows(i), :] - mean) * lax.rsqrt(variance + EPS) * gain
        activated[seq_rows(i), :] = (x / (1.0 + jnp.exp(-x))).astype(jnp.bfloat16)
        return carry

    @scoped("share")
    def share(o, dr, left, pieces_of, parts, peers, send, recv):
        to = lax.rem(rep + dr, reps)
        span = rows_of(o, block)
        keeper, kept = o // per_tp, lax.rem(o, per_tp)
        at = rep_rows(to)
        total = None
        for k, c in enumerate(pieces_of):
            term = times_transposed(left[at, k * width : (k + 1) * width], weights[c, span, :])
            total = term if total is None else total + term
        parts[o, at, :] = total.astype(jnp.bfloat16)
        slot = lax.rem(rep + reps - to, reps) * ys + lax.rem(y + ys - tp, ys)
        copy = remote(
            parts.at[o, at, :], peers.at[slot, kept], send.at[dr], recv.at[kept],
            rep=to, fs=z * ys + tp, tp=keeper,
        )
        here = jnp.logical_and(is_home, jnp.logical_and(keeper == tp, to == rep))
        pl.when(jnp.logical_not(here))(copy.start)

    def along_first(o):
        return o % 2 == 0

    def stage_copy(o, r):
        if along_first(o):
            return remote(
                mix_parts.at[o, rep_rows(other_rep), :], stage.at[o, 0], stage_send.at[0],
                stage_recv.at[o], rep=other_rep,
            )
        return remote(
            mix_parts.at[o, rep_rows(r), :], stage.at[o, r], stage_send.at[1],
            stage_recv.at[o], fs=z * ys + tp,
        )

    def last_copies(o):
        keeper, kept = o // per_tp, o % per_tp
        own_part = mix_parts.at[o, rep_rows(rep), :]
        inside = remote(
            own_part, mix_peers.at[0, kept], mix_send.at[0], mix_recv.at[kept], tp=keeper
        )
        if along_first(o):
            outside = remote(
                own_part, mix_peers.at[1, kept], mix_send.at[1], mix_recv.at[kept],
                fs=z * ys + tp, tp=keeper,
            )
        else:
            outside = remote(
                mix_parts.at[o, rep_rows(other_rep), :], mix_peers.at[1, kept],
                mix_send.at[1], mix_recv.at[kept], rep=other_rep, tp=keeper,
            )
        inner_one = jnp.logical_and(is_home, tp != keeper)
        return inside, inner_one, outside, not_home if along_first(o) else is_home

    @scoped("mix_share")
    def mix_share(o, r):
        at = rep_rows(r)
        mix_parts[o, at, :] = times_transposed(
            activated[at, :], weights[2, o * block : (o + 1) * block, :]
        ).astype(jnp.bfloat16)
        pl.when(rep != r if along_first(o) else not_home)(stage_copy(o, r).start)

    def mix_add(o, at, k):
        total = mix_parts[o, at, :].astype(jnp.float32) + stage[o, k].astype(jnp.float32)
        mix_parts[o, at, :] = total.astype(jnp.bfloat16)

    @scoped("combine")
    def combine(o):
        keeper, kept = o // per_tp, o % per_tp
        inside, inner_one, outside, outer_one = last_copies(o)

        def pass_on():
            pl.when(outer_one)(outside.start)
            pl.when(inner_one)(inside.start)

            @pl.when(jnp.logical_and(is_home, tp == keeper))
            def _():
                mix_peers[0, kept] = mix_parts[o, rep_rows(rep), :]

        if along_first(o):
            stage_copy(o, 0).wait_recv()
            mix_add(o, rep_rows(rep), 0)
            pass_on()
        else:
            @pl.when(is_home)
            def _():
                both = stage.at[o]
                remote(both, both, stage_send.at[1], stage_recv.at[o], fs=other_fs).wait_recv()
                for r in range(reps):
                    mix_add(o, rep_rows(r), r)
                pass_on()

    @scoped("mix_final")
    def mix_final(j):
        def some(start):
            at = mix_peers.at[start:, j]
            return remote(at, at, mix_send.at[0], mix_recv.at[j], rep=other_rep)

        pl.when(is_home)(some(1).wait_recv)
        pl.when(not_home)(some(0).wait_recv)
        return mix_peers[0, j].astype(jnp.float32) + mix_peers[1, j].astype(jnp.float32)

    def mix_settle():
        def sent(count, send):
            at = mix_parts.at[:count, rep_rows(rep), :]
            return remote(at, at, send, mix_recv.at[0], rep=other_rep)

        even = sum(1 for o in range(blocks) if along_first(o))
        sent(even, stage_send.at[0]).wait_send()
        pl.when(not_home)(sent((blocks - even) * reps, stage_send.at[1]).wait_send)
        pl.when(is_home)(sent(per_tp, mix_send.at[0]).wait_send)
        pl.when(not_home)(sent(even, mix_send.at[1]).wait_send)
        pl.when(is_home)(sent(blocks - even, mix_send.at[1]).wait_send)

    @scoped("peers")
    def wait_peers(j, parts, peers, send, recv):
        def some(start):
            at = peers.at[start:, j]
            return remote(at, at, send.at[0], recv.at[j], rep=other_rep)

        @pl.when(is_home)
        def _():
            peers[0, j] = parts[tp * per_tp + j, rep_rows(rep), :]
            some(1).wait_recv()

        pl.when(not_home)(some(0).wait_recv)

    def settle_share(parts, send, recv):
        for dr in range(reps):
            for count, who in ((per_tp, is_home), (blocks, not_home)):
                sent = parts.at[: count if dr == 0 else blocks, rep_rows(rep), :]
                copy = remote(sent, sent, send.at[dr], recv.at[0], rep=other_rep)
                pl.when(who)(copy.wait_send)

    def total_of(j, peers):
        total = peers[0, j].astype(jnp.float32)
        for k in range(1, members):
            total = total + peers[k, j].astype(jnp.float32)
        return total

    start_in, forward_in, finish_in, settle_in = spread(
        states, rows_in, in_send, in_recv, per_tp // 2
    )
    start_mid, forward_mid, finish_mid, settle_mid = spread(
        own_mid, rows_mid, mid_send, mid_recv, 0
    )

    def inner(*todo):
        @pl.when(middle > 0)
        def _():
            for one in todo:
                one()

    def outer(*todo):
        @pl.when(middle == 0)
        def _():
            for one in todo:
                one()

    def pump(c, i):
        return functools.partial(arrive, c, i)

    def all_of(c):
        return [pump(c, i) for i in range(1, zs)]

    def whole(c):
        return [functools.partial(begin, c), functools.partial(own, c)]

    across(0).start()
    across(1).start()
    begin(0)
    begin(1)
    for j in range(per_tp):
        start_in(j)
    own(0)
    own(1)
    across(2).start()
    across(3).start()
    padded[0:LEAD, :] = jnp.zeros((LEAD, width), jnp.float32)
    arrive(0, 1)
    arrive(1, 1)
    forward_in(0)
    inner(pump(0, 2), pump(1, 2))
    for j in range(1, per_tp // 2):
        forward_in(j)
    inner(*[pump(c, i) for i in range(3, zs) for c in (0, 1)])
    for j in range(per_tp // 2, per_tp):
        forward_in(j)
    begin(2)
    own(2)
    outer(*[pump(c, 2) for c in (0, 1)])
    for j in range(per_tp):
        finish_in(j)
    for c in range(4, chunks):
        across(c).start()
    pl.when(is_home)(home_load.wait)
    norm_all(rows_in, mix_gain)
    outer(*[pump(c, i) for i in range(3, zs) for c in (0, 1)])
    ready(0)

    inner(*all_of(2)[:1])
    outer(*whole(3))
    inside = [
        all_of(2)[1:2], whole(3), all_of(2)[2:], whole(4),
    ]
    outside = [whole(4), whole(5), whole(fourth[0]), sum([whole(c) for c in fourth[1:]], [])]
    for r in range(reps):
        for cut in ((0, (seqs + 1) // 2), ((seqs + 1) // 2, seqs)):
            with jax.named_scope("mixer"):
                lax.fori_loop(
                    r * seqs + cut[0], r * seqs + cut[1],
                    lambda k, carry: (mixer_rows(k), carry)[1], 0,
                )
            if inside:
                inner(*inside.pop(0))
                outer(*outside.pop(0))
        for one in stat_copies(r):
            one.start()
    outer(*all_of(2))
    ready(2)
    for r in range(reps):
        with jax.named_scope("stats"):
            stat_waits(r).wait_recv()
        with jax.named_scope("activate"):
            lax.fori_loop(r * seqs, (r + 1) * seqs, activate_rows, 0)
        for j in range(per_tp):
            for t in range(tps):
                mix_share(t * per_tp + j, r)

    own_load.wait()
    inner(*whole(5), *all_of(3)[:2])
    def last(i, b):
        return [functools.partial(arrive_last, i, b)]

    early = [
        all_of(3)[2:] + all_of(4)[:2],
        all_of(4)[2:] + all_of(5)[:2] + whole(fourth[0]),
        all_of(5)[2:] + sum([whole(c) for c in fourth[1:]], []),
    ]
    late = [[], all_of(3), all_of(4)[:1], all_of(4)[1:]]
    for t in range(tps):
        combine(t * per_tp)
    for j in range(per_tp):
        if j + 1 < per_tp:
            for t in range(tps):
                combine(t * per_tp + j + 1)
        mixed = mix_final(j)
        cols = slice(j * block, (j + 1) * block)
        own_mid[:, cols] = (own_in[:, cols].astype(jnp.float32) + mixed).astype(jnp.bfloat16)
        start_mid(j)

        @pl.when(is_home)
        def _():
            start = pl.multiple_of(tp * own_width + j * block, block)
            rows_mid[rep_rows(rep), pl.ds(start, block)] = own_mid[:, cols]

        if j:
            forward_mid(j - 1)
        if j < len(early):
            inner(*early[j])
        if j == per_tp - 1:
            forward_mid(j)
            inner(*[one for b in range(ys) for one in last(1, b)])
        if j < len(late):
            outer(*late[j])
    for rest in early[per_tp:]:
        inner(*rest)
    for rest in late[per_tp:]:
        outer(*rest)
    for j in range(per_tp):
        finish_mid(j)
    outer(*all_of(5))
    norm_all(rows_mid, mlp_gain)
    ready(3)

    @scoped("up")
    def up_some(k):
        def up_rows(i, carry):
            at = rep_rows(i)
            x = jnp.dot(normed[at, :], weights[3 + k], preferred_element_type=jnp.float32)
            x = jnp.maximum(x, 0.0)
            hidden[at, k * width : (k + 1) * width] = (x * x).astype(jnp.bfloat16)
            return carry

        lax.fori_loop(0, reps, up_rows, 0)

    for k in range(ups):
        up_some(k)
    fed = (hidden, fourth, fed_parts, fed_peers, fed_send, fed_recv)
    settle_in()
    settle_mid()
    mix_settle()
    for r in range(reps):
        stat_waits(r).wait_send()
    for i in range(zs):
        for b in range(ys):
            if i:
                outer(*last(i, b))
            if 1 < i + 1 < zs:
                inner(*last(i + 1, b))
            ready_last(i, b)
            for dr in (*range(1, reps), 0):
                share(planes[i] * ys + b, dr, *fed)
            if i == 1 and b == 0:
                for c in range(3 + ups):
                    drain(c)
    for j in range(per_tp):
        if j == per_tp - 1:
            for c in fourth:
                drain(c)
            drain_all()
        wait_peers(j, fed_parts, fed_peers, fed_send, fed_recv)
        cols = slice(j * block, (j + 1) * block)
        with jax.named_scope("out"):
            out[:, cols] = (
                own_mid[:, cols].astype(jnp.float32) + total_of(j, fed_peers)
            ).astype(jnp.bfloat16)
    with jax.named_scope("done"):
        settle_share(fed_parts, fed_send, fed_recv)


def plane_body(mesh, states, mix_gain, w_value, w_gate, conv_kernel, chan_gain, w_mix, mlp_gain, w_up, w_down):
    reps, n, tps = mesh.shape["rep"], mesh.shape["fs"], mesh.shape["tp"]
    rows, own_width = states.shape
    ys = tps
    zs, members = n // ys, reps * ys
    sub = own_width // members
    width = sub * tps
    channels = own_width * tps
    ups = w_up.shape[1] // own_width
    tokens = rows * reps
    block = channels // n
    blocks, per_tp = channels // block, own_width // block
    chunks = 3 + 2 * ups
    bf16, f32 = jnp.bfloat16, jnp.float32
    vmem, hbm = pl.BlockSpec(memory_space=pltpu.VMEM), pl.BlockSpec(memory_space=pl.ANY)
    dma = pltpu.SemaphoreType.DMA
    return pl.pallas_call(
        functools.partial(plane_kernel, (reps, n, tps, rows, channels, sub, ups)),
        out_shape=jax.ShapeDtypeStruct((rows, own_width), bf16),
        in_specs=[hbm, vmem, hbm, hbm, vmem, vmem, hbm, vmem, hbm, hbm],
        out_specs=vmem,
        scratch_shapes=[
            pltpu.VMEM((chunks, channels, width), bf16),
            pltpu.VMEM((tokens, channels), bf16),
            pltpu.VMEM((tokens, channels), bf16),
            pltpu.VMEM((tokens, channels), bf16),
            pltpu.VMEM((LEAD + LENGTH, width), f32),
            pltpu.VMEM((tokens, width), f32),
            pltpu.VMEM((tokens, width), bf16),
            pltpu.VMEM((tokens, ups * width), bf16),
            pltpu.VMEM((rows, own_width), bf16),
            pltpu.VMEM((rows, own_width), bf16),
            pltpu.VMEM((reps, 8, rows), f32),
            pltpu.VMEM((members, reps, 8, rows), f32),
            pltpu.VMEM((blocks, tokens, block), bf16),
            pltpu.VMEM((blocks, reps, rows, block), bf16),
            pltpu.VMEM((2, per_tp, rows, block), bf16),
            pltpu.VMEM((blocks, tokens, block), bf16),
            pltpu.VMEM((members, per_tp, rows, block), bf16),
            dma((6,)),
            dma((1,)),
            dma((chunks,)),
            dma((2,)),
            dma((zs - 1,)),
            dma((3 + ups, zs)),
            dma((zs, ys)),
            dma((chunks,)),
            dma((3,)),
            dma((zs, ys)),
            dma((5,)),
            dma((reps, tps, per_tp)),
            dma((5,)),
            dma((reps, tps, per_tp)),
            dma((reps,)),
            dma((reps,)),
            dma((2,)),
            dma((blocks,)),
            dma((2,)),
            dma((per_tp,)),
            dma((reps,)),
            dma((per_tp,)),
        ],
        compiler_params=pltpu.CompilerParams(
            collective_id=0, has_side_effects=True, vmem_limit_bytes=62 * 1024 * 1024
        ),
    )(
        states, mix_gain[None, :], w_value, w_gate, conv_kernel, chan_gain[None, :], w_mix,
        mlp_gain[None, :], w_up, w_down,
    )


def body(mesh, states, *weights):
    reps, n, tps = mesh.shape["rep"], mesh.shape["fs"], mesh.shape["tp"]
    own_width = states.shape[1]
    channels = own_width * tps
    planar = (
        reps == tps == 2
        and n % tps == 0
        and n // tps > 2
        and own_width % (reps * tps * LANES) == 0
        and channels % (n * LANES) == 0
        and own_width % (channels // n) == 0
    )
    return (plane_body if planar else ring_body)(mesh, states, *weights)


def solution(mesh):
    in_specs = (
        P(("rep", "fs"), "tp"),
        P(),
        P("fs", "tp"),
        P("fs", "tp"),
        P(),
        P(),
        P("fs", "tp"),
        P(),
        P("fs", "tp"),
        P("fs", "tp"),
    )
    out_specs = P(("rep", "fs"), "tp")
    return jax.shard_map(
        functools.partial(body, mesh),
        mesh=mesh, in_specs=in_specs, out_specs=out_specs, check_vma=False,
    )
```

```python
import functools

import jax
import jax.numpy as jnp
from jax import lax
from jax.experimental import pallas as pl
from jax.experimental.pallas import tpu as pltpu
from jax.sharding import PartitionSpec as P

LENGTH = 128
LANES = 128
LEAD = 32
EPS = 1e-06
MESH = pl.DeviceIdType.MESH


def times_transposed(left, right):
    return lax.dot_general(
        left, right, (((1,), (1,)), ((), ())), preferred_element_type=jnp.float32
    )


def ring_kernel(
    sizes,
    states, mix_gain, w_value, w_gate, conv_kernel, chan_gain, w_mix, mlp_gain, w_up, w_down,
    out,
    weights, rows_in, rows_mid, normed, padded, filtered, activated, hidden,
    own_stats, peer_stats, mix_parts, mix_peers, fed_parts, fed_peers,
    load_sems, ring_send, ring_recv, in_send, in_recv, mid_send, mid_recv,
    stat_send, stat_recv, mix_send, mix_recv, fed_send, fed_recv,
):
    reps, n, tps, rows, channels, width, ups = sizes
    own_width = width * reps
    half_way = n // 2
    shard = channels // n
    tokens = reps * rows
    pieces = tokens // LENGTH
    chunks = 3 + 2 * ups
    rep, fs, tp = lax.axis_index("rep"), lax.axis_index("fs"), lax.axis_index("tp")
    taps = conv_kernel.shape[0]
    blocks, _, block = mix_parts.shape
    per_tp = own_width // block

    def ring_index(place):
        place = lax.rem(place + n, n)
        return jnp.where(place < half_way, 2 * place, 2 * (n - 1 - place) + 1)

    place = jnp.where(lax.rem(fs, 2) == 0, fs // 2, n - 1 - fs // 2)
    neighbours = (ring_index(place + 1), ring_index(place - 1))

    barrier = pltpu.get_barrier_semaphore()
    for other in neighbours:
        pl.semaphore_signal(barrier, inc=1, device_id={"fs": other}, device_id_type=MESH)
    for dr in range(reps):
        for dt in range(tps):
            if dr or dt:
                pl.semaphore_signal(
                    barrier, inc=1,
                    device_id={"rep": lax.rem(rep + dr, reps), "tp": lax.rem(tp + dt, tps)},
                    device_id_type=MESH,
                )

    own_rows = pl.ds(pl.multiple_of(rep * rows, rows), rows)
    own_cols = pl.ds(pl.multiple_of(tp * own_width, own_width), own_width)

    def shard_at(owner, start=0, size=None):
        size = shard if size is None else size
        return pl.ds(pl.multiple_of(owner * shard + start, size), size)

    def hop(c, s, way):
        sign = 1 if way == 0 else -1
        owner = ring_index(place - sign * (s - 1))
        span = shard_at(owner)
        if s == half_way:
            span = shard_at(owner, way * (shard // 2), shard // 2)
        return pltpu.make_async_remote_copy(
            src_ref=weights.at[c, span, :],
            dst_ref=weights.at[c, span, :],
            send_sem=ring_send.at[way, c],
            recv_sem=ring_recv.at[way, c, s - 1],
            device_id={"fs": neighbours[way]},
            device_id_type=MESH,
        )

    loads = []
    for c in range(chunks):
        if c < 3:
            source, column = (w_value, w_gate, w_mix)[c], rep * width
        elif c < 3 + ups:
            source, column = w_up, (rep * ups + c - 3) * width
        else:
            source, column = w_down, (rep * ups + c - 3 - ups) * width
        loads.append(
            pltpu.make_async_copy(
                source.at[:, pl.ds(pl.multiple_of(column, width), width)],
                weights.at[c, shard_at(fs), :],
                load_sems.at[c],
            )
        )
        loads[-1].start()
    own_load = pltpu.make_async_copy(states, rows_in.at[own_rows, own_cols], load_sems.at[chunks])
    own_load.start()
    pl.semaphore_wait(barrier, 1 + reps * tps)

    def pump(c, s):
        for way in range(2):
            if s == 1:
                if way == 0:
                    loads[c].wait()
            else:
                before = hop(c, s - 1, way)
                before.wait_recv()
                before.wait_send()
            hop(c, s, way).start()

    def arrived(c):
        for way in range(2):
            last = hop(c, half_way, way)
            last.wait_recv()
            last.wait_send()

    def spread(source, target, send, recv):
        def copy(dr, dt, ahead):
            if ahead:
                span = pl.ds(pl.multiple_of(lax.rem(rep + reps - dr, reps) * rows, rows), rows)
                src = target.at[span, own_cols]
            else:
                span, src = own_rows, source
            step_r = 0 if ahead else dr
            return pltpu.make_async_remote_copy(
                src_ref=src,
                dst_ref=target.at[span, own_cols],
                send_sem=send.at[dr, dt],
                recv_sem=recv.at[dr, dt],
                device_id={"rep": lax.rem(rep + step_r, reps), "tp": lax.rem(tp + dt, tps)},
                device_id_type=MESH,
            )

        first = [copy(dr, 0, False) for dr in range(1, reps)]
        near = [copy(0, dt, False) for dt in range(1, tps)]
        for one in first + near:
            one.start()

        def forward():
            later = []
            for dr in range(1, reps):
                first[dr - 1].wait_recv()
                for dt in range(1, tps):
                    one = copy(dr, dt, True)
                    one.start()
                    later.append(one)
            return later

        def finish(later):
            for one in near + later:
                one.wait_recv()
            for one in first + near + later:
                one.wait_send()

        return forward, finish

    def norm_all(source, gain):
        def one(i, carry):
            span = pl.ds(pl.multiple_of(i * 64, 64), 64)
            x = source[span, :].astype(jnp.float32)
            scale = lax.rsqrt(jnp.mean(x * x, axis=-1, keepdims=True) + EPS)
            normed[span, :] = (x * scale * gain[...]).astype(jnp.bfloat16)
            return carry

        lax.fori_loop(0, tokens // 64, one, 0)

    def seq_rows(i):
        return pl.ds(pl.multiple_of(i * LENGTH, LENGTH), LENGTH)

    def mixer_rows(i):
        x = normed[seq_rows(i), :]
        value = jnp.dot(x, weights[0], preferred_element_type=jnp.float32)
        gate = jnp.dot(x, weights[1], preferred_element_type=jnp.float32)
        padded[LEAD : LEAD + LENGTH, :] = value * jax.nn.sigmoid(gate)

        def column(j, sums):
            cols = pl.ds(pl.multiple_of(j * LANES, LANES), LANES)
            from_all = pl.multiple_of(tp * own_width + rep * width + j * LANES, LANES)
            kern = conv_kernel[:, pl.ds(from_all, LANES)]
            total = jnp.zeros((LENGTH, LANES), jnp.float32)
            for tap in range(taps):
                begin = LEAD - (taps - 1) + tap
                total = total + kern[tap : tap + 1, :] * padded[begin : begin + LENGTH, cols]
            filtered[seq_rows(i), cols] = total
            return sums[0] + total, sums[1] + total * total

        zero = jnp.zeros((LENGTH, LANES), jnp.float32)
        one, two = lax.fori_loop(0, width // LANES, column, (zero, zero))
        lane = lax.broadcasted_iota(jnp.int32, (LENGTH, LANES), 1)
        both = jnp.where(
            lane == 0,
            jnp.sum(one, axis=-1, keepdims=True),
            jnp.where(lane == 1, jnp.sum(two, axis=-1, keepdims=True), 0.0),
        )
        own_stats[:, seq_rows(i)] = both.T[0:8, :]

    def stat_copies():
        copies = []
        for dr in range(reps):
            for dt in range(tps):
                if dr or dt:
                    copies.append(
                        pltpu.make_async_remote_copy(
                            src_ref=own_stats,
                            dst_ref=peer_stats.at[dr * tps + dt],
                            send_sem=stat_send.at[dr, dt],
                            recv_sem=stat_recv.at[dr, dt],
                            device_id={
                                "rep": lax.rem(rep + dr, reps),
                                "tp": lax.rem(tp + dt, tps),
                            },
                            device_id_type=MESH,
                        )
                    )
        return copies

    def activate_rows(i, carry):
        total = own_stats[:, seq_rows(i)]
        for k in range(1, reps * tps):
            total = total + peer_stats[k, :, seq_rows(i)]
        turned = jnp.concatenate([total] * (LANES // 8), axis=0).T
        mean = turned[:, 0:1] / channels
        variance = turned[:, 1:2] / channels - mean * mean
        gain_at = pl.multiple_of(tp * own_width + rep * width, LANES)
        gain = chan_gain[:, pl.ds(gain_at, width)]
        x = (filtered[seq_rows(i), :] - mean) * lax.rsqrt(variance + EPS) * gain
        activated[seq_rows(i), :] = (x / (1.0 + jnp.exp(-x))).astype(jnp.bfloat16)
        return carry

    def share(order, o, left, pieces_of, parts, peers, send, recv):
        span = pl.ds(pl.multiple_of(o * block, block), block)

        def one(i):
            at = pl.ds(pl.multiple_of(i * rows, rows), rows)
            total = None
            for k, c in enumerate(pieces_of):
                term = times_transposed(
                    left[at, k * width : (k + 1) * width], weights[c, span, :]
                )
                total = term if total is None else total + term
            parts[o, at, :] = total.astype(jnp.bfloat16)

        keeper = o // per_tp
        dt = lax.rem(keeper + tps - tp, tps)
        waits = []
        for dr in [*range(1, reps), 0]:
            to = lax.rem(rep + dr, reps)
            one(to)
            copy = pltpu.make_async_remote_copy(
                src_ref=parts.at[o, pl.ds(pl.multiple_of(to * rows, rows), rows), :],
                dst_ref=peers.at[dr * tps + dt, lax.rem(o, per_tp)],
                send_sem=send.at[order, dr],
                recv_sem=recv.at[dr * tps + dt, lax.rem(o, per_tp)],
                device_id={"rep": to, "tp": keeper},
                device_id_type=MESH,
            )
            if dr:
                copy.start()
                waits.append(copy.wait_send)
            else:
                pl.when(keeper != tp)(copy.start)
                waits.append(lambda k=keeper, c=copy: pl.when(k != tp)(c.wait_send))
        return waits

    def wait_peers(j, parts, peers, send, recv):
        for k in range(1, reps * tps):
            dr, dt = k // tps, k % tps
            pltpu.make_async_remote_copy(
                src_ref=parts.at[0, own_rows, :],
                dst_ref=peers.at[k, j],
                send_sem=send.at[0, 0],
                recv_sem=recv.at[k, j],
                device_id={"rep": lax.rem(rep + dr, reps), "tp": lax.rem(tp + dt, tps)},
                device_id_type=MESH,
            ).wait_recv()

    def total_of(j, parts, peers):
        total = parts[tp * per_tp + j, own_rows, :].astype(jnp.float32)
        for k in range(1, reps * tps):
            total = total + peers[k, j].astype(jnp.float32)
        return total

    stepwise = blocks == n

    def owners(s):
        if s in (0, half_way):
            return [ring_index(place + s)]
        return [ring_index(place - s), ring_index(place + s)]

    def steps_of(c):
        return range(1, half_way + 1)

    first, second = (0, 1), (2, 3)
    third = tuple(range(4, 3 + ups))
    fourth = tuple(range(3 + ups, chunks))

    pump(0, 1)
    pump(1, 1)
    forward, finish = spread(states, rows_in, in_send, in_recv)
    padded[0:LEAD, :] = jnp.zeros((LEAD, width), jnp.float32)
    pump(0, 2)
    pump(1, 2)
    later = forward()
    for s in range(3, half_way + 1):
        pump(0, s)
        if s == 3:
            own_load.wait()
            finish(later)
        pump(1, s)
        if s == 3:
            norm_all(rows_in, mix_gain)
    pump(2, 1)
    pump(3, 1)
    arrived(0)
    arrived(1)

    todo = [(c, s) for s in range(2, half_way + 1) for c in second]

    def next_hop():
        if todo:
            pump(*todo.pop(0))

    for i in range(0, pieces, 2):
        lax.fori_loop(
            i, min(i + 2, pieces), lambda k, carry: (mixer_rows(k), carry)[1], 0
        )
        next_hop()
    stats = stat_copies()
    for one in stats:
        one.start()
    for one in stats:
        one.wait_recv()
    lax.fori_loop(0, pieces, activate_rows, 0)
    waits = []
    mix = (activated, (2,), mix_parts, mix_peers, mix_send, mix_recv)
    if stepwise:
        for s in range(half_way - 1):
            for o in owners(s):
                waits += share(len(waits) // reps, o, *mix)
    while todo:
        next_hop()
    if stepwise:
        for o in owners(half_way - 1):
            waits += share(len(waits) // reps, o, *mix)
    for c in third:
        pump(c, 1)
    arrived(2)
    if stepwise:
        waits += share(len(waits) // reps, owners(half_way)[0], *mix)
    else:
        for o in range(blocks):
            waits += share(o, o, *mix)

    todo = [(c, s) for s in range(2, half_way + 1) for c in third]
    for _ in range(len(todo) // 2):
        next_hop()
    for j in range(per_tp):
        wait_peers(j, mix_parts, mix_peers, mix_send, mix_recv)
        at = pl.ds(pl.multiple_of(tp * own_width + j * block, block), block)
        rows_mid[own_rows, at] = (
            rows_in[own_rows, at].astype(jnp.float32) + total_of(j, mix_parts, mix_peers)
        ).astype(jnp.bfloat16)
    forward, finish = spread(rows_mid.at[own_rows, own_cols], rows_mid, mid_send, mid_recv)
    while todo:
        next_hop()
    for c in fourth:
        pump(c, 1)
    arrived(3)
    for c in third:
        arrived(c)
    later = forward()
    finish(later)
    norm_all(rows_mid, mlp_gain)
    todo = [(c, s) for s in range(2, half_way + 1) for c in fourth]
    next_hop()
    for k in range(ups):

        def up_rows(i, carry):
            at = pl.ds(pl.multiple_of(i * rows, rows), rows)
            x = jnp.dot(normed[at, :], weights[3 + k], preferred_element_type=jnp.float32)
            x = jnp.maximum(x, 0.0)
            hidden[at, k * width : (k + 1) * width] = (x * x).astype(jnp.bfloat16)
            return carry

        lax.fori_loop(0, reps, up_rows, 0)
        next_hop()
    done = []
    fed = (hidden, fourth, fed_parts, fed_peers, fed_send, fed_recv)
    if stepwise:
        for o in owners(0):
            done += share(len(done) // reps, o, *fed)
    for s in range(2, half_way + 1):
        while todo and todo[0][1] <= s:
            next_hop()
        if stepwise:
            for o in owners(s - 1):
                done += share(len(done) // reps, o, *fed)
    for c in fourth:
        arrived(c)
    if stepwise:
        done += share(len(done) // reps, owners(half_way)[0], *fed)
    else:
        for o in range(blocks):
            done += share(o, o, *fed)
    for j in range(per_tp):
        wait_peers(j, fed_parts, fed_peers, fed_send, fed_recv)
        at = pl.ds(pl.multiple_of(tp * own_width + j * block, block), block)
        out[:, j * block : (j + 1) * block] = (
            rows_mid[own_rows, at].astype(jnp.float32) + total_of(j, fed_parts, fed_peers)
        ).astype(jnp.bfloat16)
    for one in stats:
        one.wait_send()
    for wait in waits + done:
        wait()


def ring_body(mesh, states, mix_gain, w_value, w_gate, conv_kernel, chan_gain, w_mix, mlp_gain, w_up, w_down):
    reps, n, tps = mesh.shape["rep"], mesh.shape["fs"], mesh.shape["tp"]
    rows, own_width = states.shape
    width = own_width // reps
    channels = own_width * tps
    ups = w_up.shape[1] // own_width
    tokens = rows * reps
    group = reps * tps
    block = channels // n if channels // n >= LANES else own_width
    blocks, per_tp = channels // block, own_width // block
    chunks = 3 + 2 * ups
    bf16, f32 = jnp.bfloat16, jnp.float32
    vmem, hbm = pl.BlockSpec(memory_space=pltpu.VMEM), pl.BlockSpec(memory_space=pl.ANY)
    dma = pltpu.SemaphoreType.DMA
    return pl.pallas_call(
        functools.partial(ring_kernel, (reps, n, tps, rows, channels, width, ups)),
        out_shape=jax.ShapeDtypeStruct((rows, own_width), bf16),
        in_specs=[hbm, vmem, hbm, hbm, vmem, vmem, hbm, vmem, hbm, hbm],
        out_specs=vmem,
        scratch_shapes=[
            pltpu.VMEM((chunks, channels, width), bf16),
            pltpu.VMEM((tokens, channels), bf16),
            pltpu.VMEM((tokens, channels), bf16),
            pltpu.VMEM((tokens, channels), bf16),
            pltpu.VMEM((LEAD + LENGTH, width), f32),
            pltpu.VMEM((tokens, width), f32),
            pltpu.VMEM((tokens, width), bf16),
            pltpu.VMEM((tokens, ups * width), bf16),
            pltpu.VMEM((8, tokens), f32),
            pltpu.VMEM((group, 8, tokens), f32),
            pltpu.VMEM((blocks, tokens, block), bf16),
            pltpu.VMEM((group, per_tp, rows, block), bf16),
            pltpu.VMEM((blocks, tokens, block), bf16),
            pltpu.VMEM((group, per_tp, rows, block), bf16),
            dma((chunks + 1,)),
            dma((2, chunks)),
            dma((2, chunks, n // 2)),
            dma((reps, tps)),
            dma((reps, tps)),
            dma((reps, tps)),
            dma((reps, tps)),
            dma((reps, tps)),
            dma((reps, tps)),
            dma((blocks, reps)),
            dma((group, per_tp)),
            dma((blocks, reps)),
            dma((group, per_tp)),
        ],
        compiler_params=pltpu.CompilerParams(
            collective_id=0, has_side_effects=True, vmem_limit_bytes=62 * 1024 * 1024
        ),
    )(
        states, mix_gain[None, :], w_value, w_gate, conv_kernel, chan_gain[None, :], w_mix,
        mlp_gain[None, :], w_up, w_down,
    )


def plane_kernel(
    sizes,
    states, mix_gain_in, w_value, w_gate, taps_in, chan_gain_in, w_mix, mlp_gain_in, w_up, w_down,
    out,
    mix_gain, conv_kernel, chan_gain, mlp_gain,
    weights, rows_in, rows_mid, normed, padded, filtered, activated, hidden, own_in, own_mid,
    own_stats, peer_stats, mix_parts, stage, mix_peers, fed_parts, fed_peers,
    load_sems, y_send, y_recv, near_send, far_send, line_recv, last_recv,
    twin_send, twin_recv, last_twin,
    in_send, in_recv, mid_send, mid_recv,
    stat_send, stat_recv, stage_send, stage_recv, mix_send, mix_recv, fed_send, fed_recv,
):
    reps, n, tps, rows, channels, sub, ups = sizes
    ys = tps
    zs = n // ys
    members = reps * ys
    width = sub * tps
    own_width = sub * members
    shard = channels // n
    plane_shard = shard * ys
    tokens = reps * rows
    seqs = rows // LENGTH
    chunks = 3 + 2 * ups
    rep, fs, tp = lax.axis_index("rep"), lax.axis_index("fs"), lax.axis_index("tp")
    z, y = fs // ys, lax.rem(fs, ys)
    other_rep, other_y, other_tp = reps - 1 - rep, ys - 1 - y, tps - 1 - tp
    other_fs = z * ys + other_y
    own_group = rep * ys + y
    taps = conv_kernel.shape[0]
    blocks, _, block = mix_parts.shape
    per_tp = own_width // block

    third = tuple(range(3, 3 + ups))
    is_home = tp == y
    not_home = jnp.logical_not(is_home)
    fourth = tuple(range(3 + ups, chunks))
    per_plane = plane_shard // block
    has_next = (z < zs - 1, z > 0)
    next_fs = (fs + ys, fs - ys)
    def scoped(name):
        def wrap(f):
            def run(*args):
                with jax.named_scope("_".join([name, *(str(a) for a in args[:2] if isinstance(a, int))])):
                    return f(*args)
            return run
        return wrap

    barrier = pltpu.get_barrier_semaphore()
    for dr in range(reps):
        for dy in range(ys):
            for dt in range(tps):
                if dr or dy or dt:
                    pl.semaphore_signal(
                        barrier, inc=1,
                        device_id={
                            "rep": lax.rem(rep + dr, reps),
                            "fs": z * ys + lax.rem(y + dy, ys),
                            "tp": lax.rem(tp + dt, tps),
                        },
                        device_id_type=MESH,
                    )
    for way in range(2):
        @pl.when(has_next[way])
        def _():
            pl.semaphore_signal(
                barrier, inc=1, device_id={"fs": next_fs[way]}, device_id_type=MESH
            )

    def remote(src, dst, send, recv, **where):
        return pltpu.make_async_remote_copy(
            src_ref=src, dst_ref=dst, send_sem=send, recv_sem=recv,
            device_id=where, device_id_type=MESH,
        )

    def rows_of(index, size=shard):
        return pl.ds(pl.multiple_of(index * size, size), size)

    def rep_rows(r):
        return pl.ds(pl.multiple_of(r * rows, rows), rows)

    half = pl.ds(pl.multiple_of(tp * sub, sub), sub)

    def columns_of(c, group):
        if c < 3:
            source, at = (w_value, w_gate, w_mix)[c], group
        elif c < 3 + ups:
            source, at = w_up, group * ups + c - 3
        else:
            source, at = w_down, group * ups + c - 3 - ups
        return source.at[:, pl.ds(pl.multiple_of(at * sub, sub), sub)]

    loads = [
        pltpu.make_async_copy(
            columns_of(c, own_group), weights.at[c, rows_of(fs), half], load_sems.at[min(c, 3)]
        )
        for c in range(chunks)
    ]
    home_cols = pl.ds(pl.multiple_of(tp * own_width, own_width), own_width)
    own_load = pltpu.make_async_copy(states, own_in, load_sems.at[4])
    home_load = pltpu.make_async_copy(
        states, rows_in.at[rep_rows(rep), home_cols], load_sems.at[5]
    )
    small_loads = [
        pltpu.make_async_copy(source, target, load_sems.at[6 + k])
        for k, (source, target) in enumerate(
            (
                (mix_gain_in, mix_gain), (taps_in, conv_kernel), (chan_gain_in, chan_gain),
                (mlp_gain_in, mlp_gain),
            )
        )
    ]
    for c in range(chunks):
        loads[c].start()
    pl.when(is_home)(home_load.start)
    own_load.start()
    for one in small_loads:
        one.start()
    along_line = sum(jnp.where(has, 1, 0) for has in has_next)
    pl.semaphore_wait(barrier, reps * ys * tps - 1 + along_line)

    def across(c):
        return remote(
            columns_of(c, rep * ys + other_y), weights.at[c, rows_of(fs), half],
            y_send.at[0], y_recv.at[c], fs=other_fs,
        )

    middle = jnp.minimum(z, zs - 1 - z)

    def offset_at(i):
        low = 2 * z < zs - 1
        near = -(i + 1) // 2 if i % 2 else i // 2
        near = jnp.where(low, near, -near)
        far = jnp.where(low, i - middle, middle - i)
        return jnp.where(i <= 2 * middle, near, far)

    offsets = [offset_at(i) for i in range(zs)]
    planes = [z + off for off in offsets]

    def moved(chunk, span, send, recv, **where):
        at = weights.at[chunk, span, half]
        return remote(at, at, send, recv, **where)

    def group_of(c):
        return slice(0, 2) if c < 2 else c if c == 2 else slice(3, 3 + ups)

    def twin(c, i):
        return moved(
            c, rows_of(planes[i], plane_shard), twin_send.at[c], twin_recv.at[0 if c < 2 else min(c - 1, 2)],
            tp=other_tp,
        )

    halves = shard // LANES

    def half_rows(index, h):
        return rows_of(index * halves + h, LANES)

    def twin_last(c, i, b, h):
        return moved(
            c, half_rows(planes[i] * ys + b, h), twin_send.at[c], last_twin.at[i, b, h],
            tp=other_tp,
        )

    def ready(c):
        group = group_of(c)
        whole_half = weights.at[group, :, half]
        remote(
            whole_half, whole_half, twin_send.at[c], twin_recv.at[0 if c < 2 else min(c - 1, 2)], tp=other_tp
        ).wait_recv()

    def ready_last(i, b, h):
        moved(
            slice(3 + ups, chunks), half_rows(planes[i] * ys + b, h), twin_send.at[0],
            last_twin.at[i, b, h], tp=other_tp,
        ).wait_recv()

    def near(c, way, part):
        if c not in fourth:
            return [
                moved(
                    c, rows_of(z * ys + part), near_send.at[way], line_recv.at[c, z],
                    fs=next_fs[way],
                )
            ]
        return [
            moved(
                c, half_rows(z * ys + part, h), near_send.at[way], last_recv.at[z, part, h],
                fs=next_fs[way],
            )
            for h in range(halves)
        ]

    def send_near(c, part):
        for way in range(2):
            for one in near(c, way, part):
                pl.when(has_next[way])(one.start)

    @scoped("begin")
    def begin(c):
        if c < 3:
            loads[c].wait()
        elif c == 3:
            at = weights.at[3:, rows_of(fs), half]
            pltpu.make_async_copy(at, at, load_sems.at[3]).wait()
        send_near(c, y)

    @scoped("own")
    def own(c):
        across(c).wait_recv()
        send_near(c, other_y)
        if c in fourth:
            for b in range(ys):
                for h in range(halves):
                    twin_last(c, 0, b, h).start()
        else:
            twin(c, 0).start()

    goes = [jnp.where(off < 0, z < zs - 1, z > 0) for off in offsets]

    def onward(chunk, i, span, recv):
        to = jnp.where(offsets[i] < 0, fs + ys, fs - ys)
        return moved(chunk, span, far_send.at[i - 1], recv, fs=to)

    @scoped("arrive")
    def arrive(c, i):
        copy = onward(c, i, rows_of(planes[i], plane_shard), line_recv.at[c, planes[i]])
        copy.wait_recv()
        pl.when(goes[i])(copy.start)
        twin(c, i).start()

    @scoped("arrive_last")
    def arrive_last(i, b, h):
        span, recv = half_rows(planes[i] * ys + b, h), last_recv.at[planes[i], b, h]
        copy = onward(slice(3 + ups, chunks), i, span, recv)
        copy.wait_recv()
        for c in fourth:
            pl.when(goes[i])(onward(c, i, span, recv).start)
        for c in fourth:
            twin_last(c, i, b, h).start()

    @scoped("drain")
    def drain(chunk):
        moved(chunk, slice(None), twin_send.at[chunk], twin_recv.at[0], tp=other_tp).wait_send()

    @scoped("drain_all")
    def drain_all():
        every = slice(None)
        moved(every, rows_of(fs), y_send.at[0], y_recv.at[0], fs=other_fs).wait_send()
        for way in range(2):
            copy = moved(
                every, rows_of(z, plane_shard), near_send.at[way], y_recv.at[0], fs=next_fs[way]
            )
            pl.when(has_next[way])(copy.wait_send)
        for i in range(1, zs):
            copy = onward(every, i, rows_of(planes[i], plane_shard), y_recv.at[0])
            pl.when(goes[i])(copy.wait_send)

    def spread(source, target, send, recv, over_from):
        def at(r, h, j):
            start = pl.multiple_of(h * own_width + j * block, block)
            return target.at[rep_rows(r), pl.ds(start, block)]

        def copies(j):
            if isinstance(j, slice):
                src, dst, j = source, target.at[rep_rows(rep), home_cols], 0
            else:
                src, dst = source.at[:, j * block : (j + 1) * block], at(rep, tp, j)
            along = remote(src, dst, send.at[0], recv.at[1, tp, j], rep=other_rep, tp=y)
            over = remote(src, dst, send.at[1], recv.at[0, tp, j], fs=other_fs, tp=y)
            inside = remote(src, dst, send.at[2], recv.at[0, tp, j], tp=y)
            return along, over, inside

        def passing(h, j):
            if h == 0 and j >= over_from:
                one = at(other_rep, 0, j)
                return remote(one, one, send.at[3], recv.at[1, 0, j], fs=other_fs)
            two = at(rep, h, j)
            return remote(two, two, send.at[3 + h], recv.at[1, h, j], rep=other_rep)

        def arrival(dr, h, j):
            dst = at(rep if dr == 0 else other_rep, h, j)
            return remote(dst, dst, send.at[0], recv.at[dr, h, j], rep=other_rep)

        def start(j):
            along, over, inside = copies(j)
            along.start()
            over.start()
            pl.when(jnp.logical_not(is_home))(inside.start)

        @scoped("forward")
        def forward(j):
            if j >= over_from:
                @pl.when(is_home)
                def _():
                    arrival(1, 0, j).wait_recv()
                    passing(0, j).start()

            @pl.when(jnp.logical_not(is_home))
            def _():
                for h in range(tps):
                    if h or j < over_from:
                        arrival(0, h, j).wait_recv()
                        passing(h, j).start()

        @scoped("finish")
        def finish(j):
            arrival(1, 1, j).wait_recv()

            @pl.when(is_home)
            def _():
                arrival(0, other_tp, j).wait_recv()
                if j < over_from:
                    arrival(1, 0, j).wait_recv()

            @pl.when(jnp.logical_not(is_home))
            def _():
                arrival(1, 0, j).wait_recv()
                if j >= over_from:
                    arrival(0, 0, j).wait_recv()

        def settle():
            along, over, inside = copies(slice(None))
            along.wait_send()
            over.wait_send()
            pl.when(not_home)(inside.wait_send)

            def part(k, blocks_sent):
                if blocks_sent:
                    sent = target.at[rep_rows(rep), : blocks_sent * block]
                    remote(sent, sent, send.at[k], recv.at[0, 0, 0], fs=other_fs).wait_send()

            pl.when(is_home)(functools.partial(part, 3, per_tp - over_from))

            @pl.when(not_home)
            def _():
                part(3, over_from)
                part(4, per_tp)

        return start, forward, finish, settle

    @scoped("norm")
    def norm_all(source, gain):
        def one(i, carry):
            span = pl.ds(pl.multiple_of(i * 64, 64), 64)
            x = source[span, :].astype(jnp.float32)
            scale = lax.rsqrt(jnp.mean(x * x, axis=-1, keepdims=True) + EPS)
            normed[span, :] = (x * scale * gain[...]).astype(jnp.bfloat16)
            return carry

        lax.fori_loop(0, tokens // 64, one, 0)

    def seq_rows(i):
        return pl.ds(pl.multiple_of(i * LENGTH, LENGTH), LENGTH)

    def mixer_rows(i):
        x = normed[seq_rows(i), :]
        value = jnp.dot(x, weights[0], preferred_element_type=jnp.float32)
        gate = jnp.dot(x, weights[1], preferred_element_type=jnp.float32)
        padded[LEAD : LEAD + LENGTH, :] = value * jax.nn.sigmoid(gate)
        per_sub = sub // LANES

        def column(j, sums):
            cols = pl.ds(pl.multiple_of(j * LANES, LANES), LANES)
            from_all = pl.multiple_of(
                (j // per_sub) * own_width + own_group * sub + lax.rem(j, per_sub) * LANES, LANES
            )
            kern = conv_kernel[:, pl.ds(from_all, LANES)]
            total = jnp.zeros((LENGTH, LANES), jnp.float32)
            for tap in range(taps):
                begin = LEAD - (taps - 1) + tap
                total = total + kern[tap : tap + 1, :] * padded[begin : begin + LENGTH, cols]
            filtered[seq_rows(i), cols] = total
            return sums[0] + total, sums[1] + total * total

        zero = jnp.zeros((LENGTH, LANES), jnp.float32)
        one, two = lax.fori_loop(0, width // LANES, column, (zero, zero))
        lane = lax.broadcasted_iota(jnp.int32, (LENGTH, LANES), 1)
        both = jnp.where(
            lane == 0,
            jnp.sum(one, axis=-1, keepdims=True),
            jnp.where(lane == 1, jnp.sum(two, axis=-1, keepdims=True), 0.0),
        )
        own_stats[i // seqs, :, seq_rows(lax.rem(i, seqs))] = both.T[0:8, :]

    def stat_copies(r):
        return [
            remote(
                own_stats.at[r], peer_stats.at[dr * ys + dy, r], stat_send.at[r],
                stat_recv.at[r],
                rep=lax.rem(rep + dr, reps), fs=z * ys + lax.rem(y + dy, ys),
            )
            for dr in range(reps) for dy in range(ys) if dr or dy
        ]

    def stat_waits(r):
        at = peer_stats.at[1:, r]
        return remote(at, at, stat_send.at[r], stat_recv.at[r], rep=other_rep)

    def activate_rows(i, carry):
        within = seq_rows(lax.rem(i, seqs))
        total = own_stats[i // seqs, :, within]
        for k in range(1, members):
            total = total + peer_stats[k, i // seqs, :, within]
        turned = jnp.concatenate([total] * (LANES // 8), axis=0).T
        mean = turned[:, 0:1] / channels
        variance = turned[:, 1:2] / channels - mean * mean
        gain = jnp.concatenate(
            [
                chan_gain[:, pl.ds(pl.multiple_of(t * own_width + own_group * sub, sub), sub)]
                for t in range(tps)
            ],
            axis=1,
        )
        x = (filtered[seq_rows(i), :] - mean) * lax.rsqrt(variance + EPS) * gain
        activated[seq_rows(i), :] = (x / (1.0 + jnp.exp(-x))).astype(jnp.bfloat16)
        return carry

    @scoped("share")
    def share(o, dr, part, left, pieces_of, parts, peers, send, recv):
        to = lax.rem(rep + dr, reps)
        first, size = part
        span = pl.ds(pl.multiple_of(o * block + first, size), size)
        cols = pl.ds(first, size)
        keeper, kept = o // per_tp, lax.rem(o, per_tp)
        at = rep_rows(to)
        total = None
        for k, c in enumerate(pieces_of):
            term = times_transposed(left[at, k * width : (k + 1) * width], weights[c, span, :])
            total = term if total is None else total + term
        parts[o, at, cols] = total.astype(jnp.bfloat16)
        slot = lax.rem(rep + reps - to, reps) * ys + lax.rem(y + ys - tp, ys)
        copy = remote(
            parts.at[o, at, cols], peers.at[slot, kept, :, cols], send.at[dr], recv.at[kept],
            rep=to, fs=z * ys + tp, tp=keeper,
        )
        here = jnp.logical_and(is_home, jnp.logical_and(keeper == tp, to == rep))
        pl.when(jnp.logical_not(here))(copy.start)

    def along_first(o):
        return o % 2 == 0

    def stage_copy(o, r):
        if along_first(o):
            return remote(
                mix_parts.at[o, rep_rows(other_rep), :], stage.at[o, 0], stage_send.at[0],
                stage_recv.at[o], rep=other_rep,
            )
        return remote(
            mix_parts.at[o, rep_rows(r), :], stage.at[o, r], stage_send.at[1],
            stage_recv.at[o], fs=z * ys + tp,
        )

    def last_copies(o):
        keeper, kept = o // per_tp, o % per_tp
        own_part = mix_parts.at[o, rep_rows(rep), :]
        inside = remote(
            own_part, mix_peers.at[0, kept], mix_send.at[0], mix_recv.at[kept], tp=keeper
        )
        if along_first(o):
            outside = remote(
                own_part, mix_peers.at[1, kept], mix_send.at[1], mix_recv.at[kept],
                fs=z * ys + tp, tp=keeper,
            )
        else:
            outside = remote(
                mix_parts.at[o, rep_rows(other_rep), :], mix_peers.at[1, kept],
                mix_send.at[1], mix_recv.at[kept], rep=other_rep, tp=keeper,
            )
        inner_one = jnp.logical_and(is_home, tp != keeper)
        return inside, inner_one, outside, not_home if along_first(o) else is_home

    @scoped("mix_share")
    def mix_share(o, r):
        at = rep_rows(r)
        mix_parts[o, at, :] = times_transposed(
            activated[at, :], weights[2, o * block : (o + 1) * block, :]
        ).astype(jnp.bfloat16)
        pl.when(rep != r if along_first(o) else not_home)(stage_copy(o, r).start)

    def mix_add(o, at, k):
        total = mix_parts[o, at, :].astype(jnp.float32) + stage[o, k].astype(jnp.float32)
        mix_parts[o, at, :] = total.astype(jnp.bfloat16)

    @scoped("combine")
    def combine(o):
        keeper, kept = o // per_tp, o % per_tp
        inside, inner_one, outside, outer_one = last_copies(o)

        def pass_on():
            pl.when(outer_one)(outside.start)
            pl.when(inner_one)(inside.start)

            @pl.when(jnp.logical_and(is_home, tp == keeper))
            def _():
                mix_peers[0, kept] = mix_parts[o, rep_rows(rep), :]

        if along_first(o):
            stage_copy(o, 0).wait_recv()
            mix_add(o, rep_rows(rep), 0)
            pass_on()
        else:
            @pl.when(is_home)
            def _():
                both = stage.at[o]
                remote(both, both, stage_send.at[1], stage_recv.at[o], fs=other_fs).wait_recv()
                for r in range(reps):
                    mix_add(o, rep_rows(r), r)
                pass_on()

    @scoped("mix_final")
    def mix_final(j):
        def some(start):
            at = mix_peers.at[start:, j]
            return remote(at, at, mix_send.at[0], mix_recv.at[j], rep=other_rep)

        pl.when(is_home)(some(1).wait_recv)
        pl.when(not_home)(some(0).wait_recv)
        return mix_peers[0, j].astype(jnp.float32) + mix_peers[1, j].astype(jnp.float32)

    def mix_settle():
        def sent(count, send):
            at = mix_parts.at[:count, rep_rows(rep), :]
            return remote(at, at, send, mix_recv.at[0], rep=other_rep)

        even = sum(1 for o in range(blocks) if along_first(o))
        sent(even, stage_send.at[0]).wait_send()
        pl.when(not_home)(sent((blocks - even) * reps, stage_send.at[1]).wait_send)
        pl.when(is_home)(sent(per_tp, mix_send.at[0]).wait_send)
        pl.when(not_home)(sent(even, mix_send.at[1]).wait_send)
        pl.when(is_home)(sent(blocks - even, mix_send.at[1]).wait_send)

    @scoped("peers")
    def wait_peers(j, parts, peers, send, recv):
        def some(start):
            at = peers.at[start:, j]
            return remote(at, at, send.at[0], recv.at[j], rep=other_rep)

        @pl.when(is_home)
        def _():
            peers[0, j] = parts[tp * per_tp + j, rep_rows(rep), :]
            some(1).wait_recv()

        pl.when(not_home)(some(0).wait_recv)

    def settle_share(parts, send, recv):
        for dr in range(reps):
            for count, who in ((per_tp, is_home), (blocks, not_home)):
                sent = parts.at[: count if dr == 0 else blocks, rep_rows(rep), :]
                copy = remote(sent, sent, send.at[dr], recv.at[0], rep=other_rep)
                pl.when(who)(copy.wait_send)

    def total_of(j, peers):
        total = peers[0, j].astype(jnp.float32)
        for k in range(1, members):
            total = total + peers[k, j].astype(jnp.float32)
        return total

    start_in, forward_in, finish_in, settle_in = spread(
        states, rows_in, in_send, in_recv, per_tp // 2
    )
    start_mid, forward_mid, finish_mid, settle_mid = spread(
        own_mid, rows_mid, mid_send, mid_recv, 0
    )

    def inner(*todo):
        @pl.when(middle > 0)
        def _():
            for one in todo:
                one()

    def outer(*todo):
        @pl.when(middle == 0)
        def _():
            for one in todo:
                one()

    def pump(c, i):
        return functools.partial(arrive, c, i)

    def all_of(c):
        return [pump(c, i) for i in range(1, zs)]

    def whole(c):
        return [functools.partial(begin, c), functools.partial(own, c)]

    across(0).start()
    across(1).start()
    begin(0)
    begin(1)
    for j in range(per_tp):
        start_in(j)
    own(0)
    own(1)
    across(2).start()
    across(3).start()
    padded[0:LEAD, :] = jnp.zeros((LEAD, width), jnp.float32)
    arrive(0, 1)
    arrive(1, 1)
    forward_in(0)
    inner(pump(0, 2), pump(1, 2))
    for j in range(1, per_tp // 2):
        forward_in(j)
    inner(*[pump(c, i) for i in range(3, zs) for c in (0, 1)])
    for j in range(per_tp // 2, per_tp):
        forward_in(j)
    begin(2)
    own(2)
    outer(*[pump(c, 2) for c in (0, 1)])
    for j in range(per_tp):
        finish_in(j)
    for c in range(4, chunks):
        across(c).start()
    pl.when(is_home)(home_load.wait)
    for one in small_loads:
        one.wait()
    norm_all(rows_in, mix_gain)
    outer(*[pump(c, i) for i in range(3, zs) for c in (0, 1)])
    ready(0)

    inner(*all_of(2)[:1])
    outer(*whole(3))
    inside = [
        all_of(2)[1:2], all_of(2)[2:] + whole(3), whole(4), [],
    ]
    outside = [whole(4), whole(5), whole(fourth[0]), sum([whole(c) for c in fourth[1:]], [])]
    for r in range(reps):
        for cut in ((0, (seqs + 1) // 2), ((seqs + 1) // 2, seqs)):
            with jax.named_scope("mixer"):
                lax.fori_loop(
                    r * seqs + cut[0], r * seqs + cut[1],
                    lambda k, carry: (mixer_rows(k), carry)[1], 0,
                )
            if inside:
                inner(*inside.pop(0))
                outer(*outside.pop(0))
        for one in stat_copies(r):
            one.start()
    outer(*all_of(2))
    ready(2)
    for r in range(reps):
        with jax.named_scope("stats"):
            stat_waits(r).wait_recv()
        with jax.named_scope("activate"):
            lax.fori_loop(r * seqs, (r + 1) * seqs, activate_rows, 0)
        for j in range(per_tp):
            for t in range(tps):
                mix_share(t * per_tp + j, r)

    own_load.wait()
    inner(*whole(5), *all_of(3)[:2])
    def last(i, b):
        return [functools.partial(arrive_last, i, b, h) for h in range(halves)]

    early = [
        all_of(3)[2:] + all_of(4)[:2],
        all_of(4)[2:] + all_of(5)[:2] + whole(fourth[0]),
        all_of(5)[2:] + sum([whole(c) for c in fourth[1:]], []),
    ]
    late = [[], all_of(3), all_of(4)[:1], all_of(4)[1:]]
    for t in range(tps):
        combine(t * per_tp)
    for j in range(per_tp):
        if j + 1 < per_tp:
            for t in range(tps):
                combine(t * per_tp + j + 1)
        mixed = mix_final(j)
        cols = slice(j * block, (j + 1) * block)
        own_mid[:, cols] = (own_in[:, cols].astype(jnp.float32) + mixed).astype(jnp.bfloat16)
        start_mid(j)

        @pl.when(is_home)
        def _():
            start = pl.multiple_of(tp * own_width + j * block, block)
            rows_mid[rep_rows(rep), pl.ds(start, block)] = own_mid[:, cols]

        if j:
            forward_mid(j - 1)
        if j < len(early):
            inner(*early[j])
        if j == per_tp - 1:
            forward_mid(j)
            inner(*[one for b in range(ys) for one in last(1, b)])
        if j < len(late):
            outer(*late[j])
    for rest in early[per_tp:]:
        inner(*rest)
    for rest in late[per_tp:]:
        outer(*rest)
    for j in range(per_tp):
        finish_mid(j)
    outer(*all_of(5))
    norm_all(rows_mid, mlp_gain)
    ready(3)

    @scoped("up")
    def up_some(k):
        def up_rows(i, carry):
            at = rep_rows(i)
            x = jnp.dot(normed[at, :], weights[3 + k], preferred_element_type=jnp.float32)
            x = jnp.maximum(x, 0.0)
            hidden[at, k * width : (k + 1) * width] = (x * x).astype(jnp.bfloat16)
            return carry

        lax.fori_loop(0, reps, up_rows, 0)

    for k in range(ups):
        up_some(k)
    fed = (hidden, fourth, fed_parts, fed_peers, fed_send, fed_recv)
    settle_in()
    settle_mid()
    mix_settle()
    for r in range(reps):
        stat_waits(r).wait_send()
    for i in range(zs):
        for b in range(ys):
            if 1 < i + 1 < zs:
                inner(*last(i + 1, b))
            if i < zs - 1:
                if i:
                    outer(*last(i, b))
                for h in range(halves):
                    ready_last(i, b, h)
                for dr in (*range(1, reps), 0):
                    share(planes[i] * ys + b, dr, (0, block), *fed)
            else:
                for h in range(halves):
                    outer(last(i, b)[h])
                    ready_last(i, b, h)
                    for dr in (*range(1, reps), 0):
                        share(planes[i] * ys + b, dr, (h * LANES, LANES), *fed)
            if i == 1 and b == 0:
                for c in range(3 + ups):
                    drain(c)
    for j in range(per_tp):
        if j == per_tp - 1:
            for c in fourth:
                drain(c)
            drain_all()
        wait_peers(j, fed_parts, fed_peers, fed_send, fed_recv)
        cols = slice(j * block, (j + 1) * block)
        with jax.named_scope("out"):
            out[:, cols] = (
                own_mid[:, cols].astype(jnp.float32) + total_of(j, fed_peers)
            ).astype(jnp.bfloat16)
    with jax.named_scope("done"):
        settle_share(fed_parts, fed_send, fed_recv)


def plane_body(mesh, states, mix_gain, w_value, w_gate, conv_kernel, chan_gain, w_mix, mlp_gain, w_up, w_down):
    reps, n, tps = mesh.shape["rep"], mesh.shape["fs"], mesh.shape["tp"]
    rows, own_width = states.shape
    ys = tps
    zs, members = n // ys, reps * ys
    sub = own_width // members
    width = sub * tps
    channels = own_width * tps
    ups = w_up.shape[1] // own_width
    tokens = rows * reps
    block = channels // n
    halves = block // LANES
    blocks, per_tp = channels // block, own_width // block
    chunks = 3 + 2 * ups
    bf16, f32 = jnp.bfloat16, jnp.float32
    vmem, hbm = pl.BlockSpec(memory_space=pltpu.VMEM), pl.BlockSpec(memory_space=pl.ANY)
    dma = pltpu.SemaphoreType.DMA
    return pl.pallas_call(
        functools.partial(plane_kernel, (reps, n, tps, rows, channels, sub, ups)),
        out_shape=pltpu.VMEM((rows, own_width), bf16),
        in_specs=[hbm] * 10,
        out_specs=vmem,
        scratch_shapes=[
            pltpu.VMEM((1, channels), f32),
            pltpu.VMEM(conv_kernel.shape, f32),
            pltpu.VMEM((1, channels), f32),
            pltpu.VMEM((1, channels), f32),
            pltpu.VMEM((chunks, channels, width), bf16),
            pltpu.VMEM((tokens, channels), bf16),
            pltpu.VMEM((tokens, channels), bf16),
            pltpu.VMEM((tokens, channels), bf16),
            pltpu.VMEM((LEAD + LENGTH, width), f32),
            pltpu.VMEM((tokens, width), f32),
            pltpu.VMEM((tokens, width), bf16),
            pltpu.VMEM((tokens, ups * width), bf16),
            pltpu.VMEM((rows, own_width), bf16),
            pltpu.VMEM((rows, own_width), bf16),
            pltpu.VMEM((reps, 8, rows), f32),
            pltpu.VMEM((members, reps, 8, rows), f32),
            pltpu.VMEM((blocks, tokens, block), bf16),
            pltpu.VMEM((blocks, reps, rows, block), bf16),
            pltpu.VMEM((2, per_tp, rows, block), bf16),
            pltpu.VMEM((blocks, tokens, block), bf16),
            pltpu.VMEM((members, per_tp, rows, block), bf16),
            dma((10,)),
            dma((1,)),
            dma((chunks,)),
            dma((2,)),
            dma((zs - 1,)),
            dma((3 + ups, zs)),
            dma((zs, ys, halves)),
            dma((chunks,)),
            dma((3,)),
            dma((zs, ys, halves)),
            dma((5,)),
            dma((reps, tps, per_tp)),
            dma((5,)),
            dma((reps, tps, per_tp)),
            dma((reps,)),
            dma((reps,)),
            dma((2,)),
            dma((blocks,)),
            dma((2,)),
            dma((per_tp,)),
            dma((reps,)),
            dma((per_tp,)),
        ],
        compiler_params=pltpu.CompilerParams(
            collective_id=0, has_side_effects=True, vmem_limit_bytes=56 * 1024 * 1024
        ),
    )(
        states, mix_gain[None, :], w_value, w_gate, conv_kernel, chan_gain[None, :], w_mix,
        mlp_gain[None, :], w_up, w_down,
    )


def body(mesh, states, *weights):
    reps, n, tps = mesh.shape["rep"], mesh.shape["fs"], mesh.shape["tp"]
    own_width = states.shape[1]
    channels = own_width * tps
    planar = (
        reps == tps == 2
        and n % tps == 0
        and n // tps > 2
        and own_width % (reps * tps * LANES) == 0
        and channels % (n * LANES) == 0
        and own_width % (channels // n) == 0
    )
    return (plane_body if planar else ring_body)(mesh, states, *weights)


def solution(mesh):
    in_specs = (
        P(("rep", "fs"), "tp"),
        P(),
        P("fs", "tp"),
        P("fs", "tp"),
        P(),
        P(),
        P("fs", "tp"),
        P(),
        P("fs", "tp"),
        P("fs", "tp"),
    )
    out_specs = P(("rep", "fs"), "tp")
    return jax.shard_map(
        functools.partial(body, mesh),
        mesh=mesh, in_specs=in_specs, out_specs=out_specs, check_vma=False,
    )
```

```python
import functools

import jax
import jax.numpy as jnp
from jax import lax
from jax.experimental import pallas as pl
from jax.experimental.pallas import tpu as pltpu
from jax.sharding import PartitionSpec as P

LENGTH = 128
LANES = 128
LEAD = 32
EPS = 1e-06
MESH = pl.DeviceIdType.MESH


def times_transposed(left, right):
    return lax.dot_general(
        left, right, (((1,), (1,)), ((), ())), preferred_element_type=jnp.float32
    )


def ring_kernel(
    sizes,
    states, mix_gain, w_value, w_gate, conv_kernel, chan_gain, w_mix, mlp_gain, w_up, w_down,
    out,
    weights, rows_in, rows_mid, normed, padded, filtered, activated, hidden,
    own_stats, peer_stats, mix_parts, mix_peers, fed_parts, fed_peers,
    load_sems, ring_send, ring_recv, in_send, in_recv, mid_send, mid_recv,
    stat_send, stat_recv, mix_send, mix_recv, fed_send, fed_recv,
):
    reps, n, tps, rows, channels, width, ups = sizes
    own_width = width * reps
    half_way = n // 2
    shard = channels // n
    tokens = reps * rows
    pieces = tokens // LENGTH
    chunks = 3 + 2 * ups
    rep, fs, tp = lax.axis_index("rep"), lax.axis_index("fs"), lax.axis_index("tp")
    taps = conv_kernel.shape[0]
    blocks, _, block = mix_parts.shape
    per_tp = own_width // block

    def ring_index(place):
        place = lax.rem(place + n, n)
        return jnp.where(place < half_way, 2 * place, 2 * (n - 1 - place) + 1)

    place = jnp.where(lax.rem(fs, 2) == 0, fs // 2, n - 1 - fs // 2)
    neighbours = (ring_index(place + 1), ring_index(place - 1))

    barrier = pltpu.get_barrier_semaphore()
    for other in neighbours:
        pl.semaphore_signal(barrier, inc=1, device_id={"fs": other}, device_id_type=MESH)
    for dr in range(reps):
        for dt in range(tps):
            if dr or dt:
                pl.semaphore_signal(
                    barrier, inc=1,
                    device_id={"rep": lax.rem(rep + dr, reps), "tp": lax.rem(tp + dt, tps)},
                    device_id_type=MESH,
                )

    own_rows = pl.ds(pl.multiple_of(rep * rows, rows), rows)
    own_cols = pl.ds(pl.multiple_of(tp * own_width, own_width), own_width)

    def shard_at(owner, start=0, size=None):
        size = shard if size is None else size
        return pl.ds(pl.multiple_of(owner * shard + start, size), size)

    def hop(c, s, way):
        sign = 1 if way == 0 else -1
        owner = ring_index(place - sign * (s - 1))
        span = shard_at(owner)
        if s == half_way:
            span = shard_at(owner, way * (shard // 2), shard // 2)
        return pltpu.make_async_remote_copy(
            src_ref=weights.at[c, span, :],
            dst_ref=weights.at[c, span, :],
            send_sem=ring_send.at[way, c],
            recv_sem=ring_recv.at[way, c, s - 1],
            device_id={"fs": neighbours[way]},
            device_id_type=MESH,
        )

    loads = []
    for c in range(chunks):
        if c < 3:
            source, column = (w_value, w_gate, w_mix)[c], rep * width
        elif c < 3 + ups:
            source, column = w_up, (rep * ups + c - 3) * width
        else:
            source, column = w_down, (rep * ups + c - 3 - ups) * width
        loads.append(
            pltpu.make_async_copy(
                source.at[:, pl.ds(pl.multiple_of(column, width), width)],
                weights.at[c, shard_at(fs), :],
                load_sems.at[c],
            )
        )
        loads[-1].start()
    own_load = pltpu.make_async_copy(states, rows_in.at[own_rows, own_cols], load_sems.at[chunks])
    own_load.start()
    pl.semaphore_wait(barrier, 1 + reps * tps)

    def pump(c, s):
        for way in range(2):
            if s == 1:
                if way == 0:
                    loads[c].wait()
            else:
                before = hop(c, s - 1, way)
                before.wait_recv()
                before.wait_send()
            hop(c, s, way).start()

    def arrived(c):
        for way in range(2):
            last = hop(c, half_way, way)
            last.wait_recv()
            last.wait_send()

    def spread(source, target, send, recv):
        def copy(dr, dt, ahead):
            if ahead:
                span = pl.ds(pl.multiple_of(lax.rem(rep + reps - dr, reps) * rows, rows), rows)
                src = target.at[span, own_cols]
            else:
                span, src = own_rows, source
            step_r = 0 if ahead else dr
            return pltpu.make_async_remote_copy(
                src_ref=src,
                dst_ref=target.at[span, own_cols],
                send_sem=send.at[dr, dt],
                recv_sem=recv.at[dr, dt],
                device_id={"rep": lax.rem(rep + step_r, reps), "tp": lax.rem(tp + dt, tps)},
                device_id_type=MESH,
            )

        first = [copy(dr, 0, False) for dr in range(1, reps)]
        near = [copy(0, dt, False) for dt in range(1, tps)]
        for one in first + near:
            one.start()

        def forward():
            later = []
            for dr in range(1, reps):
                first[dr - 1].wait_recv()
                for dt in range(1, tps):
                    one = copy(dr, dt, True)
                    one.start()
                    later.append(one)
            return later

        def finish(later):
            for one in near + later:
                one.wait_recv()
            for one in first + near + later:
                one.wait_send()

        return forward, finish

    def norm_all(source, gain):
        def one(i, carry):
            span = pl.ds(pl.multiple_of(i * 64, 64), 64)
            x = source[span, :].astype(jnp.float32)
            scale = lax.rsqrt(jnp.mean(x * x, axis=-1, keepdims=True) + EPS)
            normed[span, :] = (x * scale * gain[...]).astype(jnp.bfloat16)
            return carry

        lax.fori_loop(0, tokens // 64, one, 0)

    def seq_rows(i):
        return pl.ds(pl.multiple_of(i * LENGTH, LENGTH), LENGTH)

    def mixer_rows(i):
        x = normed[seq_rows(i), :]
        value = jnp.dot(x, weights[0], preferred_element_type=jnp.float32)
        gate = jnp.dot(x, weights[1], preferred_element_type=jnp.float32)
        padded[LEAD : LEAD + LENGTH, :] = value * jax.nn.sigmoid(gate)

        def column(j, sums):
            cols = pl.ds(pl.multiple_of(j * LANES, LANES), LANES)
            from_all = pl.multiple_of(tp * own_width + rep * width + j * LANES, LANES)
            kern = conv_kernel[:, pl.ds(from_all, LANES)]
            total = jnp.zeros((LENGTH, LANES), jnp.float32)
            for tap in range(taps):
                begin = LEAD - (taps - 1) + tap
                total = total + kern[tap : tap + 1, :] * padded[begin : begin + LENGTH, cols]
            filtered[seq_rows(i), cols] = total
            return sums[0] + total, sums[1] + total * total

        zero = jnp.zeros((LENGTH, LANES), jnp.float32)
        one, two = lax.fori_loop(0, width // LANES, column, (zero, zero))
        lane = lax.broadcasted_iota(jnp.int32, (LENGTH, LANES), 1)
        both = jnp.where(
            lane == 0,
            jnp.sum(one, axis=-1, keepdims=True),
            jnp.where(lane == 1, jnp.sum(two, axis=-1, keepdims=True), 0.0),
        )
        own_stats[:, seq_rows(i)] = both.T[0:8, :]

    def stat_copies():
        copies = []
        for dr in range(reps):
            for dt in range(tps):
                if dr or dt:
                    copies.append(
                        pltpu.make_async_remote_copy(
                            src_ref=own_stats,
                            dst_ref=peer_stats.at[dr * tps + dt],
                            send_sem=stat_send.at[dr, dt],
                            recv_sem=stat_recv.at[dr, dt],
                            device_id={
                                "rep": lax.rem(rep + dr, reps),
                                "tp": lax.rem(tp + dt, tps),
                            },
                            device_id_type=MESH,
                        )
                    )
        return copies

    def activate_rows(i, carry):
        total = own_stats[:, seq_rows(i)]
        for k in range(1, reps * tps):
            total = total + peer_stats[k, :, seq_rows(i)]
        turned = jnp.concatenate([total] * (LANES // 8), axis=0).T
        mean = turned[:, 0:1] / channels
        variance = turned[:, 1:2] / channels - mean * mean
        gain_at = pl.multiple_of(tp * own_width + rep * width, LANES)
        gain = chan_gain[:, pl.ds(gain_at, width)]
        x = (filtered[seq_rows(i), :] - mean) * lax.rsqrt(variance + EPS) * gain
        activated[seq_rows(i), :] = (x / (1.0 + jnp.exp(-x))).astype(jnp.bfloat16)
        return carry

    def share(order, o, left, pieces_of, parts, peers, send, recv):
        span = pl.ds(pl.multiple_of(o * block, block), block)

        def one(i):
            at = pl.ds(pl.multiple_of(i * rows, rows), rows)
            total = None
            for k, c in enumerate(pieces_of):
                term = times_transposed(
                    left[at, k * width : (k + 1) * width], weights[c, span, :]
                )
                total = term if total is None else total + term
            parts[o, at, :] = total.astype(jnp.bfloat16)

        keeper = o // per_tp
        dt = lax.rem(keeper + tps - tp, tps)
        waits = []
        for dr in [*range(1, reps), 0]:
            to = lax.rem(rep + dr, reps)
            one(to)
            copy = pltpu.make_async_remote_copy(
                src_ref=parts.at[o, pl.ds(pl.multiple_of(to * rows, rows), rows), :],
                dst_ref=peers.at[dr * tps + dt, lax.rem(o, per_tp)],
                send_sem=send.at[order, dr],
                recv_sem=recv.at[dr * tps + dt, lax.rem(o, per_tp)],
                device_id={"rep": to, "tp": keeper},
                device_id_type=MESH,
            )
            if dr:
                copy.start()
                waits.append(copy.wait_send)
            else:
                pl.when(keeper != tp)(copy.start)
                waits.append(lambda k=keeper, c=copy: pl.when(k != tp)(c.wait_send))
        return waits

    def wait_peers(j, parts, peers, send, recv):
        for k in range(1, reps * tps):
            dr, dt = k // tps, k % tps
            pltpu.make_async_remote_copy(
                src_ref=parts.at[0, own_rows, :],
                dst_ref=peers.at[k, j],
                send_sem=send.at[0, 0],
                recv_sem=recv.at[k, j],
                device_id={"rep": lax.rem(rep + dr, reps), "tp": lax.rem(tp + dt, tps)},
                device_id_type=MESH,
            ).wait_recv()

    def total_of(j, parts, peers):
        total = parts[tp * per_tp + j, own_rows, :].astype(jnp.float32)
        for k in range(1, reps * tps):
            total = total + peers[k, j].astype(jnp.float32)
        return total

    stepwise = blocks == n

    def owners(s):
        if s in (0, half_way):
            return [ring_index(place + s)]
        return [ring_index(place - s), ring_index(place + s)]

    def steps_of(c):
        return range(1, half_way + 1)

    first, second = (0, 1), (2, 3)
    third = tuple(range(4, 3 + ups))
    fourth = tuple(range(3 + ups, chunks))

    pump(0, 1)
    pump(1, 1)
    forward, finish = spread(states, rows_in, in_send, in_recv)
    padded[0:LEAD, :] = jnp.zeros((LEAD, width), jnp.float32)
    pump(0, 2)
    pump(1, 2)
    later = forward()
    for s in range(3, half_way + 1):
        pump(0, s)
        if s == 3:
            own_load.wait()
            finish(later)
        pump(1, s)
        if s == 3:
            norm_all(rows_in, mix_gain)
    pump(2, 1)
    pump(3, 1)
    arrived(0)
    arrived(1)

    todo = [(c, s) for s in range(2, half_way + 1) for c in second]

    def next_hop():
        if todo:
            pump(*todo.pop(0))

    for i in range(0, pieces, 2):
        lax.fori_loop(
            i, min(i + 2, pieces), lambda k, carry: (mixer_rows(k), carry)[1], 0
        )
        next_hop()
    stats = stat_copies()
    for one in stats:
        one.start()
    for one in stats:
        one.wait_recv()
    lax.fori_loop(0, pieces, activate_rows, 0)
    waits = []
    mix = (activated, (2,), mix_parts, mix_peers, mix_send, mix_recv)
    if stepwise:
        for s in range(half_way - 1):
            for o in owners(s):
                waits += share(len(waits) // reps, o, *mix)
    while todo:
        next_hop()
    if stepwise:
        for o in owners(half_way - 1):
            waits += share(len(waits) // reps, o, *mix)
    for c in third:
        pump(c, 1)
    arrived(2)
    if stepwise:
        waits += share(len(waits) // reps, owners(half_way)[0], *mix)
    else:
        for o in range(blocks):
            waits += share(o, o, *mix)

    todo = [(c, s) for s in range(2, half_way + 1) for c in third]
    for _ in range(len(todo) // 2):
        next_hop()
    for j in range(per_tp):
        wait_peers(j, mix_parts, mix_peers, mix_send, mix_recv)
        at = pl.ds(pl.multiple_of(tp * own_width + j * block, block), block)
        rows_mid[own_rows, at] = (
            rows_in[own_rows, at].astype(jnp.float32) + total_of(j, mix_parts, mix_peers)
        ).astype(jnp.bfloat16)
    forward, finish = spread(rows_mid.at[own_rows, own_cols], rows_mid, mid_send, mid_recv)
    while todo:
        next_hop()
    for c in fourth:
        pump(c, 1)
    arrived(3)
    for c in third:
        arrived(c)
    later = forward()
    finish(later)
    norm_all(rows_mid, mlp_gain)
    todo = [(c, s) for s in range(2, half_way + 1) for c in fourth]
    next_hop()
    for k in range(ups):

        def up_rows(i, carry):
            at = pl.ds(pl.multiple_of(i * rows, rows), rows)
            x = jnp.dot(normed[at, :], weights[3 + k], preferred_element_type=jnp.float32)
            x = jnp.maximum(x, 0.0)
            hidden[at, k * width : (k + 1) * width] = (x * x).astype(jnp.bfloat16)
            return carry

        lax.fori_loop(0, reps, up_rows, 0)
        next_hop()
    done = []
    fed = (hidden, fourth, fed_parts, fed_peers, fed_send, fed_recv)
    if stepwise:
        for o in owners(0):
            done += share(len(done) // reps, o, *fed)
    for s in range(2, half_way + 1):
        while todo and todo[0][1] <= s:
            next_hop()
        if stepwise:
            for o in owners(s - 1):
                done += share(len(done) // reps, o, *fed)
    for c in fourth:
        arrived(c)
    if stepwise:
        done += share(len(done) // reps, owners(half_way)[0], *fed)
    else:
        for o in range(blocks):
            done += share(o, o, *fed)
    for j in range(per_tp):
        wait_peers(j, fed_parts, fed_peers, fed_send, fed_recv)
        at = pl.ds(pl.multiple_of(tp * own_width + j * block, block), block)
        out[:, j * block : (j + 1) * block] = (
            rows_mid[own_rows, at].astype(jnp.float32) + total_of(j, fed_parts, fed_peers)
        ).astype(jnp.bfloat16)
    for one in stats:
        one.wait_send()
    for wait in waits + done:
        wait()


def ring_body(mesh, states, mix_gain, w_value, w_gate, conv_kernel, chan_gain, w_mix, mlp_gain, w_up, w_down):
    reps, n, tps = mesh.shape["rep"], mesh.shape["fs"], mesh.shape["tp"]
    rows, own_width = states.shape
    width = own_width // reps
    channels = own_width * tps
    ups = w_up.shape[1] // own_width
    tokens = rows * reps
    group = reps * tps
    block = channels // n if channels // n >= LANES else own_width
    blocks, per_tp = channels // block, own_width // block
    chunks = 3 + 2 * ups
    bf16, f32 = jnp.bfloat16, jnp.float32
    vmem, hbm = pl.BlockSpec(memory_space=pltpu.VMEM), pl.BlockSpec(memory_space=pl.ANY)
    dma = pltpu.SemaphoreType.DMA
    return pl.pallas_call(
        functools.partial(ring_kernel, (reps, n, tps, rows, channels, width, ups)),
        out_shape=jax.ShapeDtypeStruct((rows, own_width), bf16),
        in_specs=[hbm, vmem, hbm, hbm, vmem, vmem, hbm, vmem, hbm, hbm],
        out_specs=vmem,
        scratch_shapes=[
            pltpu.VMEM((chunks, channels, width), bf16),
            pltpu.VMEM((tokens, channels), bf16),
            pltpu.VMEM((tokens, channels), bf16),
            pltpu.VMEM((tokens, channels), bf16),
            pltpu.VMEM((LEAD + LENGTH, width), f32),
            pltpu.VMEM((tokens, width), f32),
            pltpu.VMEM((tokens, width), bf16),
            pltpu.VMEM((tokens, ups * width), bf16),
            pltpu.VMEM((8, tokens), f32),
            pltpu.VMEM((group, 8, tokens), f32),
            pltpu.VMEM((blocks, tokens, block), bf16),
            pltpu.VMEM((group, per_tp, rows, block), bf16),
            pltpu.VMEM((blocks, tokens, block), bf16),
            pltpu.VMEM((group, per_tp, rows, block), bf16),
            dma((chunks + 1,)),
            dma((2, chunks)),
            dma((2, chunks, n // 2)),
            dma((reps, tps)),
            dma((reps, tps)),
            dma((reps, tps)),
            dma((reps, tps)),
            dma((reps, tps)),
            dma((reps, tps)),
            dma((blocks, reps)),
            dma((group, per_tp)),
            dma((blocks, reps)),
            dma((group, per_tp)),
        ],
        compiler_params=pltpu.CompilerParams(
            collective_id=0, has_side_effects=True, vmem_limit_bytes=62 * 1024 * 1024
        ),
    )(
        states, mix_gain[None, :], w_value, w_gate, conv_kernel, chan_gain[None, :], w_mix,
        mlp_gain[None, :], w_up, w_down,
    )


def plane_kernel(
    sizes,
    states, mix_gain_in, w_value, w_gate, taps_in, chan_gain_in, w_mix, mlp_gain_in, w_up, w_down,
    out,
    mix_gain, conv_kernel, chan_gain, mlp_gain,
    weights, rows_in, rows_mid, normed, padded, filtered, activated, hidden, own_in, own_mid,
    own_stats, peer_stats, mix_parts, stage, mix_peers, fed_parts, fed_stage, fed_peers,
    load_sems, y_send, y_recv, near_send, far_send, line_recv, last_recv,
    twin_send, twin_recv, last_twin,
    in_send, in_recv, mid_send, mid_recv,
    stat_send, stat_recv, stage_send, stage_recv, mix_send, mix_recv, fed_send, fed_recv,
    fed_stage_send, fed_stage_recv, fed_pass_send,
):
    reps, n, tps, rows, channels, sub, ups = sizes
    ys = tps
    zs = n // ys
    members = reps * ys
    width = sub * tps
    own_width = sub * members
    shard = channels // n
    plane_shard = shard * ys
    tokens = reps * rows
    seqs = rows // LENGTH
    chunks = 3 + 2 * ups
    rep, fs, tp = lax.axis_index("rep"), lax.axis_index("fs"), lax.axis_index("tp")
    z, y = fs // ys, lax.rem(fs, ys)
    other_rep, other_y, other_tp = reps - 1 - rep, ys - 1 - y, tps - 1 - tp
    other_fs = z * ys + other_y
    own_group = rep * ys + y
    taps = conv_kernel.shape[0]
    blocks, _, block = mix_parts.shape
    per_tp = own_width // block

    third = tuple(range(3, 3 + ups))
    is_home = tp == y
    not_home = jnp.logical_not(is_home)
    fourth = tuple(range(3 + ups, chunks))
    per_plane = plane_shard // block
    has_next = (z < zs - 1, z > 0)
    next_fs = (fs + ys, fs - ys)
    def scoped(name):
        def wrap(f):
            def run(*args):
                with jax.named_scope("_".join([name, *(str(a) for a in args[:2] if isinstance(a, int))])):
                    return f(*args)
            return run
        return wrap

    barrier = pltpu.get_barrier_semaphore()
    for dr in range(reps):
        for dy in range(ys):
            for dt in range(tps):
                if dr or dy or dt:
                    pl.semaphore_signal(
                        barrier, inc=1,
                        device_id={
                            "rep": lax.rem(rep + dr, reps),
                            "fs": z * ys + lax.rem(y + dy, ys),
                            "tp": lax.rem(tp + dt, tps),
                        },
                        device_id_type=MESH,
                    )
    for way in range(2):
        @pl.when(has_next[way])
        def _():
            pl.semaphore_signal(
                barrier, inc=1, device_id={"fs": next_fs[way]}, device_id_type=MESH
            )

    def remote(src, dst, send, recv, **where):
        return pltpu.make_async_remote_copy(
            src_ref=src, dst_ref=dst, send_sem=send, recv_sem=recv,
            device_id=where, device_id_type=MESH,
        )

    def rows_of(index, size=shard):
        return pl.ds(pl.multiple_of(index * size, size), size)

    def rep_rows(r):
        return pl.ds(pl.multiple_of(r * rows, rows), rows)

    half = pl.ds(pl.multiple_of(tp * sub, sub), sub)

    def columns_of(c, group):
        if c < 3:
            source, at = (w_value, w_gate, w_mix)[c], group
        elif c < 3 + ups:
            source, at = w_up, group * ups + c - 3
        else:
            source, at = w_down, group * ups + c - 3 - ups
        return source.at[:, pl.ds(pl.multiple_of(at * sub, sub), sub)]

    loads = [
        pltpu.make_async_copy(
            columns_of(c, own_group), weights.at[c, rows_of(fs), half], load_sems.at[min(c, 3)]
        )
        for c in range(chunks)
    ]
    home_cols = pl.ds(pl.multiple_of(tp * own_width, own_width), own_width)
    own_load = pltpu.make_async_copy(states, own_in, load_sems.at[4])
    home_load = pltpu.make_async_copy(
        states, rows_in.at[rep_rows(rep), home_cols], load_sems.at[5]
    )
    small_loads = [
        pltpu.make_async_copy(source, target, load_sems.at[6 + k])
        for k, (source, target) in enumerate(
            (
                (mix_gain_in, mix_gain), (taps_in, conv_kernel), (chan_gain_in, chan_gain),
                (mlp_gain_in, mlp_gain),
            )
        )
    ]
    for c in range(chunks):
        loads[c].start()
    pl.when(is_home)(home_load.start)
    own_load.start()
    for one in small_loads:
        one.start()
    along_line = sum(jnp.where(has, 1, 0) for has in has_next)
    pl.semaphore_wait(barrier, reps * ys * tps - 1 + along_line)

    def across(c):
        return remote(
            columns_of(c, rep * ys + other_y), weights.at[c, rows_of(fs), half],
            y_send.at[0], y_recv.at[c], fs=other_fs,
        )

    middle = jnp.minimum(z, zs - 1 - z)

    def offset_at(i):
        low = 2 * z < zs - 1
        near = -(i + 1) // 2 if i % 2 else i // 2
        near = jnp.where(low, near, -near)
        far = jnp.where(low, i - middle, middle - i)
        return jnp.where(i <= 2 * middle, near, far)

    offsets = [offset_at(i) for i in range(zs)]
    planes = [z + off for off in offsets]

    def moved(chunk, span, send, recv, **where):
        at = weights.at[chunk, span, half]
        return remote(at, at, send, recv, **where)

    def batch_of(c):
        return 0 if c < 3 else 1 if c < 3 + ups else 2

    def group_of(c):
        return slice(0, 2) if c < 2 else c if c == 2 else slice(3, 3 + ups)

    def twin(c, i):
        return moved(
            c, rows_of(planes[i], plane_shard), twin_send.at[batch_of(c)], twin_recv.at[0 if c < 2 else min(c - 1, 2)],
            tp=other_tp,
        )

    halves = shard // LANES

    def half_rows(index, h):
        return rows_of(index * halves + h, LANES)

    def twin_last(c, i, b, h):
        return moved(
            c, half_rows(planes[i] * ys + b, h), twin_send.at[batch_of(c)], last_twin.at[i, b, h],
            tp=other_tp,
        )

    def ready(c):
        group = group_of(c)
        whole_half = weights.at[group, :, half]
        remote(
            whole_half, whole_half, twin_send.at[batch_of(c)], twin_recv.at[0 if c < 2 else min(c - 1, 2)], tp=other_tp
        ).wait_recv()

    def ready_last(i, b, h):
        moved(
            slice(3 + ups, chunks), half_rows(planes[i] * ys + b, h), twin_send.at[0],
            last_twin.at[i, b, h], tp=other_tp,
        ).wait_recv()

    def near(c, way, part):
        if c not in fourth:
            return [
                moved(
                    c, rows_of(z * ys + part), near_send.at[way], line_recv.at[c, z],
                    fs=next_fs[way],
                )
            ]
        return [
            moved(
                c, half_rows(z * ys + part, h), near_send.at[way], last_recv.at[z, part, h],
                fs=next_fs[way],
            )
            for h in range(halves)
        ]

    def send_near(c, part):
        for way in range(2):
            for one in near(c, way, part):
                pl.when(has_next[way])(one.start)

    @scoped("begin")
    def begin(c):
        if c < 3:
            loads[c].wait()
        elif c == 3:
            at = weights.at[3:, rows_of(fs), half]
            pltpu.make_async_copy(at, at, load_sems.at[3]).wait()
        send_near(c, y)

    @scoped("own")
    def own(c):
        across(c).wait_recv()
        send_near(c, other_y)
        if c in fourth:
            for b in range(ys):
                for h in range(halves):
                    twin_last(c, 0, b, h).start()
        else:
            twin(c, 0).start()

    goes = [jnp.where(off < 0, z < zs - 1, z > 0) for off in offsets]

    def onward(chunk, i, span, recv):
        to = jnp.where(offsets[i] < 0, fs + ys, fs - ys)
        return moved(chunk, span, far_send.at[i - 1], recv, fs=to)

    @scoped("arrive")
    def arrive(c, i):
        copy = onward(c, i, rows_of(planes[i], plane_shard), line_recv.at[c, planes[i]])
        copy.wait_recv()
        pl.when(goes[i])(copy.start)
        twin(c, i).start()

    @scoped("arrive_last")
    def arrive_last(i, b, h):
        span, recv = half_rows(planes[i] * ys + b, h), last_recv.at[planes[i], b, h]
        copy = onward(slice(3 + ups, chunks), i, span, recv)
        copy.wait_recv()
        for c in fourth:
            pl.when(goes[i])(onward(c, i, span, recv).start)
        for c in fourth:
            twin_last(c, i, b, h).start()

    @scoped("drain")
    def drain(k):
        batch = slice((0, 3, 3 + ups)[k], (3, 3 + ups, chunks)[k])
        moved(batch, slice(None), twin_send.at[k], twin_recv.at[0], tp=other_tp).wait_send()

    @scoped("drain_all")
    def drain_all():
        every = slice(None)
        moved(every, rows_of(fs), y_send.at[0], y_recv.at[0], fs=other_fs).wait_send()
        for way in range(2):
            copy = moved(
                every, rows_of(z, plane_shard), near_send.at[way], y_recv.at[0], fs=next_fs[way]
            )
            pl.when(has_next[way])(copy.wait_send)
        for i in range(1, zs):
            copy = onward(every, i, rows_of(planes[i], plane_shard), y_recv.at[0])
            pl.when(goes[i])(copy.wait_send)

    def spread(source, target, send, recv, over_from):
        def at(r, h, j):
            start = pl.multiple_of(h * own_width + j * block, block)
            return target.at[rep_rows(r), pl.ds(start, block)]

        def copies(j):
            if isinstance(j, slice):
                src, dst, j = source, target.at[rep_rows(rep), home_cols], 0
            else:
                src, dst = source.at[:, j * block : (j + 1) * block], at(rep, tp, j)
            along = remote(src, dst, send.at[0], recv.at[1, tp, j], rep=other_rep, tp=y)
            over = remote(src, dst, send.at[1], recv.at[0, tp, j], fs=other_fs, tp=y)
            inside = remote(src, dst, send.at[2], recv.at[0, tp, j], tp=y)
            return along, over, inside

        def passing(h, j):
            if h == 0 and j >= over_from:
                one = at(other_rep, 0, j)
                return remote(one, one, send.at[3], recv.at[1, 0, j], fs=other_fs)
            two = at(rep, h, j)
            return remote(two, two, send.at[3 + h], recv.at[1, h, j], rep=other_rep)

        def arrival(dr, h, j):
            dst = at(rep if dr == 0 else other_rep, h, j)
            return remote(dst, dst, send.at[0], recv.at[dr, h, j], rep=other_rep)

        def start(j):
            along, over, inside = copies(j)
            along.start()
            over.start()
            pl.when(jnp.logical_not(is_home))(inside.start)

        @scoped("forward")
        def forward(j):
            if j >= over_from:
                @pl.when(is_home)
                def _():
                    arrival(1, 0, j).wait_recv()
                    passing(0, j).start()

            @pl.when(jnp.logical_not(is_home))
            def _():
                for h in range(tps):
                    if h or j < over_from:
                        arrival(0, h, j).wait_recv()
                        passing(h, j).start()

        @scoped("finish")
        def finish(j):
            arrival(1, 1, j).wait_recv()

            @pl.when(is_home)
            def _():
                arrival(0, other_tp, j).wait_recv()
                if j < over_from:
                    arrival(1, 0, j).wait_recv()

            @pl.when(jnp.logical_not(is_home))
            def _():
                arrival(1, 0, j).wait_recv()
                if j >= over_from:
                    arrival(0, 0, j).wait_recv()

        def settle():
            along, over, inside = copies(slice(None))
            along.wait_send()
            over.wait_send()
            pl.when(not_home)(inside.wait_send)

            def part(k, blocks_sent):
                if blocks_sent:
                    sent = target.at[rep_rows(rep), : blocks_sent * block]
                    remote(sent, sent, send.at[k], recv.at[0, 0, 0], fs=other_fs).wait_send()

            pl.when(is_home)(functools.partial(part, 3, per_tp - over_from))

            @pl.when(not_home)
            def _():
                part(3, over_from)
                part(4, per_tp)

        return start, forward, finish, settle

    @scoped("norm")
    def norm_all(source, gain):
        def one(i, carry):
            span = pl.ds(pl.multiple_of(i * 64, 64), 64)
            x = source[span, :].astype(jnp.float32)
            scale = lax.rsqrt(jnp.mean(x * x, axis=-1, keepdims=True) + EPS)
            normed[span, :] = (x * scale * gain[...]).astype(jnp.bfloat16)
            return carry

        lax.fori_loop(0, tokens // 64, one, 0)

    def seq_rows(i):
        return pl.ds(pl.multiple_of(i * LENGTH, LENGTH), LENGTH)

    def mixer_rows(i):
        x = normed[seq_rows(i), :]
        value = jnp.dot(x, weights[0], preferred_element_type=jnp.float32)
        gate = jnp.dot(x, weights[1], preferred_element_type=jnp.float32)
        padded[LEAD : LEAD + LENGTH, :] = value * jax.nn.sigmoid(gate)
        per_sub = sub // LANES

        def column(j, sums):
            cols = pl.ds(pl.multiple_of(j * LANES, LANES), LANES)
            from_all = pl.multiple_of(
                (j // per_sub) * own_width + own_group * sub + lax.rem(j, per_sub) * LANES, LANES
            )
            kern = conv_kernel[:, pl.ds(from_all, LANES)]
            total = jnp.zeros((LENGTH, LANES), jnp.float32)
            for tap in range(taps):
                begin = LEAD - (taps - 1) + tap
                total = total + kern[tap : tap + 1, :] * padded[begin : begin + LENGTH, cols]
            filtered[seq_rows(i), cols] = total
            return sums[0] + total, sums[1] + total * total

        zero = jnp.zeros((LENGTH, LANES), jnp.float32)
        one, two = lax.fori_loop(0, width // LANES, column, (zero, zero))
        lane = lax.broadcasted_iota(jnp.int32, (LENGTH, LANES), 1)
        both = jnp.where(
            lane == 0,
            jnp.sum(one, axis=-1, keepdims=True),
            jnp.where(lane == 1, jnp.sum(two, axis=-1, keepdims=True), 0.0),
        )
        own_stats[i // seqs, :, seq_rows(lax.rem(i, seqs))] = both.T[0:8, :]

    def stat_copies(r):
        return [
            remote(
                own_stats.at[r], peer_stats.at[dr * ys + dy, r], stat_send.at[r],
                stat_recv.at[r],
                rep=lax.rem(rep + dr, reps), fs=z * ys + lax.rem(y + dy, ys),
            )
            for dr in range(reps) for dy in range(ys) if dr or dy
        ]

    def stat_waits(r):
        at = peer_stats.at[1:, r]
        return remote(at, at, stat_send.at[r], stat_recv.at[r], rep=other_rep)

    def activate_rows(i, carry):
        within = seq_rows(lax.rem(i, seqs))
        total = own_stats[i // seqs, :, within]
        for k in range(1, members):
            total = total + peer_stats[k, i // seqs, :, within]
        turned = jnp.concatenate([total] * (LANES // 8), axis=0).T
        mean = turned[:, 0:1] / channels
        variance = turned[:, 1:2] / channels - mean * mean
        gain = jnp.concatenate(
            [
                chan_gain[:, pl.ds(pl.multiple_of(t * own_width + own_group * sub, sub), sub)]
                for t in range(tps)
            ],
            axis=1,
        )
        x = (filtered[seq_rows(i), :] - mean) * lax.rsqrt(variance + EPS) * gain
        activated[seq_rows(i), :] = (x / (1.0 + jnp.exp(-x))).astype(jnp.bfloat16)
        return carry

    @scoped("share")
    def share(o, dr, part, left, pieces_of, parts, peers, send, recv):
        to = lax.rem(rep + dr, reps)
        first, size = part
        span = pl.ds(pl.multiple_of(o * block + first, size), size)
        cols = pl.ds(first, size)
        keeper, kept = o // per_tp, lax.rem(o, per_tp)
        at = rep_rows(to)
        total = None
        for k, c in enumerate(pieces_of):
            term = times_transposed(left[at, k * width : (k + 1) * width], weights[c, span, :])
            total = term if total is None else total + term
        parts[o, at, cols] = total.astype(jnp.bfloat16)
        slot = lax.rem(rep + reps - to, reps) * ys + lax.rem(y + ys - tp, ys)
        copy = remote(
            parts.at[o, at, cols], peers.at[slot, kept, :, cols], send.at[dr], recv.at[kept],
            rep=to, fs=z * ys + tp, tp=keeper,
        )
        here = jnp.logical_and(is_home, jnp.logical_and(keeper == tp, to == rep))
        pl.when(jnp.logical_not(here))(copy.start)

    def along_first(o):
        return o % 2 == 0

    def stage_copy(o, r):
        if along_first(o):
            return remote(
                mix_parts.at[o, rep_rows(other_rep), :], stage.at[o, 0], stage_send.at[0],
                stage_recv.at[o], rep=other_rep,
            )
        return remote(
            mix_parts.at[o, rep_rows(r), :], stage.at[o, r], stage_send.at[1],
            stage_recv.at[o], fs=z * ys + tp,
        )

    def last_copies(o):
        keeper, kept = o // per_tp, o % per_tp
        own_part = mix_parts.at[o, rep_rows(rep), :]
        inside = remote(
            own_part, mix_peers.at[0, kept], mix_send.at[0], mix_recv.at[kept], tp=keeper
        )
        if along_first(o):
            outside = remote(
                own_part, mix_peers.at[1, kept], mix_send.at[1], mix_recv.at[kept],
                fs=z * ys + tp, tp=keeper,
            )
        else:
            outside = remote(
                mix_parts.at[o, rep_rows(other_rep), :], mix_peers.at[1, kept],
                mix_send.at[1], mix_recv.at[kept], rep=other_rep, tp=keeper,
            )
        inner_one = jnp.logical_and(is_home, tp != keeper)
        return inside, inner_one, outside, not_home if along_first(o) else is_home

    @scoped("mix_share")
    def mix_share(o, r):
        at = rep_rows(r)
        mix_parts[o, at, :] = times_transposed(
            activated[at, :], weights[2, o * block : (o + 1) * block, :]
        ).astype(jnp.bfloat16)
        pl.when(rep != r if along_first(o) else not_home)(stage_copy(o, r).start)

    def mix_add(o, at, k):
        total = mix_parts[o, at, :].astype(jnp.float32) + stage[o, k].astype(jnp.float32)
        mix_parts[o, at, :] = total.astype(jnp.bfloat16)

    @scoped("combine")
    def combine(o):
        keeper, kept = o // per_tp, o % per_tp
        inside, inner_one, outside, outer_one = last_copies(o)

        def pass_on():
            pl.when(outer_one)(outside.start)
            pl.when(inner_one)(inside.start)

            @pl.when(jnp.logical_and(is_home, tp == keeper))
            def _():
                mix_peers[0, kept] = mix_parts[o, rep_rows(rep), :]

        if along_first(o):
            stage_copy(o, 0).wait_recv()
            mix_add(o, rep_rows(rep), 0)
            pass_on()
        else:
            @pl.when(is_home)
            def _():
                both = stage.at[o]
                remote(both, both, stage_send.at[1], stage_recv.at[o], fs=other_fs).wait_recv()
                for r in range(reps):
                    mix_add(o, rep_rows(r), r)
                pass_on()

    @scoped("mix_final")
    def mix_final(j):
        def some(start):
            at = mix_peers.at[start:, j]
            return remote(at, at, mix_send.at[0], mix_recv.at[j], rep=other_rep)

        pl.when(is_home)(some(1).wait_recv)
        pl.when(not_home)(some(0).wait_recv)
        return mix_peers[0, j].astype(jnp.float32) + mix_peers[1, j].astype(jnp.float32)

    def mix_settle():
        def sent(count, send):
            at = mix_parts.at[:count, rep_rows(rep), :]
            return remote(at, at, send, mix_recv.at[0], rep=other_rep)

        even = sum(1 for o in range(blocks) if along_first(o))
        sent(even, stage_send.at[0]).wait_send()
        pl.when(not_home)(sent((blocks - even) * reps, stage_send.at[1]).wait_send)
        pl.when(is_home)(sent(per_tp, mix_send.at[0]).wait_send)
        pl.when(not_home)(sent(even, mix_send.at[1]).wait_send)
        pl.when(is_home)(sent(blocks - even, mix_send.at[1]).wait_send)

    @scoped("peers")
    def wait_peers(j, parts, peers, send, recv):
        def some(start, stop):
            at = peers.at[start:stop, j]
            return remote(at, at, send.at[0], recv.at[j], rep=other_rep)

        direct = (tp * per_tp + j) // ys == planes[zs - 1]
        for is_direct, stop in ((direct, members), (jnp.logical_not(direct), 2)):
            pl.when(jnp.logical_and(is_home, is_direct))(some(1, stop).wait_recv)
            pl.when(jnp.logical_and(not_home, is_direct))(some(0, stop).wait_recv)

        @pl.when(is_home)
        def _():
            peers[0, j] = parts[tp * per_tp + j, rep_rows(rep), :]

        return direct

    def term_of(o, dr, part, k, c, left):
        at = rep_rows(lax.rem(rep + dr, reps))
        span = pl.ds(pl.multiple_of(o * block + part[0], part[1]), part[1])
        return times_transposed(left[at, k * width : (k + 1) * width], weights[c, span, :])

    def fed_stage_copy(i, b, r):
        o, k = planes[i] * ys + b, i * ys + b
        if b % 2 == 0:
            return remote(
                fed_parts.at[o, rep_rows(other_rep), :], fed_stage.at[k, 0],
                fed_stage_send.at[0], fed_stage_recv.at[k], rep=other_rep,
            )
        return remote(
            fed_parts.at[o, rep_rows(r), :], fed_stage.at[k, r],
            fed_stage_send.at[1], fed_stage_recv.at[k], fs=z * ys + tp,
        )

    @scoped("fed_share")
    def fed_share(i, b):
        o = planes[i] * ys + b
        for dr in (*range(1, reps), 0):
            to = lax.rem(rep + dr, reps)
            total = None
            for k, c in enumerate(fourth):
                term = term_of(o, dr, (0, block), k, c, hidden)
                total = term if total is None else total + term
            fed_parts[o, rep_rows(to), :] = total.astype(jnp.bfloat16)
            if b % 2:
                pl.when(not_home)(fed_stage_copy(i, b, to).start)
            elif dr:
                fed_stage_copy(i, b, to).start()

    @scoped("fed_combine")
    def fed_combine(i, b):
        o, k = planes[i] * ys + b, i * ys + b
        keeper, kept = o // per_tp, lax.rem(o, per_tp)
        own_part = fed_parts.at[o, rep_rows(rep), :]
        inside = remote(
            own_part, fed_peers.at[0, kept], fed_pass_send.at[0], fed_recv.at[kept], tp=keeper
        )

        def add(r, slot):
            at = rep_rows(r)
            total = fed_parts[o, at, :].astype(jnp.float32) + fed_stage[k, slot].astype(
                jnp.float32
            )
            fed_parts[o, at, :] = total.astype(jnp.bfloat16)

        if b % 2 == 0:
            fed_stage_copy(i, b, 0).wait_recv()
            add(rep, 0)
            outside = remote(
                own_part, fed_peers.at[1, kept], fed_pass_send.at[1], fed_recv.at[kept],
                fs=z * ys + tp, tp=keeper,
            )
            pl.when(not_home)(outside.start)
            pl.when(jnp.logical_and(is_home, keeper != tp))(inside.start)
        else:
            outside = remote(
                fed_parts.at[o, rep_rows(other_rep), :], fed_peers.at[1, kept],
                fed_pass_send.at[1], fed_recv.at[kept], rep=other_rep, tp=keeper,
            )

            @pl.when(is_home)
            def _():
                both = fed_stage.at[k]
                remote(
                    both, both, fed_stage_send.at[1], fed_stage_recv.at[k], fs=other_fs
                ).wait_recv()
                for r in range(reps):
                    add(r, r)
                outside.start()
                pl.when(keeper != tp)(inside.start)

    def settle_share(parts, send, recv):
        def sent(count, sem):
            at = parts.at[:count, rep_rows(rep), :]
            return remote(at, at, sem, recv.at[0], rep=other_rep).wait_send

        last_away = planes[zs - 1] * ys // per_tp != tp
        last_here = jnp.logical_not(last_away)
        for dr in range(1, reps):
            sent(ys, send.at[dr])()
        pl.when(jnp.logical_or(not_home, last_away))(sent(ys, send.at[0]))
        sent(zs - 1, fed_stage_send.at[0])()
        pl.when(not_home)(sent((zs - 1) * reps, fed_stage_send.at[1]))
        sent(zs - 1, fed_pass_send.at[1])()
        if per_tp > ys:
            pl.when(jnp.logical_and(is_home, last_away))(sent(per_tp - ys, fed_pass_send.at[0]))
        pl.when(jnp.logical_and(is_home, last_here))(sent(per_tp, fed_pass_send.at[0]))

    def total_of(j, peers, count):
        total = peers[0, j].astype(jnp.float32)
        for k in range(1, count):
            total = total + peers[k, j].astype(jnp.float32)
        return total

    start_in, forward_in, finish_in, settle_in = spread(
        states, rows_in, in_send, in_recv, per_tp // 2
    )
    start_mid, forward_mid, finish_mid, settle_mid = spread(
        own_mid, rows_mid, mid_send, mid_recv, 0
    )

    def inner(*todo):
        @pl.when(middle > 0)
        def _():
            for one in todo:
                one()

    def outer(*todo):
        @pl.when(middle == 0)
        def _():
            for one in todo:
                one()

    def pump(c, i):
        return functools.partial(arrive, c, i)

    def all_of(c):
        return [pump(c, i) for i in range(1, zs)]

    def whole(c):
        return [functools.partial(begin, c), functools.partial(own, c)]

    across(0).start()
    across(1).start()
    begin(0)
    begin(1)
    for j in range(per_tp):
        start_in(j)
    own(0)
    own(1)
    across(2).start()
    across(3).start()
    begin(2)
    padded[0:LEAD, :] = jnp.zeros((LEAD, width), jnp.float32)
    arrive(0, 1)
    inner(pump(0, 2))
    arrive(1, 1)
    inner(pump(1, 2))
    forward_in(0)
    for j in range(1, per_tp // 2):
        forward_in(j)
    inner(*[pump(c, i) for i in range(3, zs) for c in (0, 1)])
    for j in range(per_tp // 2, per_tp):
        forward_in(j)
    own(2)
    outer(*[pump(c, 2) for c in (0, 1)])
    for j in range(per_tp):
        finish_in(j)
    for c in range(4, chunks):
        across(c).start()
    pl.when(is_home)(home_load.wait)
    for one in small_loads:
        one.wait()
    norm_all(rows_in, mix_gain)
    outer(*[pump(c, i) for i in range(3, zs) for c in (0, 1)])
    ready(0)

    inner(*all_of(2)[:1], functools.partial(begin, 3))
    outer(*whole(3))
    inside = [
        all_of(2)[1:2], all_of(2)[2:] + [functools.partial(own, 3)], whole(4), [],
    ]
    outside = [whole(4), whole(5), whole(fourth[0]), sum([whole(c) for c in fourth[1:]], [])]
    for r in range(reps):
        for cut in ((0, (seqs + 1) // 2), ((seqs + 1) // 2, seqs)):
            with jax.named_scope("mixer"):
                lax.fori_loop(
                    r * seqs + cut[0], r * seqs + cut[1],
                    lambda k, carry: (mixer_rows(k), carry)[1], 0,
                )
            if inside:
                inner(*inside.pop(0))
                outer(*outside.pop(0))
        for one in stat_copies(r):
            one.start()
    outer(*all_of(2))
    ready(2)
    for r in range(reps):
        with jax.named_scope("stats"):
            stat_waits(r).wait_recv()
        with jax.named_scope("activate"):
            lax.fori_loop(r * seqs, (r + 1) * seqs, activate_rows, 0)
        for j in range(per_tp):
            for t in range(tps):
                mix_share(t * per_tp + j, r)

    own_load.wait()
    inner(*whole(5), *all_of(3)[:2], *whole(fourth[0]))
    def last(i, b):
        return [functools.partial(arrive_last, i, b, h) for h in range(halves)]

    early = [
        all_of(3)[2:] + all_of(4)[:2],
        all_of(4)[2:] + all_of(5)[:2],
        all_of(5)[2:] + sum([whole(c) for c in fourth[1:]], []),
    ]
    late = [[], all_of(3), all_of(4)[:1], all_of(4)[1:]]
    for t in range(tps):
        combine(t * per_tp)
    for j in range(per_tp):
        if j + 1 < per_tp:
            for t in range(tps):
                combine(t * per_tp + j + 1)
        mixed = mix_final(j)
        cols = slice(j * block, (j + 1) * block)
        own_mid[:, cols] = (own_in[:, cols].astype(jnp.float32) + mixed).astype(jnp.bfloat16)
        start_mid(j)

        @pl.when(is_home)
        def _():
            start = pl.multiple_of(tp * own_width + j * block, block)
            rows_mid[rep_rows(rep), pl.ds(start, block)] = own_mid[:, cols]

        if j:
            forward_mid(j - 1)
        if j < len(early):
            inner(*early[j])
        if j == per_tp - 1:
            forward_mid(j)
            inner(*[one for b in range(ys) for one in last(1, b)])
        if j < len(late):
            outer(*late[j])
    for rest in early[per_tp:]:
        inner(*rest)
    for rest in late[per_tp:]:
        outer(*rest)
    for j in range(per_tp):
        finish_mid(j)
    outer(*all_of(5))
    inner(*last(2, 0))
    norm_all(rows_mid, mlp_gain)
    ready(3)

    @scoped("up")
    def up_some(k):
        def up_rows(i, carry):
            at = rep_rows(i)
            x = jnp.dot(normed[at, :], weights[3 + k], preferred_element_type=jnp.float32)
            x = jnp.maximum(x, 0.0)
            hidden[at, k * width : (k + 1) * width] = (x * x).astype(jnp.bfloat16)
            return carry

        lax.fori_loop(0, reps, up_rows, 0)

    for k in range(ups):
        up_some(k)
    pending = []
    fed = (hidden, fourth, fed_parts, fed_peers, fed_send, fed_recv)
    settle_in()
    settle_mid()
    mix_settle()
    for r in range(reps):
        stat_waits(r).wait_send()
    for i in range(zs):
        for b in range(ys):
            if i == 0 and b:
                inner(*last(2, b))
            if 0 < i < zs - 2:
                inner(*last(i + 2, b))
            if i < zs - 1:
                if i:
                    outer(*last(i, b))
                for h in range(halves):
                    ready_last(i, b, h)
                fed_share(i, b)
                pending.append((i, b))
                if len(pending) > 3:
                    fed_combine(*pending.pop(0))
            else:
                for h in range(halves):
                    outer(last(i, b)[h])
                    ready_last(i, b, h)
                    for dr in (*range(1, reps), 0):
                        share(planes[i] * ys + b, dr, (h * LANES, LANES), *fed)
                    if pending:
                        fed_combine(*pending.pop(0))
            if i == 1 and b == 0:
                drain(0)
                drain(1)
    while pending:
        fed_combine(*pending.pop(0))
    for j in range(per_tp):
        if j == per_tp - 1:
            drain(2)
            drain_all()
        direct = wait_peers(j, fed_parts, fed_peers, fed_send, fed_recv)
        cols = slice(j * block, (j + 1) * block)
        with jax.named_scope("out"):
            for is_direct, count in ((direct, members), (jnp.logical_not(direct), 2)):
                @pl.when(is_direct)
                def _():
                    out[:, cols] = (
                        own_mid[:, cols].astype(jnp.float32) + total_of(j, fed_peers, count)
                    ).astype(jnp.bfloat16)
    with jax.named_scope("done"):
        settle_share(fed_parts, fed_send, fed_recv)


def plane_body(mesh, states, mix_gain, w_value, w_gate, conv_kernel, chan_gain, w_mix, mlp_gain, w_up, w_down):
    reps, n, tps = mesh.shape["rep"], mesh.shape["fs"], mesh.shape["tp"]
    rows, own_width = states.shape
    ys = tps
    zs, members = n // ys, reps * ys
    sub = own_width // members
    width = sub * tps
    channels = own_width * tps
    ups = w_up.shape[1] // own_width
    tokens = rows * reps
    block = channels // n
    halves = block // LANES
    blocks, per_tp = channels // block, own_width // block
    chunks = 3 + 2 * ups
    bf16, f32 = jnp.bfloat16, jnp.float32
    vmem, hbm = pl.BlockSpec(memory_space=pltpu.VMEM), pl.BlockSpec(memory_space=pl.ANY)
    dma = pltpu.SemaphoreType.DMA
    return pl.pallas_call(
        functools.partial(plane_kernel, (reps, n, tps, rows, channels, sub, ups)),
        out_shape=pltpu.VMEM((rows, own_width), bf16),
        in_specs=[hbm] * 10,
        out_specs=vmem,
        scratch_shapes=[
            pltpu.VMEM((1, channels), f32),
            pltpu.VMEM(conv_kernel.shape, f32),
            pltpu.VMEM((1, channels), f32),
            pltpu.VMEM((1, channels), f32),
            pltpu.VMEM((chunks, channels, width), bf16),
            pltpu.VMEM((tokens, channels), bf16),
            pltpu.VMEM((tokens, channels), bf16),
            pltpu.VMEM((tokens, channels), bf16),
            pltpu.VMEM((LEAD + LENGTH, width), f32),
            pltpu.VMEM((tokens, width), f32),
            pltpu.VMEM((tokens, width), bf16),
            pltpu.VMEM((tokens, ups * width), bf16),
            pltpu.VMEM((rows, own_width), bf16),
            pltpu.VMEM((rows, own_width), bf16),
            pltpu.VMEM((reps, 8, rows), f32),
            pltpu.VMEM((members, reps, 8, rows), f32),
            pltpu.VMEM((blocks, tokens, block), bf16),
            pltpu.VMEM((blocks, reps, rows, block), bf16),
            pltpu.VMEM((2, per_tp, rows, block), bf16),
            pltpu.VMEM((blocks, tokens, block), bf16),
            pltpu.VMEM(((zs - 1) * ys, reps, rows, block), bf16),
            pltpu.VMEM((members, per_tp, rows, block), bf16),
            dma((10,)),
            dma((1,)),
            dma((chunks,)),
            dma((2,)),
            dma((zs - 1,)),
            dma((3 + ups, zs)),
            dma((zs, ys, halves)),
            dma((3,)),
            dma((3,)),
            dma((zs, ys, halves)),
            dma((5,)),
            dma((reps, tps, per_tp)),
            dma((5,)),
            dma((reps, tps, per_tp)),
            dma((reps,)),
            dma((reps,)),
            dma((2,)),
            dma((blocks,)),
            dma((2,)),
            dma((per_tp,)),
            dma((reps,)),
            dma((per_tp,)),
            dma((2,)),
            dma(((zs - 1) * ys,)),
            dma((2,)),
        ],
        compiler_params=pltpu.CompilerParams(
            collective_id=0, has_side_effects=True, vmem_limit_bytes=56 * 1024 * 1024
        ),
    )(
        states, mix_gain[None, :], w_value, w_gate, conv_kernel, chan_gain[None, :], w_mix,
        mlp_gain[None, :], w_up, w_down,
    )


def body(mesh, states, *weights):
    reps, n, tps = mesh.shape["rep"], mesh.shape["fs"], mesh.shape["tp"]
    own_width = states.shape[1]
    channels = own_width * tps
    planar = (
        reps == tps == 2
        and n % tps == 0
        and n // tps > 2
        and own_width % (reps * tps * LANES) == 0
        and channels % (n * LANES) == 0
        and own_width % (tps * (channels // n)) == 0
    )
    return (plane_body if planar else ring_body)(mesh, states, *weights)


def solution(mesh):
    in_specs = (
        P(("rep", "fs"), "tp"),
        P(),
        P("fs", "tp"),
        P("fs", "tp"),
        P(),
        P(),
        P("fs", "tp"),
        P(),
        P("fs", "tp"),
        P("fs", "tp"),
    )
    out_specs = P(("rep", "fs"), "tp")
    return jax.shard_map(
        functools.partial(body, mesh),
        mesh=mesh, in_specs=in_specs, out_specs=out_specs, check_vma=False,
    )
```

```python
import functools

import jax
import jax.numpy as jnp
from jax import lax
from jax.experimental import pallas as pl
from jax.experimental.pallas import tpu as pltpu
from jax.sharding import PartitionSpec as P

LENGTH = 128
LANES = 128
LEAD = 32
EPS = 1e-06
MESH = pl.DeviceIdType.MESH


def times_transposed(left, right):
    return lax.dot_general(
        left, right, (((1,), (1,)), ((), ())), preferred_element_type=jnp.float32
    )


def ring_kernel(
    sizes,
    states, mix_gain, w_value, w_gate, conv_kernel, chan_gain, w_mix, mlp_gain, w_up, w_down,
    out,
    weights, rows_in, rows_mid, normed, padded, filtered, activated, hidden,
    own_stats, peer_stats, mix_parts, mix_peers, fed_parts, fed_peers,
    load_sems, ring_send, ring_recv, in_send, in_recv, mid_send, mid_recv,
    stat_send, stat_recv, mix_send, mix_recv, fed_send, fed_recv,
):
    reps, n, tps, rows, channels, width, ups = sizes
    own_width = width * reps
    half_way = n // 2
    shard = channels // n
    tokens = reps * rows
    pieces = tokens // LENGTH
    chunks = 3 + 2 * ups
    rep, fs, tp = lax.axis_index("rep"), lax.axis_index("fs"), lax.axis_index("tp")
    taps = conv_kernel.shape[0]
    blocks, _, block = mix_parts.shape
    per_tp = own_width // block

    def ring_index(place):
        place = lax.rem(place + n, n)
        return jnp.where(place < half_way, 2 * place, 2 * (n - 1 - place) + 1)

    place = jnp.where(lax.rem(fs, 2) == 0, fs // 2, n - 1 - fs // 2)
    neighbours = (ring_index(place + 1), ring_index(place - 1))

    barrier = pltpu.get_barrier_semaphore()
    for other in neighbours:
        pl.semaphore_signal(barrier, inc=1, device_id={"fs": other}, device_id_type=MESH)
    for dr in range(reps):
        for dt in range(tps):
            if dr or dt:
                pl.semaphore_signal(
                    barrier, inc=1,
                    device_id={"rep": lax.rem(rep + dr, reps), "tp": lax.rem(tp + dt, tps)},
                    device_id_type=MESH,
                )

    own_rows = pl.ds(pl.multiple_of(rep * rows, rows), rows)
    own_cols = pl.ds(pl.multiple_of(tp * own_width, own_width), own_width)

    def shard_at(owner, start=0, size=None):
        size = shard if size is None else size
        return pl.ds(pl.multiple_of(owner * shard + start, size), size)

    def hop(c, s, way):
        sign = 1 if way == 0 else -1
        owner = ring_index(place - sign * (s - 1))
        span = shard_at(owner)
        if s == half_way:
            span = shard_at(owner, way * (shard // 2), shard // 2)
        return pltpu.make_async_remote_copy(
            src_ref=weights.at[c, span, :],
            dst_ref=weights.at[c, span, :],
            send_sem=ring_send.at[way, c],
            recv_sem=ring_recv.at[way, c, s - 1],
            device_id={"fs": neighbours[way]},
            device_id_type=MESH,
        )

    loads = []
    for c in range(chunks):
        if c < 3:
            source, column = (w_value, w_gate, w_mix)[c], rep * width
        elif c < 3 + ups:
            source, column = w_up, (rep * ups + c - 3) * width
        else:
            source, column = w_down, (rep * ups + c - 3 - ups) * width
        loads.append(
            pltpu.make_async_copy(
                source.at[:, pl.ds(pl.multiple_of(column, width), width)],
                weights.at[c, shard_at(fs), :],
                load_sems.at[c],
            )
        )
        loads[-1].start()
    own_load = pltpu.make_async_copy(states, rows_in.at[own_rows, own_cols], load_sems.at[chunks])
    own_load.start()
    pl.semaphore_wait(barrier, 1 + reps * tps)

    def pump(c, s):
        for way in range(2):
            if s == 1:
                if way == 0:
                    loads[c].wait()
            else:
                before = hop(c, s - 1, way)
                before.wait_recv()
                before.wait_send()
            hop(c, s, way).start()

    def arrived(c):
        for way in range(2):
            last = hop(c, half_way, way)
            last.wait_recv()
            last.wait_send()

    def spread(source, target, send, recv):
        def copy(dr, dt, ahead):
            if ahead:
                span = pl.ds(pl.multiple_of(lax.rem(rep + reps - dr, reps) * rows, rows), rows)
                src = target.at[span, own_cols]
            else:
                span, src = own_rows, source
            step_r = 0 if ahead else dr
            return pltpu.make_async_remote_copy(
                src_ref=src,
                dst_ref=target.at[span, own_cols],
                send_sem=send.at[dr, dt],
                recv_sem=recv.at[dr, dt],
                device_id={"rep": lax.rem(rep + step_r, reps), "tp": lax.rem(tp + dt, tps)},
                device_id_type=MESH,
            )

        first = [copy(dr, 0, False) for dr in range(1, reps)]
        near = [copy(0, dt, False) for dt in range(1, tps)]
        for one in first + near:
            one.start()

        def forward():
            later = []
            for dr in range(1, reps):
                first[dr - 1].wait_recv()
                for dt in range(1, tps):
                    one = copy(dr, dt, True)
                    one.start()
                    later.append(one)
            return later

        def finish(later):
            for one in near + later:
                one.wait_recv()
            for one in first + near + later:
                one.wait_send()

        return forward, finish

    def norm_all(source, gain):
        def one(i, carry):
            span = pl.ds(pl.multiple_of(i * 64, 64), 64)
            x = source[span, :].astype(jnp.float32)
            scale = lax.rsqrt(jnp.mean(x * x, axis=-1, keepdims=True) + EPS)
            normed[span, :] = (x * scale * gain[...]).astype(jnp.bfloat16)
            return carry

        lax.fori_loop(0, tokens // 64, one, 0)

    def seq_rows(i):
        return pl.ds(pl.multiple_of(i * LENGTH, LENGTH), LENGTH)

    def mixer_rows(i):
        x = normed[seq_rows(i), :]
        value = jnp.dot(x, weights[0], preferred_element_type=jnp.float32)
        gate = jnp.dot(x, weights[1], preferred_element_type=jnp.float32)
        padded[LEAD : LEAD + LENGTH, :] = value * jax.nn.sigmoid(gate)

        def column(j, sums):
            cols = pl.ds(pl.multiple_of(j * LANES, LANES), LANES)
            from_all = pl.multiple_of(tp * own_width + rep * width + j * LANES, LANES)
            kern = conv_kernel[:, pl.ds(from_all, LANES)]
            total = jnp.zeros((LENGTH, LANES), jnp.float32)
            for tap in range(taps):
                begin = LEAD - (taps - 1) + tap
                total = total + kern[tap : tap + 1, :] * padded[begin : begin + LENGTH, cols]
            filtered[seq_rows(i), cols] = total
            return sums[0] + total, sums[1] + total * total

        zero = jnp.zeros((LENGTH, LANES), jnp.float32)
        one, two = lax.fori_loop(0, width // LANES, column, (zero, zero))
        lane = lax.broadcasted_iota(jnp.int32, (LENGTH, LANES), 1)
        both = jnp.where(
            lane == 0,
            jnp.sum(one, axis=-1, keepdims=True),
            jnp.where(lane == 1, jnp.sum(two, axis=-1, keepdims=True), 0.0),
        )
        own_stats[:, seq_rows(i)] = both.T[0:8, :]

    def stat_copies():
        copies = []
        for dr in range(reps):
            for dt in range(tps):
                if dr or dt:
                    copies.append(
                        pltpu.make_async_remote_copy(
                            src_ref=own_stats,
                            dst_ref=peer_stats.at[dr * tps + dt],
                            send_sem=stat_send.at[dr, dt],
                            recv_sem=stat_recv.at[dr, dt],
                            device_id={
                                "rep": lax.rem(rep + dr, reps),
                                "tp": lax.rem(tp + dt, tps),
                            },
                            device_id_type=MESH,
                        )
                    )
        return copies

    def activate_rows(i, carry):
        total = own_stats[:, seq_rows(i)]
        for k in range(1, reps * tps):
            total = total + peer_stats[k, :, seq_rows(i)]
        turned = jnp.concatenate([total] * (LANES // 8), axis=0).T
        mean = turned[:, 0:1] / channels
        variance = turned[:, 1:2] / channels - mean * mean
        gain_at = pl.multiple_of(tp * own_width + rep * width, LANES)
        gain = chan_gain[:, pl.ds(gain_at, width)]
        x = (filtered[seq_rows(i), :] - mean) * lax.rsqrt(variance + EPS) * gain
        activated[seq_rows(i), :] = (x / (1.0 + jnp.exp(-x))).astype(jnp.bfloat16)
        return carry

    def share(order, o, left, pieces_of, parts, peers, send, recv):
        span = pl.ds(pl.multiple_of(o * block, block), block)

        def one(i):
            at = pl.ds(pl.multiple_of(i * rows, rows), rows)
            total = None
            for k, c in enumerate(pieces_of):
                term = times_transposed(
                    left[at, k * width : (k + 1) * width], weights[c, span, :]
                )
                total = term if total is None else total + term
            parts[o, at, :] = total.astype(jnp.bfloat16)

        keeper = o // per_tp
        dt = lax.rem(keeper + tps - tp, tps)
        waits = []
        for dr in [*range(1, reps), 0]:
            to = lax.rem(rep + dr, reps)
            one(to)
            copy = pltpu.make_async_remote_copy(
                src_ref=parts.at[o, pl.ds(pl.multiple_of(to * rows, rows), rows), :],
                dst_ref=peers.at[dr * tps + dt, lax.rem(o, per_tp)],
                send_sem=send.at[order, dr],
                recv_sem=recv.at[dr * tps + dt, lax.rem(o, per_tp)],
                device_id={"rep": to, "tp": keeper},
                device_id_type=MESH,
            )
            if dr:
                copy.start()
                waits.append(copy.wait_send)
            else:
                pl.when(keeper != tp)(copy.start)
                waits.append(lambda k=keeper, c=copy: pl.when(k != tp)(c.wait_send))
        return waits

    def wait_peers(j, parts, peers, send, recv):
        for k in range(1, reps * tps):
            dr, dt = k // tps, k % tps
            pltpu.make_async_remote_copy(
                src_ref=parts.at[0, own_rows, :],
                dst_ref=peers.at[k, j],
                send_sem=send.at[0, 0],
                recv_sem=recv.at[k, j],
                device_id={"rep": lax.rem(rep + dr, reps), "tp": lax.rem(tp + dt, tps)},
                device_id_type=MESH,
            ).wait_recv()

    def total_of(j, parts, peers):
        total = parts[tp * per_tp + j, own_rows, :].astype(jnp.float32)
        for k in range(1, reps * tps):
            total = total + peers[k, j].astype(jnp.float32)
        return total

    stepwise = blocks == n

    def owners(s):
        if s in (0, half_way):
            return [ring_index(place + s)]
        return [ring_index(place - s), ring_index(place + s)]

    def steps_of(c):
        return range(1, half_way + 1)

    first, second = (0, 1), (2, 3)
    third = tuple(range(4, 3 + ups))
    fourth = tuple(range(3 + ups, chunks))

    pump(0, 1)
    pump(1, 1)
    forward, finish = spread(states, rows_in, in_send, in_recv)
    padded[0:LEAD, :] = jnp.zeros((LEAD, width), jnp.float32)
    pump(0, 2)
    pump(1, 2)
    later = forward()
    for s in range(3, half_way + 1):
        pump(0, s)
        if s == 3:
            own_load.wait()
            finish(later)
        pump(1, s)
        if s == 3:
            norm_all(rows_in, mix_gain)
    pump(2, 1)
    pump(3, 1)
    arrived(0)
    arrived(1)

    todo = [(c, s) for s in range(2, half_way + 1) for c in second]

    def next_hop():
        if todo:
            pump(*todo.pop(0))

    for i in range(0, pieces, 2):
        lax.fori_loop(
            i, min(i + 2, pieces), lambda k, carry: (mixer_rows(k), carry)[1], 0
        )
        next_hop()
    stats = stat_copies()
    for one in stats:
        one.start()
    for one in stats:
        one.wait_recv()
    lax.fori_loop(0, pieces, activate_rows, 0)
    waits = []
    mix = (activated, (2,), mix_parts, mix_peers, mix_send, mix_recv)
    if stepwise:
        for s in range(half_way - 1):
            for o in owners(s):
                waits += share(len(waits) // reps, o, *mix)
    while todo:
        next_hop()
    if stepwise:
        for o in owners(half_way - 1):
            waits += share(len(waits) // reps, o, *mix)
    for c in third:
        pump(c, 1)
    arrived(2)
    if stepwise:
        waits += share(len(waits) // reps, owners(half_way)[0], *mix)
    else:
        for o in range(blocks):
            waits += share(o, o, *mix)

    todo = [(c, s) for s in range(2, half_way + 1) for c in third]
    for _ in range(len(todo) // 2):
        next_hop()
    for j in range(per_tp):
        wait_peers(j, mix_parts, mix_peers, mix_send, mix_recv)
        at = pl.ds(pl.multiple_of(tp * own_width + j * block, block), block)
        rows_mid[own_rows, at] = (
            rows_in[own_rows, at].astype(jnp.float32) + total_of(j, mix_parts, mix_peers)
        ).astype(jnp.bfloat16)
    forward, finish = spread(rows_mid.at[own_rows, own_cols], rows_mid, mid_send, mid_recv)
    while todo:
        next_hop()
    for c in fourth:
        pump(c, 1)
    arrived(3)
    for c in third:
        arrived(c)
    later = forward()
    finish(later)
    norm_all(rows_mid, mlp_gain)
    todo = [(c, s) for s in range(2, half_way + 1) for c in fourth]
    next_hop()
    for k in range(ups):

        def up_rows(i, carry):
            at = pl.ds(pl.multiple_of(i * rows, rows), rows)
            x = jnp.dot(normed[at, :], weights[3 + k], preferred_element_type=jnp.float32)
            x = jnp.maximum(x, 0.0)
            hidden[at, k * width : (k + 1) * width] = (x * x).astype(jnp.bfloat16)
            return carry

        lax.fori_loop(0, reps, up_rows, 0)
        next_hop()
    done = []
    fed = (hidden, fourth, fed_parts, fed_peers, fed_send, fed_recv)
    if stepwise:
        for o in owners(0):
            done += share(len(done) // reps, o, *fed)
    for s in range(2, half_way + 1):
        while todo and todo[0][1] <= s:
            next_hop()
        if stepwise:
            for o in owners(s - 1):
                done += share(len(done) // reps, o, *fed)
    for c in fourth:
        arrived(c)
    if stepwise:
        done += share(len(done) // reps, owners(half_way)[0], *fed)
    else:
        for o in range(blocks):
            done += share(o, o, *fed)
    for j in range(per_tp):
        wait_peers(j, fed_parts, fed_peers, fed_send, fed_recv)
        at = pl.ds(pl.multiple_of(tp * own_width + j * block, block), block)
        out[:, j * block : (j + 1) * block] = (
            rows_mid[own_rows, at].astype(jnp.float32) + total_of(j, fed_parts, fed_peers)
        ).astype(jnp.bfloat16)
    for one in stats:
        one.wait_send()
    for wait in waits + done:
        wait()


def ring_body(mesh, states, mix_gain, w_value, w_gate, conv_kernel, chan_gain, w_mix, mlp_gain, w_up, w_down):
    reps, n, tps = mesh.shape["rep"], mesh.shape["fs"], mesh.shape["tp"]
    rows, own_width = states.shape
    width = own_width // reps
    channels = own_width * tps
    ups = w_up.shape[1] // own_width
    tokens = rows * reps
    group = reps * tps
    block = channels // n if channels // n >= LANES else own_width
    blocks, per_tp = channels // block, own_width // block
    chunks = 3 + 2 * ups
    bf16, f32 = jnp.bfloat16, jnp.float32
    vmem, hbm = pl.BlockSpec(memory_space=pltpu.VMEM), pl.BlockSpec(memory_space=pl.ANY)
    dma = pltpu.SemaphoreType.DMA
    return pl.pallas_call(
        functools.partial(ring_kernel, (reps, n, tps, rows, channels, width, ups)),
        out_shape=jax.ShapeDtypeStruct((rows, own_width), bf16),
        in_specs=[hbm, vmem, hbm, hbm, vmem, vmem, hbm, vmem, hbm, hbm],
        out_specs=vmem,
        scratch_shapes=[
            pltpu.VMEM((chunks, channels, width), bf16),
            pltpu.VMEM((tokens, channels), bf16),
            pltpu.VMEM((tokens, channels), bf16),
            pltpu.VMEM((tokens, channels), bf16),
            pltpu.VMEM((LEAD + LENGTH, width), f32),
            pltpu.VMEM((tokens, width), f32),
            pltpu.VMEM((tokens, width), bf16),
            pltpu.VMEM((tokens, ups * width), bf16),
            pltpu.VMEM((8, tokens), f32),
            pltpu.VMEM((group, 8, tokens), f32),
            pltpu.VMEM((blocks, tokens, block), bf16),
            pltpu.VMEM((group, per_tp, rows, block), bf16),
            pltpu.VMEM((blocks, tokens, block), bf16),
            pltpu.VMEM((group, per_tp, rows, block), bf16),
            dma((chunks + 1,)),
            dma((2, chunks)),
            dma((2, chunks, n // 2)),
            dma((reps, tps)),
            dma((reps, tps)),
            dma((reps, tps)),
            dma((reps, tps)),
            dma((reps, tps)),
            dma((reps, tps)),
            dma((blocks, reps)),
            dma((group, per_tp)),
            dma((blocks, reps)),
            dma((group, per_tp)),
        ],
        compiler_params=pltpu.CompilerParams(
            collective_id=0, has_side_effects=True, vmem_limit_bytes=62 * 1024 * 1024
        ),
    )(
        states, mix_gain[None, :], w_value, w_gate, conv_kernel, chan_gain[None, :], w_mix,
        mlp_gain[None, :], w_up, w_down,
    )


def plane_kernel(
    sizes,
    states, mix_gain_in, w_value, w_gate, taps_in, chan_gain_in, w_mix, mlp_gain_in, w_up, w_down,
    out,
    mix_gain, conv_kernel, chan_gain, mlp_gain,
    weights, rows_in, rows_mid, normed, padded, filtered, activated, hidden, own_in, own_mid,
    own_stats, peer_stats, mix_parts, stage, mix_peers, fed_parts, fed_stage, fed_peers,
    load_sems, y_send, y_recv, near_send, far_send, line_recv, last_recv,
    twin_send, twin_recv, last_twin,
    in_send, in_recv, mid_send, mid_recv,
    stat_send, stat_recv, stage_send, stage_recv, mix_send, mix_recv, fed_send, fed_recv,
    fed_stage_send, fed_stage_recv, fed_pass_send,
):
    reps, n, tps, rows, channels, sub, ups = sizes
    ys = tps
    zs = n // ys
    members = reps * ys
    width = sub * tps
    own_width = sub * members
    shard = channels // n
    plane_shard = shard * ys
    tokens = reps * rows
    seqs = rows // LENGTH
    chunks = 3 + 2 * ups
    rep, fs, tp = lax.axis_index("rep"), lax.axis_index("fs"), lax.axis_index("tp")
    z, y = fs // ys, lax.rem(fs, ys)
    other_rep, other_y, other_tp = reps - 1 - rep, ys - 1 - y, tps - 1 - tp
    other_fs = z * ys + other_y
    own_group = rep * ys + y
    taps = conv_kernel.shape[0]
    blocks, _, block = mix_parts.shape
    per_tp = own_width // block

    third = tuple(range(3, 3 + ups))
    is_home = tp == y
    not_home = jnp.logical_not(is_home)
    fourth = tuple(range(3 + ups, chunks))
    per_plane = plane_shard // block
    has_next = (z < zs - 1, z > 0)
    next_fs = (fs + ys, fs - ys)
    def scoped(name):
        def wrap(f):
            def run(*args):
                with jax.named_scope("_".join([name, *(str(a) for a in args[:2] if isinstance(a, int))])):
                    return f(*args)
            return run
        return wrap

    barrier = pltpu.get_barrier_semaphore()
    for dr in range(reps):
        for dy in range(ys):
            for dt in range(tps):
                if dr or dy or dt:
                    pl.semaphore_signal(
                        barrier, inc=1,
                        device_id={
                            "rep": lax.rem(rep + dr, reps),
                            "fs": z * ys + lax.rem(y + dy, ys),
                            "tp": lax.rem(tp + dt, tps),
                        },
                        device_id_type=MESH,
                    )
    for way in range(2):
        @pl.when(has_next[way])
        def _():
            pl.semaphore_signal(
                barrier, inc=1, device_id={"fs": next_fs[way]}, device_id_type=MESH
            )

    def remote(src, dst, send, recv, **where):
        return pltpu.make_async_remote_copy(
            src_ref=src, dst_ref=dst, send_sem=send, recv_sem=recv,
            device_id=where, device_id_type=MESH,
        )

    def rows_of(index, size=shard):
        return pl.ds(pl.multiple_of(index * size, size), size)

    def rep_rows(r):
        return pl.ds(pl.multiple_of(r * rows, rows), rows)

    half = pl.ds(pl.multiple_of(tp * sub, sub), sub)

    def columns_of(c, group):
        if c < 3:
            source, at = (w_value, w_gate, w_mix)[c], group
        elif c < 3 + ups:
            source, at = w_up, group * ups + c - 3
        else:
            source, at = w_down, group * ups + c - 3 - ups
        return source.at[:, pl.ds(pl.multiple_of(at * sub, sub), sub)]

    loads = [
        pltpu.make_async_copy(
            columns_of(c, own_group), weights.at[c, rows_of(fs), half], load_sems.at[min(c, 3)]
        )
        for c in range(chunks)
    ]
    home_cols = pl.ds(pl.multiple_of(tp * own_width, own_width), own_width)
    own_load = pltpu.make_async_copy(states, own_in, load_sems.at[4])
    home_load = pltpu.make_async_copy(
        states, rows_in.at[rep_rows(rep), home_cols], load_sems.at[5]
    )
    small_loads = [
        pltpu.make_async_copy(source, target, load_sems.at[6 + k])
        for k, (source, target) in enumerate(
            (
                (mix_gain_in, mix_gain), (taps_in, conv_kernel), (chan_gain_in, chan_gain),
                (mlp_gain_in, mlp_gain),
            )
        )
    ]
    for c in range(chunks):
        loads[c].start()
    pl.when(is_home)(home_load.start)
    own_load.start()
    for one in small_loads:
        one.start()
    along_line = sum(jnp.where(has, 1, 0) for has in has_next)
    pl.semaphore_wait(barrier, reps * ys * tps - 1 + along_line)

    def across(c):
        return remote(
            columns_of(c, rep * ys + other_y), weights.at[c, rows_of(fs), half],
            y_send.at[0], y_recv.at[c], fs=other_fs,
        )

    middle = jnp.minimum(z, zs - 1 - z)

    def offset_at(i):
        low = 2 * z < zs - 1
        near = -(i + 1) // 2 if i % 2 else i // 2
        near = jnp.where(low, near, -near)
        far = jnp.where(low, i - middle, middle - i)
        return jnp.where(i <= 2 * middle, near, far)

    offsets = [offset_at(i) for i in range(zs)]
    planes = [z + off for off in offsets]

    def moved(chunk, span, send, recv, **where):
        at = weights.at[chunk, span, half]
        return remote(at, at, send, recv, **where)

    def batch_of(c):
        return 0 if c < 3 else 1 if c < 3 + ups else 2

    def group_of(c):
        return slice(0, 2) if c < 2 else c if c == 2 else slice(3, 3 + ups)

    def twin(c, i):
        return moved(
            c, rows_of(planes[i], plane_shard), twin_send.at[batch_of(c)], twin_recv.at[0 if c < 2 else min(c - 1, 2)],
            tp=other_tp,
        )

    halves = shard // LANES

    def is_last(b, h):
        return b == ys - 1 and h == halves - 1

    def slot_of(c, part, h):
        slot = part * halves + h
        extra = c - fourth[0]
        if isinstance(part, int):
            return slot + extra if is_last(part, h) else slot
        return slot + jnp.where(part == ys - 1, extra, 0) if h == halves - 1 else slot

    def half_rows(index, h):
        return rows_of(index * halves + h, LANES)

    def twin_last(c, i, b, h):
        return moved(
            c, half_rows(planes[i] * ys + b, h), twin_send.at[batch_of(c)],
            last_twin.at[i, slot_of(c, b, h)], tp=other_tp,
        )

    def ready(c):
        group = group_of(c)
        whole_half = weights.at[group, :, half]
        remote(
            whole_half, whole_half, twin_send.at[batch_of(c)], twin_recv.at[0 if c < 2 else min(c - 1, 2)], tp=other_tp
        ).wait_recv()

    def ready_last(i, b, h, some=None):
        def wait(chunk, first):
            moved(
                chunk, half_rows(planes[i] * ys + b, h), twin_send.at[0],
                last_twin.at[i, slot_of(first, b, h)], tp=other_tp,
            ).wait_recv()

        if is_last(b, h):
            for c in fourth if some is None else some:
                wait(c, c)
        else:
            wait(slice(3 + ups, chunks), fourth[0])

    def near(c, way, part):
        if c not in fourth:
            return [
                moved(
                    c, rows_of(z * ys + part), near_send.at[way], line_recv.at[c, z],
                    fs=next_fs[way],
                )
            ]
        return [
            moved(
                c, half_rows(z * ys + part, h), near_send.at[way],
                last_recv.at[z, slot_of(c, part, h)],
                fs=next_fs[way],
            )
            for h in range(halves)
        ]

    def send_near(c, part):
        for way in range(2):
            for one in near(c, way, part):
                pl.when(has_next[way])(one.start)

    @scoped("begin")
    def begin(c):
        if c < 3:
            loads[c].wait()
        elif c == 3:
            at = weights.at[3:, rows_of(fs), half]
            pltpu.make_async_copy(at, at, load_sems.at[3]).wait()
        send_near(c, y)

    @scoped("own")
    def own(c):
        across(c).wait_recv()
        send_near(c, other_y)
        if c in fourth:
            for b in range(ys):
                for h in range(halves):
                    twin_last(c, 0, b, h).start()
        else:
            twin(c, 0).start()

    goes = [jnp.where(off < 0, z < zs - 1, z > 0) for off in offsets]

    def onward(chunk, i, span, recv):
        to = jnp.where(offsets[i] < 0, fs + ys, fs - ys)
        return moved(chunk, span, far_send.at[i - 1], recv, fs=to)

    @scoped("arrive")
    def arrive(c, i):
        copy = onward(c, i, rows_of(planes[i], plane_shard), line_recv.at[c, planes[i]])
        copy.wait_recv()
        pl.when(goes[i])(copy.start)
        twin(c, i).start()

    @scoped("arrive_last")
    def arrive_last(i, b, h, some=fourth):
        span = half_rows(planes[i] * ys + b, h)

        def copy(chunk, first):
            return onward(chunk, i, span, last_recv.at[planes[i], slot_of(first, b, h)])

        if not is_last(b, h):
            copy(slice(3 + ups, chunks), fourth[0]).wait_recv()
        for c in some:
            if is_last(b, h):
                copy(c, c).wait_recv()
            pl.when(goes[i])(copy(c, c).start)
            twin_last(c, i, b, h).start()

    @scoped("drain")
    def drain(k):
        batch = slice((0, 3, 3 + ups)[k], (3, 3 + ups, chunks)[k])
        moved(batch, slice(None), twin_send.at[k], twin_recv.at[0], tp=other_tp).wait_send()

    @scoped("drain_all")
    def drain_all():
        every = slice(None)
        moved(every, rows_of(fs), y_send.at[0], y_recv.at[0], fs=other_fs).wait_send()
        for way in range(2):
            copy = moved(
                every, rows_of(z, plane_shard), near_send.at[way], y_recv.at[0], fs=next_fs[way]
            )
            pl.when(has_next[way])(copy.wait_send)
        for i in range(1, zs):
            copy = onward(every, i, rows_of(planes[i], plane_shard), y_recv.at[0])
            pl.when(goes[i])(copy.wait_send)

    def spread(source, target, send, recv, over_from):
        def at(r, h, j):
            start = pl.multiple_of(h * own_width + j * block, block)
            return target.at[rep_rows(r), pl.ds(start, block)]

        def copies(j):
            if isinstance(j, slice):
                src, dst, j = source, target.at[rep_rows(rep), home_cols], 0
            else:
                src, dst = source.at[:, j * block : (j + 1) * block], at(rep, tp, j)
            along = remote(src, dst, send.at[0], recv.at[1, tp, j], rep=other_rep, tp=y)
            over = remote(src, dst, send.at[1], recv.at[0, tp, j], fs=other_fs, tp=y)
            inside = remote(src, dst, send.at[2], recv.at[0, tp, j], tp=y)
            return along, over, inside

        def passing(h, j):
            if h == 0 and j >= over_from:
                one = at(other_rep, 0, j)
                return remote(one, one, send.at[3], recv.at[1, 0, j], fs=other_fs)
            two = at(rep, h, j)
            return remote(two, two, send.at[3 + h], recv.at[1, h, j], rep=other_rep)

        def arrival(dr, h, j):
            dst = at(rep if dr == 0 else other_rep, h, j)
            return remote(dst, dst, send.at[0], recv.at[dr, h, j], rep=other_rep)

        def start(j):
            along, over, inside = copies(j)
            along.start()
            over.start()
            pl.when(jnp.logical_not(is_home))(inside.start)

        @scoped("forward")
        def forward(j):
            if j >= over_from:
                @pl.when(is_home)
                def _():
                    arrival(1, 0, j).wait_recv()
                    passing(0, j).start()

            @pl.when(jnp.logical_not(is_home))
            def _():
                for h in range(tps):
                    if h or j < over_from:
                        arrival(0, h, j).wait_recv()
                        passing(h, j).start()

        @scoped("finish")
        def finish(j):
            arrival(1, 1, j).wait_recv()

            @pl.when(is_home)
            def _():
                arrival(0, other_tp, j).wait_recv()
                if j < over_from:
                    arrival(1, 0, j).wait_recv()

            @pl.when(jnp.logical_not(is_home))
            def _():
                arrival(1, 0, j).wait_recv()
                if j >= over_from:
                    arrival(0, 0, j).wait_recv()

        def settle():
            along, over, inside = copies(slice(None))
            along.wait_send()
            over.wait_send()
            pl.when(not_home)(inside.wait_send)

            def part(k, blocks_sent):
                if blocks_sent:
                    sent = target.at[rep_rows(rep), : blocks_sent * block]
                    remote(sent, sent, send.at[k], recv.at[0, 0, 0], fs=other_fs).wait_send()

            pl.when(is_home)(functools.partial(part, 3, per_tp - over_from))

            @pl.when(not_home)
            def _():
                part(3, over_from)
                part(4, per_tp)

        return start, forward, finish, settle

    @scoped("norm")
    def norm_all(source, gain):
        def one(i, carry):
            span = pl.ds(pl.multiple_of(i * 64, 64), 64)
            x = source[span, :].astype(jnp.float32)
            scale = lax.rsqrt(jnp.mean(x * x, axis=-1, keepdims=True) + EPS)
            normed[span, :] = (x * scale * gain[...]).astype(jnp.bfloat16)
            return carry

        lax.fori_loop(0, tokens // 64, one, 0)

    def seq_rows(i):
        return pl.ds(pl.multiple_of(i * LENGTH, LENGTH), LENGTH)

    def mixer_rows(i):
        x = normed[seq_rows(i), :]
        value = jnp.dot(x, weights[0], preferred_element_type=jnp.float32)
        gate = jnp.dot(x, weights[1], preferred_element_type=jnp.float32)
        padded[LEAD : LEAD + LENGTH, :] = value * jax.nn.sigmoid(gate)
        per_sub = sub // LANES

        def column(j, sums):
            cols = pl.ds(pl.multiple_of(j * LANES, LANES), LANES)
            from_all = pl.multiple_of(
                (j // per_sub) * own_width + own_group * sub + lax.rem(j, per_sub) * LANES, LANES
            )
            kern = conv_kernel[:, pl.ds(from_all, LANES)]
            total = jnp.zeros((LENGTH, LANES), jnp.float32)
            for tap in range(taps):
                begin = LEAD - (taps - 1) + tap
                total = total + kern[tap : tap + 1, :] * padded[begin : begin + LENGTH, cols]
            filtered[seq_rows(i), cols] = total
            return sums[0] + total, sums[1] + total * total

        zero = jnp.zeros((LENGTH, LANES), jnp.float32)
        one, two = lax.fori_loop(0, width // LANES, column, (zero, zero))
        lane = lax.broadcasted_iota(jnp.int32, (LENGTH, LANES), 1)
        both = jnp.where(
            lane == 0,
            jnp.sum(one, axis=-1, keepdims=True),
            jnp.where(lane == 1, jnp.sum(two, axis=-1, keepdims=True), 0.0),
        )
        own_stats[i // seqs, :, seq_rows(lax.rem(i, seqs))] = both.T[0:8, :]

    def stat_copies(r):
        return [
            remote(
                own_stats.at[r], peer_stats.at[dr * ys + dy, r], stat_send.at[r],
                stat_recv.at[r],
                rep=lax.rem(rep + dr, reps), fs=z * ys + lax.rem(y + dy, ys),
            )
            for dr in range(reps) for dy in range(ys) if dr or dy
        ]

    def stat_waits(r):
        at = peer_stats.at[1:, r]
        return remote(at, at, stat_send.at[r], stat_recv.at[r], rep=other_rep)

    def activate_rows(i, carry):
        within = seq_rows(lax.rem(i, seqs))
        total = own_stats[i // seqs, :, within]
        for k in range(1, members):
            total = total + peer_stats[k, i // seqs, :, within]
        turned = jnp.concatenate([total] * (LANES // 8), axis=0).T
        mean = turned[:, 0:1] / channels
        variance = turned[:, 1:2] / channels - mean * mean
        gain = jnp.concatenate(
            [
                chan_gain[:, pl.ds(pl.multiple_of(t * own_width + own_group * sub, sub), sub)]
                for t in range(tps)
            ],
            axis=1,
        )
        x = (filtered[seq_rows(i), :] - mean) * lax.rsqrt(variance + EPS) * gain
        activated[seq_rows(i), :] = (x / (1.0 + jnp.exp(-x))).astype(jnp.bfloat16)
        return carry

    def term_of(o, dr, part, k, c, left):
        at = rep_rows(lax.rem(rep + dr, reps))
        span = pl.ds(pl.multiple_of(o * block + part[0], part[1]), part[1])
        return times_transposed(left[at, k * width : (k + 1) * width], weights[c, span, :])

    def send_share(o, dr, part, total, parts, peers, send, recv):
        to = lax.rem(rep + dr, reps)
        cols, at = pl.ds(*part), rep_rows(to)
        keeper, kept = o // per_tp, lax.rem(o, per_tp)
        parts[o, at, cols] = total.astype(jnp.bfloat16)
        slot = lax.rem(rep + reps - to, reps) * ys + lax.rem(y + ys - tp, ys)
        copy = remote(
            parts.at[o, at, cols], peers.at[slot, kept, :, cols], send.at[dr], recv.at[kept],
            rep=to, fs=z * ys + tp, tp=keeper,
        )
        here = jnp.logical_and(is_home, jnp.logical_and(keeper == tp, to == rep))
        pl.when(jnp.logical_not(here))(copy.start)

    @scoped("share")
    def share(o, dr, part, left, pieces_of, *where):
        total = None
        for k, c in enumerate(pieces_of):
            term = term_of(o, dr, part, k, c, left)
            total = term if total is None else total + term
        send_share(o, dr, part, total, *where)

    def along_first(o):
        return o % 2 == 0

    def stage_copy(o, r):
        if along_first(o):
            return remote(
                mix_parts.at[o, rep_rows(other_rep), :], stage.at[o, 0], stage_send.at[0],
                stage_recv.at[o], rep=other_rep,
            )
        return remote(
            mix_parts.at[o, rep_rows(r), :], stage.at[o, r], stage_send.at[1],
            stage_recv.at[o], fs=z * ys + tp,
        )

    def last_copies(o):
        keeper, kept = o // per_tp, o % per_tp
        own_part = mix_parts.at[o, rep_rows(rep), :]
        inside = remote(
            own_part, mix_peers.at[0, kept], mix_send.at[0], mix_recv.at[kept], tp=keeper
        )
        if along_first(o):
            outside = remote(
                own_part, mix_peers.at[1, kept], mix_send.at[1], mix_recv.at[kept],
                fs=z * ys + tp, tp=keeper,
            )
        else:
            outside = remote(
                mix_parts.at[o, rep_rows(other_rep), :], mix_peers.at[1, kept],
                mix_send.at[1], mix_recv.at[kept], rep=other_rep, tp=keeper,
            )
        inner_one = jnp.logical_and(is_home, tp != keeper)
        return inside, inner_one, outside, not_home if along_first(o) else is_home

    @scoped("mix_share")
    def mix_share(o, r):
        at = rep_rows(r)
        mix_parts[o, at, :] = times_transposed(
            activated[at, :], weights[2, o * block : (o + 1) * block, :]
        ).astype(jnp.bfloat16)
        pl.when(rep != r if along_first(o) else not_home)(stage_copy(o, r).start)

    def mix_add(o, at, k):
        total = mix_parts[o, at, :].astype(jnp.float32) + stage[o, k].astype(jnp.float32)
        mix_parts[o, at, :] = total.astype(jnp.bfloat16)

    @scoped("combine")
    def combine(o):
        keeper, kept = o // per_tp, o % per_tp
        inside, inner_one, outside, outer_one = last_copies(o)

        def pass_on():
            pl.when(outer_one)(outside.start)
            pl.when(inner_one)(inside.start)

            @pl.when(jnp.logical_and(is_home, tp == keeper))
            def _():
                mix_peers[0, kept] = mix_parts[o, rep_rows(rep), :]

        if along_first(o):
            stage_copy(o, 0).wait_recv()
            mix_add(o, rep_rows(rep), 0)
            pass_on()
        else:
            @pl.when(is_home)
            def _():
                both = stage.at[o]
                remote(both, both, stage_send.at[1], stage_recv.at[o], fs=other_fs).wait_recv()
                for r in range(reps):
                    mix_add(o, rep_rows(r), r)
                pass_on()

    @scoped("mix_final")
    def mix_final(j):
        def some(start):
            at = mix_peers.at[start:, j]
            return remote(at, at, mix_send.at[0], mix_recv.at[j], rep=other_rep)

        pl.when(is_home)(some(1).wait_recv)
        pl.when(not_home)(some(0).wait_recv)
        return mix_peers[0, j].astype(jnp.float32) + mix_peers[1, j].astype(jnp.float32)

    def mix_settle():
        def sent(count, send):
            at = mix_parts.at[:count, rep_rows(rep), :]
            return remote(at, at, send, mix_recv.at[0], rep=other_rep)

        even = sum(1 for o in range(blocks) if along_first(o))
        sent(even, stage_send.at[0]).wait_send()
        pl.when(not_home)(sent((blocks - even) * reps, stage_send.at[1]).wait_send)
        pl.when(is_home)(sent(per_tp, mix_send.at[0]).wait_send)
        pl.when(not_home)(sent(even, mix_send.at[1]).wait_send)
        pl.when(is_home)(sent(blocks - even, mix_send.at[1]).wait_send)

    @scoped("peers")
    def wait_peers(j, parts, peers, send, recv):
        def some(start, stop):
            at = peers.at[start:stop, j]
            return remote(at, at, send.at[0], recv.at[j], rep=other_rep)

        direct = (tp * per_tp + j) // ys == planes[zs - 1]
        for is_direct, stop in ((direct, members), (jnp.logical_not(direct), 2)):
            pl.when(jnp.logical_and(is_home, is_direct))(some(1, stop).wait_recv)
            pl.when(jnp.logical_and(not_home, is_direct))(some(0, stop).wait_recv)

        @pl.when(is_home)
        def _():
            peers[0, j] = parts[tp * per_tp + j, rep_rows(rep), :]

        return direct

    def fed_stage_copy(i, b, r):
        o, k = planes[i] * ys + b, i * ys + b
        if b % 2 == 0:
            return remote(
                fed_parts.at[o, rep_rows(other_rep), :], fed_stage.at[k, 0],
                fed_stage_send.at[0], fed_stage_recv.at[k], rep=other_rep,
            )
        return remote(
            fed_parts.at[o, rep_rows(r), :], fed_stage.at[k, r],
            fed_stage_send.at[1], fed_stage_recv.at[k], fs=z * ys + tp,
        )

    @scoped("fed_share")
    def fed_share(i, b):
        o = planes[i] * ys + b
        for dr in (*range(1, reps), 0):
            to = lax.rem(rep + dr, reps)
            total = None
            for k, c in enumerate(fourth):
                term = term_of(o, dr, (0, block), k, c, hidden)
                total = term if total is None else total + term
            fed_parts[o, rep_rows(to), :] = total.astype(jnp.bfloat16)
            if b % 2:
                pl.when(not_home)(fed_stage_copy(i, b, to).start)
            elif dr:
                fed_stage_copy(i, b, to).start()

    @scoped("fed_combine")
    def fed_combine(i, b):
        o, k = planes[i] * ys + b, i * ys + b
        keeper, kept = o // per_tp, lax.rem(o, per_tp)
        own_part = fed_parts.at[o, rep_rows(rep), :]
        inside = remote(
            own_part, fed_peers.at[0, kept], fed_pass_send.at[0], fed_recv.at[kept], tp=keeper
        )

        def add(r, slot):
            at = rep_rows(r)
            total = fed_parts[o, at, :].astype(jnp.float32) + fed_stage[k, slot].astype(
                jnp.float32
            )
            fed_parts[o, at, :] = total.astype(jnp.bfloat16)

        if b % 2 == 0:
            fed_stage_copy(i, b, 0).wait_recv()
            add(rep, 0)
            outside = remote(
                own_part, fed_peers.at[1, kept], fed_pass_send.at[1], fed_recv.at[kept],
                fs=z * ys + tp, tp=keeper,
            )
            pl.when(not_home)(outside.start)
            pl.when(jnp.logical_and(is_home, keeper != tp))(inside.start)
        else:
            outside = remote(
                fed_parts.at[o, rep_rows(other_rep), :], fed_peers.at[1, kept],
                fed_pass_send.at[1], fed_recv.at[kept], rep=other_rep, tp=keeper,
            )

            @pl.when(is_home)
            def _():
                both = fed_stage.at[k]
                remote(
                    both, both, fed_stage_send.at[1], fed_stage_recv.at[k], fs=other_fs
                ).wait_recv()
                for r in range(reps):
                    add(r, r)
                outside.start()
                pl.when(keeper != tp)(inside.start)

    def settle_share(parts, send, recv):
        def sent(count, sem):
            at = parts.at[:count, rep_rows(rep), :]
            return remote(at, at, sem, recv.at[0], rep=other_rep).wait_send

        last_away = planes[zs - 1] * ys // per_tp != tp
        last_here = jnp.logical_not(last_away)
        for dr in range(1, reps):
            sent(ys, send.at[dr])()
        pl.when(jnp.logical_or(not_home, last_away))(sent(ys, send.at[0]))
        sent(zs - 1, fed_stage_send.at[0])()
        pl.when(not_home)(sent((zs - 1) * reps, fed_stage_send.at[1]))
        sent(zs - 1, fed_pass_send.at[1])()
        if per_tp > ys:
            pl.when(jnp.logical_and(is_home, last_away))(sent(per_tp - ys, fed_pass_send.at[0]))
        pl.when(jnp.logical_and(is_home, last_here))(sent(per_tp, fed_pass_send.at[0]))

    def total_of(j, peers, count):
        total = peers[0, j].astype(jnp.float32)
        for k in range(1, count):
            total = total + peers[k, j].astype(jnp.float32)
        return total

    start_in, forward_in, finish_in, settle_in = spread(
        states, rows_in, in_send, in_recv, per_tp // 2
    )
    start_mid, forward_mid, finish_mid, settle_mid = spread(
        own_mid, rows_mid, mid_send, mid_recv, 0
    )

    def inner(*todo):
        @pl.when(middle > 0)
        def _():
            for one in todo:
                one()

    def outer(*todo):
        @pl.when(middle == 0)
        def _():
            for one in todo:
                one()

    def pump(c, i):
        return functools.partial(arrive, c, i)

    def all_of(c):
        return [pump(c, i) for i in range(1, zs)]

    def whole(c):
        return [functools.partial(begin, c), functools.partial(own, c)]

    across(0).start()
    across(1).start()
    begin(0)
    begin(1)
    for j in range(per_tp):
        start_in(j)
    own(0)
    own(1)
    across(2).start()
    across(3).start()
    begin(2)
    padded[0:LEAD, :] = jnp.zeros((LEAD, width), jnp.float32)
    arrive(0, 1)
    inner(pump(0, 2))
    arrive(1, 1)
    inner(pump(1, 2))
    forward_in(0)
    for j in range(1, per_tp // 2):
        forward_in(j)
    inner(*[pump(c, i) for i in range(3, zs) for c in (0, 1)])
    for j in range(per_tp // 2, per_tp):
        forward_in(j)
    own(2)
    outer(*[pump(c, 2) for c in (0, 1)])
    for j in range(per_tp):
        finish_in(j)
    for c in range(4, chunks):
        across(c).start()
    pl.when(is_home)(home_load.wait)
    for one in small_loads:
        one.wait()
    norm_all(rows_in, mix_gain)
    outer(*[pump(c, i) for i in range(3, zs) for c in (0, 1)])
    ready(0)

    inner(*all_of(2)[:1], functools.partial(begin, 3))
    outer(*whole(3))
    inside = [
        all_of(2)[1:2], all_of(2)[2:] + [functools.partial(own, 3)], whole(4), [],
    ]
    outside = [whole(4), whole(5), whole(fourth[0]), sum([whole(c) for c in fourth[1:]], [])]
    for r in range(reps):
        for cut in ((0, (seqs + 1) // 2), ((seqs + 1) // 2, seqs)):
            with jax.named_scope("mixer"):
                lax.fori_loop(
                    r * seqs + cut[0], r * seqs + cut[1],
                    lambda k, carry: (mixer_rows(k), carry)[1], 0,
                )
            if inside:
                inner(*inside.pop(0))
                outer(*outside.pop(0))
        for one in stat_copies(r):
            one.start()
    outer(*all_of(2))
    ready(2)
    for r in range(reps):
        with jax.named_scope("stats"):
            stat_waits(r).wait_recv()
        with jax.named_scope("activate"):
            lax.fori_loop(r * seqs, (r + 1) * seqs, activate_rows, 0)
        for j in range(per_tp):
            for t in range(tps):
                mix_share(t * per_tp + j, r)

    own_load.wait()
    inner(*whole(5), *all_of(3)[:2], *whole(fourth[0]))
    def last(i, b):
        return [functools.partial(arrive_last, i, b, h) for h in range(halves)]

    early = [
        all_of(3)[2:] + all_of(4)[:2],
        all_of(4)[2:] + all_of(5)[:2],
        all_of(5)[2:] + sum([whole(c) for c in fourth[1:]], []),
    ]
    late = [[], all_of(3), all_of(4)[:1], all_of(4)[1:]]
    for t in range(tps):
        combine(t * per_tp)
    for j in range(per_tp):
        if j + 1 < per_tp:
            for t in range(tps):
                combine(t * per_tp + j + 1)
        mixed = mix_final(j)
        cols = slice(j * block, (j + 1) * block)
        own_mid[:, cols] = (own_in[:, cols].astype(jnp.float32) + mixed).astype(jnp.bfloat16)
        start_mid(j)

        @pl.when(is_home)
        def _():
            start = pl.multiple_of(tp * own_width + j * block, block)
            rows_mid[rep_rows(rep), pl.ds(start, block)] = own_mid[:, cols]

        if j:
            forward_mid(j - 1)
        if j < len(early):
            inner(*early[j])
        if j == per_tp - 1:
            forward_mid(j)
            inner(*[one for b in range(ys) for one in last(1, b)])
        if j < len(late):
            outer(*late[j])
    for rest in early[per_tp:]:
        inner(*rest)
    for rest in late[per_tp:]:
        outer(*rest)
    for j in range(per_tp):
        finish_mid(j)
    outer(*all_of(5))
    inner(*last(2, 0))
    norm_all(rows_mid, mlp_gain)
    ready(3)

    @scoped("up")
    def up_some(k):
        def up_rows(i, carry):
            at = rep_rows(i)
            x = jnp.dot(normed[at, :], weights[3 + k], preferred_element_type=jnp.float32)
            x = jnp.maximum(x, 0.0)
            hidden[at, k * width : (k + 1) * width] = (x * x).astype(jnp.bfloat16)
            return carry

        lax.fori_loop(0, reps, up_rows, 0)

    for k in range(ups):
        up_some(k)
    pending = []
    fed = (hidden, fourth, fed_parts, fed_peers, fed_send, fed_recv)
    settle_in()
    settle_mid()
    mix_settle()
    for r in range(reps):
        stat_waits(r).wait_send()
    for i in range(zs):
        for b in range(ys):
            if i == 0 and b:
                inner(*last(2, b))
            if 0 < i < zs - 2:
                inner(*last(i + 2, b))
            if i < zs - 1:
                if i:
                    outer(*last(i, b))
                for h in range(halves):
                    ready_last(i, b, h)
                fed_share(i, b)
                pending.append((i, b))
                if len(pending) > 3:
                    fed_combine(*pending.pop(0))
            else:
                o, ways = planes[i] * ys + b, (*range(1, reps), 0)
                final = functools.partial(arrive_last, i, b, halves - 1)
                for h in range(halves):
                    part = (h * LANES, LANES)
                    if not is_last(b, h):
                        outer(last(i, b)[h])
                        ready_last(i, b, h)
                        for n_way, dr in enumerate(ways):
                            share(o, dr, part, *fed)
                            if n_way == 0 and is_last(b, h + 1):
                                outer(functools.partial(final, fourth[:-1]))
                        for _ in range(2):
                            if pending:
                                fed_combine(*pending.pop(0))
                        continue
                    if halves == 1:
                        outer(functools.partial(final, fourth[:-1]))
                    outer(functools.partial(final, fourth[-1:]))
                    totals = [None] * reps
                    for k, c in enumerate(fourth):
                        ready_last(i, b, h, (c,))
                        for dr in ways:
                            term = term_of(o, dr, part, k, c, hidden)
                            totals[dr] = term if k == 0 else totals[dr] + term
                            if k == ups - 1:
                                send_share(o, dr, part, totals[dr], *fed[2:])
            if i == 1 and b == 0:
                drain(0)
                drain(1)
    while pending:
        fed_combine(*pending.pop(0))
    for j in range(per_tp):
        if j == per_tp - 1:
            drain(2)
            drain_all()
        direct = wait_peers(j, fed_parts, fed_peers, fed_send, fed_recv)
        cols = slice(j * block, (j + 1) * block)
        with jax.named_scope("out"):
            for is_direct, count in ((direct, members), (jnp.logical_not(direct), 2)):
                @pl.when(is_direct)
                def _():
                    out[:, cols] = (
                        own_mid[:, cols].astype(jnp.float32) + total_of(j, fed_peers, count)
                    ).astype(jnp.bfloat16)
    with jax.named_scope("done"):
        settle_share(fed_parts, fed_send, fed_recv)


def plane_body(mesh, states, mix_gain, w_value, w_gate, conv_kernel, chan_gain, w_mix, mlp_gain, w_up, w_down):
    reps, n, tps = mesh.shape["rep"], mesh.shape["fs"], mesh.shape["tp"]
    rows, own_width = states.shape
    ys = tps
    zs, members = n // ys, reps * ys
    sub = own_width // members
    width = sub * tps
    channels = own_width * tps
    ups = w_up.shape[1] // own_width
    tokens = rows * reps
    block = channels // n
    halves = block // LANES
    blocks, per_tp = channels // block, own_width // block
    chunks = 3 + 2 * ups
    bf16, f32 = jnp.bfloat16, jnp.float32
    vmem, hbm = pl.BlockSpec(memory_space=pltpu.VMEM), pl.BlockSpec(memory_space=pl.ANY)
    dma = pltpu.SemaphoreType.DMA
    return pl.pallas_call(
        functools.partial(plane_kernel, (reps, n, tps, rows, channels, sub, ups)),
        out_shape=pltpu.VMEM((rows, own_width), bf16),
        in_specs=[hbm] * 10,
        out_specs=vmem,
        scratch_shapes=[
            pltpu.VMEM((1, channels), f32),
            pltpu.VMEM(conv_kernel.shape, f32),
            pltpu.VMEM((1, channels), f32),
            pltpu.VMEM((1, channels), f32),
            pltpu.VMEM((chunks, channels, width), bf16),
            pltpu.VMEM((tokens, channels), bf16),
            pltpu.VMEM((tokens, channels), bf16),
            pltpu.VMEM((tokens, channels), bf16),
            pltpu.VMEM((LEAD + LENGTH, width), f32),
            pltpu.VMEM((tokens, width), f32),
            pltpu.VMEM((tokens, width), bf16),
            pltpu.VMEM((tokens, ups * width), bf16),
            pltpu.VMEM((rows, own_width), bf16),
            pltpu.VMEM((rows, own_width), bf16),
            pltpu.VMEM((reps, 8, rows), f32),
            pltpu.VMEM((members, reps, 8, rows), f32),
            pltpu.VMEM((blocks, tokens, block), bf16),
            pltpu.VMEM((blocks, reps, rows, block), bf16),
            pltpu.VMEM((2, per_tp, rows, block), bf16),
            pltpu.VMEM((blocks, tokens, block), bf16),
            pltpu.VMEM(((zs - 1) * ys, reps, rows, block), bf16),
            pltpu.VMEM((members, per_tp, rows, block), bf16),
            dma((10,)),
            dma((1,)),
            dma((chunks,)),
            dma((2,)),
            dma((zs - 1,)),
            dma((3 + ups, zs)),
            dma((zs, ys * halves + ups - 1)),
            dma((3,)),
            dma((3,)),
            dma((zs, ys * halves + ups - 1)),
            dma((5,)),
            dma((reps, tps, per_tp)),
            dma((5,)),
            dma((reps, tps, per_tp)),
            dma((reps,)),
            dma((reps,)),
            dma((2,)),
            dma((blocks,)),
            dma((2,)),
            dma((per_tp,)),
            dma((reps,)),
            dma((per_tp,)),
            dma((2,)),
            dma(((zs - 1) * ys,)),
            dma((2,)),
        ],
        compiler_params=pltpu.CompilerParams(
            collective_id=0, has_side_effects=True, vmem_limit_bytes=56 * 1024 * 1024
        ),
    )(
        states, mix_gain[None, :], w_value, w_gate, conv_kernel, chan_gain[None, :], w_mix,
        mlp_gain[None, :], w_up, w_down,
    )


def body(mesh, states, *weights):
    reps, n, tps = mesh.shape["rep"], mesh.shape["fs"], mesh.shape["tp"]
    own_width = states.shape[1]
    channels = own_width * tps
    planar = (
        reps == tps == 2
        and n % tps == 0
        and n // tps > 2
        and own_width % (reps * tps * LANES) == 0
        and channels % (n * LANES) == 0
        and own_width % (tps * (channels // n)) == 0
    )
    return (plane_body if planar else ring_body)(mesh, states, *weights)


def solution(mesh):
    in_specs = (
        P(("rep", "fs"), "tp"),
        P(),
        P("fs", "tp"),
        P("fs", "tp"),
        P(),
        P(),
        P("fs", "tp"),
        P(),
        P("fs", "tp"),
        P("fs", "tp"),
    )
    out_specs = P(("rep", "fs"), "tp")
    return jax.shard_map(
        functools.partial(body, mesh),
        mesh=mesh, in_specs=in_specs, out_specs=out_specs, check_vma=False,
    )
```
